32 devices in a mesh: grp: 2 (over y), sp: 4 (over z), dp: 4 (over x, core).
Axes of the slice: x: 2, y: 2, z: 4, core: 2. Of those that a mesh axis runs over, the one named last changes fastest.
Arguments:
- query_rows: bfloat16 [8, 512, 2048], P(('grp', 'dp'), 'sp'), parts along dimension 0, may hold values from -6 to 6
- key_rows: bfloat16 [8, 512, 2048], P(('grp', 'dp'), 'sp'), parts along dimension 0, may hold values from -6 to 6
- value_rows: bfloat16 [8, 512, 2048], P(('grp', 'dp'), 'sp'), parts along dimension 0, may hold values from -6 to 6
- query_gain: float32 [64], replicated, may hold values from 1.1 to 7
- key_gain: float32 [64], replicated, may hold values from 1.1 to 7
- lambdas: float32 [16], replicated, may hold values from 0.3 to 0.8
- head_gain: float32 [128], replicated, may hold values from 0.1 to 1.9
- out_weight: bfloat16 [2048, 2048], P(None, 'dp'), may hold values from -0.125 to 0.125
Outputs:
- attended: bfloat16 [8, 512, 2048], P(('grp', 'dp'), 'sp'), parts along dimension 0
The draws below stay inside these ranges and needn't reach their ends.
There are 2 independent parts, one for each index of `grp`. The reference program is written for one: setup_inputs(seed, part) draws one part's arguments, and reference() takes and returns one part's arrays. A program takes and returns all parts, laid end to end along the dimension named above; an argument that names none is the same for every part. Nothing has to cross between parts.
All inputs are finite; a program needn't handle non-finite values.
Results may differ from the reference program's by a relative error of at most 0.008.
The reference program's roundings to bfloat16 on the way count: a program that leaves them out, or rounds other values in their place, can miss the bound.
Values may be sent and summed in bfloat16 or wider, within the bound.
A program may use at most 128 MiB of HBM per device.

```python
import jax
import jax.numpy as jnp
from jax import lax

D = 2048
HEADS = 16
HEAD = 64
VDIM = 128
LENGTH = 512
SEQS = 4


def paired_rows(key):
    shape = (SEQS, LENGTH, HEADS * 2 * HEAD)
    key_part = jnp.clip(jax.random.normal(jax.random.fold_in(key, 101), shape, jnp.float32), -6.0, 6.0)
    query_part = jnp.clip(jax.random.normal(jax.random.fold_in(key, 202), shape, jnp.float32), -6.0, 6.0)
    return (query_part, key_part)


def draw_query_rows(key, part):
    return paired_rows(key)[0].astype(jnp.bfloat16)


def draw_key_rows(key, part):
    return paired_rows(key)[1].astype(jnp.bfloat16)


def gain_draw(key):
    return jax.random.uniform(key, (HEAD,), jnp.float32, 1.1, 1.7)


def draw_query_gain(key, part):
    return gain_draw(jax.random.fold_in(key, 31))


def draw_key_gain(key, part):
    return gain_draw(jax.random.fold_in(key, 32))


def shard_levels(key, shape, cuts, smallest, largest):
    level, own = 1.0, jax.random.fold_in(key, 6)
    for dim, shards_of in cuts:
        steps = jnp.exp(jax.random.uniform(jax.random.fold_in(own, dim), (shards_of,), jnp.float32, smallest / len(cuts), largest / len(cuts)))
        level = level * jnp.repeat(steps, shape[dim] // shards_of).reshape([-1 if axis == dim else 1 for axis in range(len(shape))])
    return level


def noise(rng, shape, scale, limit, split=(), kind=jnp.bfloat16):
    factor_of = shard_levels(rng, shape, split, -0.22, 0.18) if split else 1.0
    values = jax.random.normal(rng, shape, jnp.float32) * scale * factor_of
    return jnp.minimum(jnp.maximum(values, -limit), limit).astype(kind)


def setup_inputs(seed: int = 0, part: int = 0) -> dict:
    key_of = jax.random.split(jax.random.key(seed), 9)
    own_keys = jax.random.split(jax.random.fold_in(key_of[8], part), 9)
    query_rows = draw_query_rows(jax.random.fold_in(jax.random.fold_in(key_of[8], part), 71), part)
    key_rows = draw_key_rows(jax.random.fold_in(jax.random.fold_in(key_of[8], part), 71), part)
    value_rows = noise(own_keys[2], (SEQS, LENGTH, HEADS * VDIM), 1.0, 6.0, ((0, 4), (1, 4)))
    query_gain = draw_query_gain(jax.random.fold_in(key_of[8], 71), part)
    key_gain = draw_key_gain(jax.random.fold_in(key_of[8], 71), part)
    lambdas = jnp.clip(jax.random.uniform(key_of[5], (HEADS,), jnp.float32, 0.3, 0.8), 0.3, 0.8)
    head_gain = jnp.clip(1.0 + 0.18 * jax.random.normal(key_of[6], (VDIM,), jnp.float32), 0.1, 1.9)
    out_weight = noise(key_of[7], (HEADS * VDIM, D), (HEADS * VDIM) ** -0.5, 0.125, ((1, 4),))
    return {"query_rows": query_rows, "key_rows": key_rows, "value_rows": value_rows, "query_gain": query_gain, "key_gain": key_gain, "lambdas": lambdas, "head_gain": head_gain, "out_weight": out_weight}


EPSILON = 1e-06
OUT_SCALE = 0.8

def norm_rotate(field_rows, gain_vector, positions):
    widened = field_rows.astype(jnp.float32)
    normed = widened * lax.rsqrt(lax.optimization_barrier(jnp.mean(widened * widened, axis=-1, keepdims=True)) + EPSILON) * gain_vector
    half_size = field_rows.shape[-1] // 2
    inverse = 10000.0 ** (-jnp.arange(half_size, dtype=jnp.float32) / half_size)
    angles = (positions[:, None] * inverse[None, :]).reshape(positions.shape[0], 1, 1, half_size)
    cosine_part = jnp.cos(angles)
    sine_part = jnp.sin(angles)
    first_half = normed[..., :half_size]
    second_half = normed[..., half_size:]
    turned = jnp.concatenate([first_half * cosine_part - second_half * sine_part, second_half * cosine_part + first_half * sine_part], axis=-1)
    return turned.astype(jnp.bfloat16)

def head_norm(raw_heads, gain_vector):
    scaled = raw_heads * lax.rsqrt(lax.optimization_barrier(jnp.mean(raw_heads * raw_heads, axis=-1, keepdims=True)) + EPSILON)
    return (scaled * gain_vector * OUT_SCALE).astype(jnp.bfloat16)

def block_size(length):
    return 512 if length % 512 == 0 else length

def attend(query_head, key_head, value_head, weight_two, gain_vector):
    length = query_head.shape[0]
    block_rows = block_size(length)
    score_scale = query_head.shape[-1] ** (-0.5)
    key_wide = key_head.astype(jnp.float32)
    key_positions = jnp.arange(length, dtype=jnp.int32)

    def one_block(number):
        first_row = number * block_rows
        query_block = lax.dynamic_slice_in_dim(query_head, first_row, block_rows, 0).astype(jnp.float32)
        scores = jnp.einsum('qcd,kcd->cqk', query_block, key_wide) * score_scale
        query_positions = first_row + jnp.arange(block_rows, dtype=jnp.int32)
        visible = key_positions[None, :] <= query_positions[:, None]
        scores = jnp.where(visible[None], scores, -1e+30)
        highest = lax.optimization_barrier(jnp.max(scores, axis=-1, keepdims=True))
        exponent = jnp.exp(scores - highest)
        probabilities = exponent / lax.optimization_barrier(jnp.sum(exponent, axis=-1, keepdims=True))
        mixing = (probabilities[0] - weight_two * probabilities[1]).astype(jnp.bfloat16)
        return jnp.dot(mixing, value_head, preferred_element_type=jnp.float32)
    blocks = lax.map(one_block, jnp.arange(length // block_rows, dtype=jnp.int32))
    return head_norm(blocks.reshape(length, value_head.shape[-1]), gain_vector)

def reference(query_rows, key_rows, value_rows, query_gain, key_gain, lambdas, head_gain, out_weight):
    seq_count = query_rows.shape[0]
    length = query_rows.shape[1]
    positions = jnp.arange(length, dtype=jnp.float32)
    query_rot = norm_rotate(query_rows.reshape(seq_count, length, HEADS, 2, HEAD), query_gain, positions)
    key_rot = norm_rotate(key_rows.reshape(seq_count, length, HEADS, 2, HEAD), key_gain, positions)
    value_heads = value_rows.reshape(seq_count, length, HEADS, VDIM)

    def per_item(number):
        seq_index = number // HEADS
        head_index = number % HEADS
        return attend(query_rot[seq_index, :, head_index], key_rot[seq_index, :, head_index], value_heads[seq_index, :, head_index], lambdas[head_index], head_gain)
    outputs = lax.map(per_item, jnp.arange(seq_count * HEADS, dtype=jnp.int32))
    outputs = outputs.reshape(seq_count, HEADS, length, VDIM).transpose(0, 2, 1, 3)
    outputs = outputs.reshape(seq_count * length, HEADS * VDIM)
    attended = jnp.dot(outputs, out_weight, preferred_element_type=jnp.float32).astype(jnp.bfloat16)
    return attended.reshape(seq_count, length, out_weight.shape[1])
```

```python
import functools
import math

import jax
import jax.numpy as jnp
import numpy as np
from jax import lax
from jax.experimental import pallas as pl
from jax.experimental.pallas import tpu as pltpu
from jax.sharding import PartitionSpec as P

EPSILON = 1e-06
OUT_SCALE = 0.8
CORES = 2
CHUNKS = 2
WAYS = 2
PARTS = 4
GROUP = 4
LAG = 3
MESH = pl.DeviceIdType.MESH


def rotation_tables(length, head_size):
    half = head_size // 2
    inverse = np.float32(10000.0) ** (-np.arange(half, dtype=np.float32) / np.float32(half))
    angles = np.arange(length, dtype=np.float32)[:, None] * inverse.astype(np.float32)[None, :]
    cosine, sine = np.cos(angles), np.sin(angles)
    return (
        np.concatenate([cosine] * 4, axis=1).astype(np.float32),
        np.concatenate([-sine, sine] * 2, axis=1).astype(np.float32),
    )


def kernel(
    n, n_dp, n_grp, head_size, q_ref, k_ref, v_ref, qg_ref, kg_ref, lam_ref, hg_ref, w_ref, cos_in, sin_in,
    out_ref, total, rx, rot_q, rot_k, heads_out, hrx, wfull,
    in_send, in_recv, ret_send, ret_recv, wx_send, wx_recv, wy_send, wy_recv, wc_send, wc_recv, own_sem, cos_ref, sin_ref, table_sem,
):
    me = lax.axis_index("sp")
    dp = lax.axis_index("dp")
    ways = WAYS if n_grp == WAYS else 1
    grp = lax.axis_index("grp") if ways > 1 else 0
    cores = CORES if n_dp % CORES == 0 else 1
    nx = n_dp // cores
    xi, core = dp // cores, lax.rem(dp, cores)
    tok = q_ref.shape[1]
    width = 2 * head_size
    local_heads = rx.shape[1]
    length = rx.shape[2]
    depth = w_ref.shape[0]
    cols = w_ref.shape[1]
    piece = depth // (CHUNKS * ways)

    def sp_peer(off):
        return lax.rem(me + off, n)

    def dp_index(xo, co):
        return lax.rem(xi + xo, nx) * cores + lax.rem(core + co, cores)

    barrier = pltpu.get_barrier_semaphore()
    for off in range(1, n):
        pl.semaphore_signal(barrier, inc=1, device_id={"sp": sp_peer(off)}, device_id_type=MESH)
    for xo in range(1, nx):
        pl.semaphore_signal(barrier, inc=1, device_id={"dp": dp_index(xo, 0)}, device_id_type=MESH)
    for co in range(1, cores):
        pl.semaphore_signal(barrier, inc=1, device_id={"dp": dp_index(0, co)}, device_id_type=MESH)

    if ways > 1:
        pl.semaphore_signal(
            barrier, inc=1, device_id={"grp": lax.rem(grp + 1, ways)}, device_id_type=MESH
        )

    sources = (k_ref, q_ref, v_ref)

    def own_rows(t, j):
        column = pl.multiple_of((me * local_heads + j) * width, width)
        return pltpu.make_async_copy(
            sources[t].at[0, :, pl.ds(column, width)],
            rx.at[t, j, pl.ds(pl.multiple_of(me * tok, tok), tok), :],
            in_recv.at[t, j, 0],
        )

    def rows_to(t, j, off):
        peer = sp_peer(off)
        column = pl.multiple_of((peer * local_heads + j) * width, width)
        return pltpu.make_async_remote_copy(
            src_ref=sources[t].at[0, :, pl.ds(column, width)],
            dst_ref=rx.at[t, j, pl.ds(pl.multiple_of(me * tok, tok), tok), :],
            send_sem=in_send.at[t, j, off],
            recv_sem=in_recv.at[t, j, off],
            device_id={"sp": peer},
            device_id_type=MESH,
        )

    def rows_from(t, j, off):
        peer = lax.rem(me + n - off, n)
        block = rx.at[t, j, pl.ds(pl.multiple_of(peer * tok, tok), tok), :]
        return pltpu.make_async_remote_copy(
            src_ref=block, dst_ref=block, send_sem=in_send.at[t, j, off],
            recv_sem=in_recv.at[t, j, off], device_id={"sp": peer}, device_id_type=MESH,
        )

    def piece_rows(r, way):
        first = (r * ways + lax.rem(grp + way, ways)) * piece
        return pl.ds(pl.multiple_of(first, piece), piece)

    def moved(source, target, send_sem, recv_sem, device):
        return pltpu.make_async_remote_copy(
            src_ref=source, dst_ref=target, send_sem=send_sem, recv_sem=recv_sem,
            device_id=device, device_id_type=MESH,
        )

    def weight_x(xo, r):
        rows = piece_rows(r, 0)
        return moved(
            w_ref.at[rows, :], wfull.at[dp, rows, :], wx_send.at[xo, r], wx_recv.at[xo, r],
            {"dp": dp_index(xo, 0)},
        )

    def weight_x_in(xo, r):
        block = wfull.at[dp_index(nx - xo, 0), piece_rows(r, 0), :]
        return moved(block, block, wx_send.at[xo, r], wx_recv.at[xo, r], {"dp": dp_index(xo, 0)})

    def weight_y(xo, r):
        block = wfull.at[dp_index(nx - xo, 0), piece_rows(r, 0), :]
        return moved(block, block, wy_send.at[xo, r], wy_recv.at[xo, r], {"grp": lax.rem(grp + 1, ways)})

    def weight_y_in(xo, r):
        block = wfull.at[dp_index(nx - xo, 0), piece_rows(r, 1), :]
        return moved(block, block, wy_send.at[xo, r], wy_recv.at[xo, r], {"grp": lax.rem(grp + 1, ways)})

    def weight_core(xo, r, way):
        rows = piece_rows(r, way)
        target = wfull.at[dp_index(nx - xo, 0), rows, :]
        return moved(
            w_ref.at[rows, :] if xo == 0 else target, target,
            wc_send.at[xo, r, way], wc_recv.at[xo, r, way], {"dp": dp_index(0, 1)},
        )

    def weight_core_in(xo, r, way):
        block = wfull.at[dp_index(nx - xo, 1), piece_rows(r, way), :]
        return moved(
            block, block, wc_send.at[xo, r, way], wc_recv.at[xo, r, way], {"dp": dp_index(0, 1)}
        )

    own_weight = pltpu.make_async_copy(w_ref, wfull.at[dp], own_sem)
    own_weight.start()
    tables = [
        pltpu.make_async_copy(cos_in, cos_ref, table_sem.at[0]),
        pltpu.make_async_copy(sin_in, sin_ref, table_sem.at[1]),
    ]
    for table in tables:
        table.start()
    for j in range(local_heads):
        for t in range(3):
            own_rows(t, j).start()
    pl.semaphore_wait(barrier, (n - 1) + (nx - 1) + (cores - 1) + (ways - 1))
    for j in range(local_heads):
        for t in range(3):
            for off in range(1, n):
                rows_to(t, j, off).start()
        if j == 0:
            for r in range(CHUNKS):
                for xo in range(1, nx):
                    weight_x(xo, r).start()
            if cores > 1:
                for r in range(CHUNKS):
                    for way in range(ways):
                        weight_core(0, r, way).start()

    lane = lax.broadcasted_iota(jnp.int32, (1, width), 1)
    low_map = lane < head_size
    low_half = lax.rem(lane, head_size) < head_size // 2

    def norm_rotate(block, gain):
        x = block.astype(jnp.float32)
        square = x * x
        low = jnp.sum(jnp.where(low_map, square, 0.0), axis=1, keepdims=True)
        high = jnp.sum(jnp.where(low_map, 0.0, square), axis=1, keepdims=True)
        low = lax.rsqrt(low * (1.0 / head_size) + EPSILON)
        high = lax.rsqrt(high * (1.0 / head_size) + EPSILON)
        y = x * jnp.where(low_map, low, high) * gain
        quarter = head_size // 2
        turned = jnp.where(low_half, pltpu.roll(y, width - quarter, 1), pltpu.roll(y, quarter, 1))
        return (y * cos_ref[...] + turned * sin_ref[...]).astype(jnp.bfloat16)

    def heads_to(j, i):
        column = pl.multiple_of(me * width, width)
        off = lax.rem(i + n - me, n)
        return pltpu.make_async_remote_copy(
            src_ref=heads_out.at[j, i], dst_ref=hrx.at[j, :, pl.ds(column, width)],
            send_sem=ret_send.at[j, off], recv_sem=ret_recv.at[j, off],
            device_id={"sp": i}, device_id_type=MESH,
        )

    def heads_from(j, off):
        peer = lax.rem(me + n - off, n)
        column = pl.multiple_of(peer * width, width)
        block = hrx.at[j, :, pl.ds(column, width)]
        return pltpu.make_async_remote_copy(
            src_ref=block, dst_ref=block, send_sem=ret_send.at[j, off],
            recv_sem=ret_recv.at[j, off], device_id={"sp": peer}, device_id_type=MESH,
        )

    groups = math.gcd(n, 4)
    per_group = n // groups
    segment = length // groups
    factor = head_size ** (-0.5) * math.log2(math.e)
    contract = (((1,), (1,)), ((), ()))

    def query_block(j, g, i, lam):
        rows = pl.ds(i * tok, tok) if isinstance(i, int) else pl.ds(pl.multiple_of(i * tok, tok), tok)
        q = rot_q[rows, :]
        zero = jnp.zeros_like(q)
        both = jnp.concatenate([jnp.where(low_map, q, zero), jnp.where(low_map, zero, q)], axis=0)
        start = g * segment
        spans = ([(0, start)] if g else []) + [(start, segment)]
        parts = []
        for first, size in spans:
            scores = lax.dot_general(
                both, rot_k[first : first + size, :], contract, preferred_element_type=jnp.float32
            )
            if first == start:
                shape = (2 * tok, size)
                row = lax.rem(lax.broadcasted_iota(jnp.int32, shape, 0), tok) + i * tok
                column = lax.broadcasted_iota(jnp.int32, shape, 1) + first
                scores = jnp.where(column <= row, scores, -1e30)
            parts.append(scores)
        top = functools.reduce(jnp.maximum, [jnp.max(s, axis=1, keepdims=True) for s in parts])
        parts = [jnp.exp2((s - top) * factor) for s in parts]
        total = functools.reduce(jnp.add, [jnp.sum(e, axis=1, keepdims=True) for e in parts])
        inverse = 1.0 / total
        one, two = inverse[:tok], inverse[tok:] * lam
        raw = None
        for (first, size), e in zip(spans, parts):
            mixing = (e[:tok] * one - e[tok:] * two).astype(jnp.bfloat16)
            term = jnp.dot(mixing, rx[2, j, first : first + size, :], preferred_element_type=jnp.float32)
            raw = term if raw is None else raw + term
        scaled = raw * lax.rsqrt(jnp.mean(raw * raw, axis=1, keepdims=True) + EPSILON)
        result = (scaled * hg_ref[...] * OUT_SCALE).astype(jnp.bfloat16)

        @pl.when(i == me)
        def _():
            hrx[j, :, pl.ds(pl.multiple_of(me * width, width), width)] = result

        @pl.when(i != me)
        def _():
            heads_out[j, i] = result
            heads_to(j, i).start()

    def forward(stage):
        if stage < CHUNKS:
            for xo in range(1, nx):
                weight_x_in(xo, stage).wait_recv()
                if ways > 1:
                    weight_y(xo, stage).start()
                if cores > 1:
                    weight_core(xo, stage, 0).start()
        elif ways > 1:
            for xo in range(1, nx):
                weight_y_in(xo, stage - CHUNKS).wait_recv()
                if cores > 1:
                    weight_core(xo, stage - CHUNKS, 1).start()

    for table in tables:
        table.wait()
    for j in range(local_heads):
        lam = lam_ref[me * local_heads + j]
        for t, (target, gain) in enumerate(((rot_k, kg_ref), (rot_q, qg_ref), (None, None))):
            own_rows(t, j).wait()
            for off in range(1, n):
                rows_from(t, j, off).wait_recv()
            if target is not None:
                target[...] = norm_rotate(rx[t, j], jnp.concatenate([gain[...]] * 2, axis=1))
        for g in range(groups):
            if per_group == 1:
                query_block(j, g, g, lam)
            else:
                def step(b, carry, j=j, g=g, lam=lam):
                    query_block(j, g, g * per_group + b, lam)
                    return carry
                lax.fori_loop(0, per_group, step, 0)
        for stage in range(2 * CHUNKS):
            if j == min(stage, local_heads - 1):
                forward(stage)

    own_weight.wait()
    if cores > 1:
        for xo in range(nx):
            for r in range(CHUNKS):
                for way in range(ways):
                    weight_core_in(xo, r, way).wait_recv()

    for j in range(local_heads):
        for off in range(1, n):
            heads_from(j, off).wait_recv()
        rows = hrx[j]
        for index in range(n_dp):
            matching = jnp.concatenate(
                [wfull[index, pl.ds((s * local_heads + j) * width, width), :] for s in range(n)], axis=0
            )
            term = jnp.dot(rows, matching, preferred_element_type=jnp.float32)
            span = slice(index * cols, (index + 1) * cols)
            if j:
                term = total[:, span] + term
            if j == local_heads - 1:
                out_ref[0, :, span] = term.astype(out_ref.dtype)
            else:
                total[:, span] = term

    for j in range(local_heads):
        for off in range(1, n):
            for t in range(3):
                rows_to(t, j, off).wait_send()
            heads_to(j, sp_peer(off)).wait_send()
    for r in range(CHUNKS):
        for xo in range(nx):
            if xo:
                weight_x(xo, r).wait_send()
                if ways > 1:
                    weight_y(xo, r).wait_send()
            if cores > 1:
                for way in range(ways):
                    weight_core(xo, r, way).wait_send()


def local(n, n_dp, n_grp, query_rows, key_rows, value_rows, query_gain, key_gain, lambdas, head_gain, out_weight):
    tok = query_rows.shape[1]
    head_size = query_gain.shape[0]
    width = head_gain.shape[0]
    local_heads = lambdas.shape[0] // n
    length = tok * n
    depth, cols = out_weight.shape
    cores = CORES if n_dp % CORES == 0 else 1
    nx = n_dp // cores
    cosine, sine = rotation_tables(length, head_size)
    anywhere = pl.BlockSpec(memory_space=pl.ANY)
    vmem = pl.BlockSpec(memory_space=pltpu.VMEM)
    dma = pltpu.SemaphoreType.DMA
    return pl.pallas_call(
        functools.partial(kernel, n, n_dp, n_grp, head_size),
        out_shape=jax.ShapeDtypeStruct((1, tok, n_dp * cols), jnp.bfloat16),
        in_specs=[anywhere] * 3
        + [vmem, vmem, pl.BlockSpec(memory_space=pltpu.SMEM), vmem, anywhere, anywhere, anywhere],
        out_specs=vmem,
        scratch_shapes=[
            pltpu.VMEM((tok, n_dp * cols), jnp.float32),
            pltpu.VMEM((3, local_heads, length, width), jnp.bfloat16),
            pltpu.VMEM((length, width), jnp.bfloat16),
            pltpu.VMEM((length, width), jnp.bfloat16),
            pltpu.VMEM((local_heads, n, tok, width), jnp.bfloat16),
            pltpu.VMEM((local_heads, tok, n * width), jnp.bfloat16),
            pltpu.VMEM((n_dp, depth, cols), jnp.bfloat16),
            dma((3, local_heads, n)),
            dma((3, local_heads, n)),
            dma((local_heads, n)),
            dma((local_heads, n)),
            dma((nx, CHUNKS)),
            dma((nx, CHUNKS)),
            dma((nx, CHUNKS)),
            dma((nx, CHUNKS)),
            dma((nx, CHUNKS, WAYS)),
            dma((nx, CHUNKS, WAYS)),
            dma(()),
            pltpu.VMEM((length, width), jnp.float32),
            pltpu.VMEM((length, width), jnp.float32),
            dma((2,)),
        ],
        compiler_params=pltpu.CompilerParams(
            collective_id=0, has_side_effects=True, vmem_limit_bytes=56 * 1024 * 1024
        ),
    )(
        query_rows, key_rows, value_rows,
        query_gain[None, :], key_gain[None, :], lambdas, head_gain[None, :],
        out_weight, jnp.asarray(cosine), jnp.asarray(sine),
    )


def split_kernel(
    n, n_dp, n_grp, head_size, chunks, q_in, k_in, v_in, qg_ref, kg_ref, lam_ref, hg_ref, w_ref, cos_in, sin_in,
    out_ref, total, rows_in, q_rot, k_rot, v_turn, big, small, big_out, small_out, kept, kept_top, gain_turn, heads, wfull,
    cos_ref, sin_ref, load_sem, big_send, big_recv, small_send, small_recv,
    wx_send, wx_recv, wy_send, wy_recv, wc_send, wc_recv,
):
    me = lax.axis_index("sp")
    dp = lax.axis_index("dp")
    ways = WAYS if n_grp == WAYS else 1
    grp = lax.axis_index("grp") if ways > 1 else 0
    cores = CORES if n_dp % CORES == 0 else 1
    nx = n_dp // cores
    xi, core = dp // cores, lax.rem(dp, cores)
    count, tok, width = q_rot.shape
    depth, cols = w_ref.shape
    piece = depth // (chunks * ways)
    factor = head_size ** (-0.5) * math.log2(math.e)

    def dp_index(xo, co):
        return lax.rem(xi + xo, nx) * cores + lax.rem(core + co, cores)

    barrier = pltpu.get_barrier_semaphore()
    for off in range(1, n):
        pl.semaphore_signal(barrier, inc=1, device_id={"sp": lax.rem(me + off, n)}, device_id_type=MESH)
    for xo in range(1, nx):
        pl.semaphore_signal(barrier, inc=1, device_id={"dp": dp_index(xo, 0)}, device_id_type=MESH)
    for co in range(1, cores):
        pl.semaphore_signal(barrier, inc=1, device_id={"dp": dp_index(0, co)}, device_id_type=MESH)
    if ways > 1:
        pl.semaphore_signal(barrier, inc=1, device_id={"grp": lax.rem(grp + 1, ways)}, device_id_type=MESH)

    own = pl.ds(pl.multiple_of(me * tok, tok), tok)
    loads = [
        pltpu.make_async_copy(q_in.at[0], rows_in.at[0], load_sem.at[0]),
        pltpu.make_async_copy(k_in.at[0], rows_in.at[1], load_sem.at[1]),
        pltpu.make_async_copy(v_in.at[0], rows_in.at[2], load_sem.at[2]),
        pltpu.make_async_copy(cos_in.at[own, :], cos_ref, load_sem.at[3]),
        pltpu.make_async_copy(sin_in.at[own, :], sin_ref, load_sem.at[4]),
    ]
    own_weight = pltpu.make_async_copy(w_ref, wfull.at[dp], load_sem.at[5])
    for load in loads:
        load.start()
    own_weight.start()

    def moved(source, target, send_sem, recv_sem, device):
        return pltpu.make_async_remote_copy(
            src_ref=source, dst_ref=target, send_sem=send_sem, recv_sem=recv_sem,
            device_id=device, device_id_type=MESH,
        )

    def piece_rows(r, way):
        first = (r * ways + lax.rem(grp + way, ways)) * piece
        return pl.ds(pl.multiple_of(first, piece), piece)

    def weight_x(xo, r):
        rows = piece_rows(r, 0)
        return moved(
            w_ref.at[rows, :], wfull.at[dp, rows, :], wx_send.at[xo, r], wx_recv.at[xo, r],
            {"dp": dp_index(xo, 0)},
        )

    def weight_x_in(xo, r):
        block = wfull.at[dp_index(nx - xo, 0), piece_rows(r, 0), :]
        return moved(block, block, wx_send.at[xo, r], wx_recv.at[xo, r], {"dp": dp_index(xo, 0)})

    def weight_y(xo, r):
        block = wfull.at[dp_index(nx - xo, 0), piece_rows(r, 0), :]
        return moved(block, block, wy_send.at[xo, r], wy_recv.at[xo, r], {"grp": lax.rem(grp + 1, ways)})

    def weight_y_in(xo, r):
        block = wfull.at[dp_index(nx - xo, 0), piece_rows(r, 1), :]
        return moved(block, block, wy_send.at[xo, r], wy_recv.at[xo, r], {"grp": lax.rem(grp + 1, ways)})

    def weight_core(xo, r, way):
        rows = piece_rows(r, way)
        target = wfull.at[dp_index(nx - xo, 0), rows, :]
        return moved(
            w_ref.at[rows, :] if xo == 0 else target, target,
            wc_send.at[xo, r, way], wc_recv.at[xo, r, way], {"dp": dp_index(0, 1)},
        )

    def weight_core_in(xo, r, way):
        block = wfull.at[dp_index(nx - xo, 1), piece_rows(r, way), :]
        return moved(block, block, wc_send.at[xo, r, way], wc_recv.at[xo, r, way], {"dp": dp_index(0, 1)})

    def forward_x(r):
        for xo in range(1, nx):
            weight_x_in(xo, r).wait_recv()
            if ways > 1:
                weight_y(xo, r).start()
            if cores > 1:
                weight_core(xo, r, 0).start()

    def forward_y(r):
        if ways > 1:
            for xo in range(1, nx):
                weight_y_in(xo, r).wait_recv()
                if cores > 1:
                    weight_core(xo, r, 1).start()

    def big_to(source, lane, slot, h, peer):
        return moved(source.at[h], big.at[slot, h], big_send.at[lane, h], big_recv.at[slot, h], {"sp": peer})

    def small_to(lane, slot, h, peer):
        return moved(
            small_out.at[lane, h], small.at[slot, h], small_send.at[lane, h], small_recv.at[slot, h], {"sp": peer}
        )

    def big_in(slot, h):
        block = big.at[slot, h]
        moved(block, block, big_send.at[0, h], big_recv.at[slot, h], {"sp": lax.rem(me + 1, n)}).wait_recv()

    def small_in(slot, h):
        block = small.at[slot, h]
        moved(block, block, small_send.at[0, h], small_recv.at[slot, h], {"sp": lax.rem(me + 1, n)}).wait_recv()

    pl.semaphore_wait(barrier, (n - 1) + (nx - 1) + (cores - 1) + (ways - 1))
    for r in range(chunks):
        for xo in range(1, nx):
            weight_x(xo, r).start()
    if cores > 1:
        for r in range(chunks):
            for way in range(ways):
                weight_core(0, r, way).start()

    lane = lax.broadcasted_iota(jnp.int32, (1, width), 1)
    low_map = lane < head_size
    low_half = lax.rem(lane, head_size) < head_size // 2

    def norm_rotate(block, gain):
        x = block.astype(jnp.float32)
        square = x * x
        low = jnp.sum(jnp.where(low_map, square, 0.0), axis=1, keepdims=True)
        high = jnp.sum(jnp.where(low_map, 0.0, square), axis=1, keepdims=True)
        low = lax.rsqrt(low * (1.0 / head_size) + EPSILON)
        high = lax.rsqrt(high * (1.0 / head_size) + EPSILON)
        y = x * jnp.where(low_map, low, high) * gain
        quarter = head_size // 2
        turned = jnp.where(low_half, pltpu.roll(y, width - quarter, 1), pltpu.roll(y, quarter, 1))
        return (y * cos_ref[...] + turned * sin_ref[...]).astype(jnp.bfloat16)

    for load in loads:
        load.wait()
    gain_turn[...] = jnp.broadcast_to(hg_ref[...], (tok, width)).T
    q_gain = jnp.concatenate([qg_ref[...]] * 2, axis=1)
    k_gain = jnp.concatenate([kg_ref[...]] * 2, axis=1)
    causal = lax.broadcasted_iota(jnp.int32, (tok, 2 * tok), 0) <= lax.rem(
        lax.broadcasted_iota(jnp.int32, (tok, 2 * tok), 1), tok
    )

    def head_columns(h):
        return pl.ds(pl.multiple_of(h * width, width), width)

    def turned_scores(keys, q):
        zero = jnp.zeros_like(q)
        both = jnp.concatenate([jnp.where(low_map, q, zero), jnp.where(low_map, zero, q)], axis=0)
        return lax.dot_general(keys, both, (((1,), (1,)), ((), ())), preferred_element_type=jnp.float32)

    def exponents(scores):
        top = jnp.max(scores, axis=0, keepdims=True)
        e = jnp.exp2((scores - top) * factor)
        return top * factor, e, jnp.sum(e, axis=0, keepdims=True)

    def mixed(e, scale, lam, values):
        one, two = scale[:, :tok], scale[:, tok:] * lam
        mixing = (e[:, :tok] * one - e[:, tok:] * two).astype(jnp.bfloat16)
        return jnp.dot(values, mixing, preferred_element_type=jnp.float32)

    def put_pair(ref, first, h, pair):
        ref[first, h, 0:1, :] = pair[:, :tok]
        ref[first, h, 1:2, :] = pair[:, tok:]

    def get_pair(ref, first, h):
        return jnp.concatenate([ref[first, h, 0:1, :], ref[first, h, 1:2, :]], axis=1)

    def joined(levels):
        top = functools.reduce(jnp.maximum, levels)
        return top + jnp.log2(functools.reduce(jnp.add, [jnp.exp2(l - top) for l in levels]))

    def finish(raw, h):
        scaled = raw * lax.rsqrt(jnp.mean(raw * raw, axis=0, keepdims=True) + EPSILON)
        result = (scaled * gain_turn[...] * OUT_SCALE).T
        heads[:, head_columns(h)] = result.astype(jnp.bfloat16)

    def partial_scores(keys, q, slot, h, masked):
        scores = turned_scores(keys, q)
        if masked:
            scores = jnp.where(causal, scores, -1e30)
        top, e, z = exponents(scores)
        kept[slot, h] = e
        put_pair(kept_top, slot, h, top)
        put_pair(small_out, slot, h, top + jnp.log2(z))

    def prepare(h, carry):
        span = head_columns(h)
        q_rot[h] = norm_rotate(rows_in[0, :, span], q_gain)

        @pl.when(me == 2)
        def _():
            big_to(q_rot, 0, 2, h, 1).start()

        @pl.when(me == 3)
        def _():
            big_to(q_rot, 1, 3, h, 2).start()
            big_to(q_rot, 0, 3, h, 1).start()

        k_rot[h] = norm_rotate(rows_in[1, :, span], k_gain)
        v_turn[h] = rows_in[2, :, span].astype(jnp.float32).T.astype(jnp.bfloat16)

        @pl.when(me == 0)
        def _():
            big_to(k_rot, 0, 0, h, 1).start()
            big_to(v_turn, 1, 1, h, 1).start()

        @pl.when(me >= 2)
        def _():
            partial_scores(k_rot[h], q_rot[h], 0, h, True)
            small_to(0, me - 2, h, 1).start()

        return carry

    lax.fori_loop(0, count, prepare, 0)

    def lowest(h):
        scores = jnp.where(causal, turned_scores(k_rot[h], q_rot[h]), -1e30)
        _, e, z = exponents(scores)
        finish(mixed(e, 1.0 / z, lam_ref[h], v_turn[h]), h)

    def centre_keys(h):
        return (
            jnp.concatenate([big[0, h], k_rot[h]], axis=0),
            jnp.concatenate([big[1, h], v_turn[h]], axis=1),
        )

    def served(h, slot, levels, keys, values):
        top, e, z = exponents(turned_scores(keys, big[slot, h]))
        level = joined([top + jnp.log2(z)] + levels)
        big_out[slot - 2, h] = mixed(e, jnp.exp2(top - level), lam_ref[h], values).astype(jnp.bfloat16)
        put_pair(small_out, slot - 2, h, level)

    def centre_second(h):
        big_in(0, h)
        big_in(1, h)
        big_in(2, h)
        small_in(0, h)
        keys, values = centre_keys(h)
        served(h, 2, [get_pair(small, 0, h)], keys, values)
        scores = turned_scores(keys, q_rot[h])
        scores = jnp.concatenate([scores[:tok], jnp.where(causal, scores[tok:], -1e30)], axis=0)
        _, e, z = exponents(scores)
        finish(mixed(e, 1.0 / z, lam_ref[h], values), h)
        big_to(big_out.at[0], 0, 0, h, 2).start()
        small_to(0, 0, h, 2).start()

    def centre_third(h):
        big_in(3, h)
        small_in(1, h)
        small_in(2, h)
        keys, values = centre_keys(h)
        served(h, 3, [get_pair(small, 1, h), get_pair(small, 2, h)], keys, values)
        small_to(1, 1, h, 2).start()
        big_to(big_out.at[1], 1, 0, h, 3).start()
        moved(
            small_out.at[1, h], small.at[1, h], small_send.at[2, h], small_recv.at[1, h], {"sp": 3}
        ).start()

    def upper_scores(h):
        big_in(3, h)
        partial_scores(k_rot[h], big[3, h], 1, h, False)
        small_to(1, 2, h, 1).start()

    def upper_raw(h, slot, level):
        scale = jnp.exp2(get_pair(kept_top, slot, h) - level)
        return mixed(kept[slot, h], scale, lam_ref[h], v_turn[h])

    def upper_help(h):
        small_in(1, h)
        big_out[1, h] = upper_raw(h, 1, get_pair(small, 1, h)).astype(jnp.bfloat16)
        big_to(big_out.at[1], 1, 1, h, 3).start()

    def upper_second(h):
        big_in(0, h)
        small_in(0, h)
        finish(upper_raw(h, 0, get_pair(small, 0, h)) + big[0, h].astype(jnp.float32), h)

    def upper_third(h):
        big_in(0, h)
        small_in(1, h)
        big_in(1, h)
        raw = upper_raw(h, 0, get_pair(small, 1, h)) + big[0, h].astype(jnp.float32)
        finish(raw + big[1, h].astype(jnp.float32), h)

    group = GROUP
    per_chunk = count // chunks

    def project(g, first, last):
        step = group * width
        rows = pl.ds(g * step, step) if isinstance(g, int) else pl.ds(pl.multiple_of(g * step, step), step)
        if cores > 1:
            for xo in range(nx):
                for r in range(group // per_chunk):
                    for way in range(ways):
                        weight_core_in(xo, g * (group // per_chunk) + r, way).wait_recv()
        block = heads[:, rows]
        for index in range(n_dp):
            term = jnp.dot(block, wfull[index, rows, :], preferred_element_type=jnp.float32)
            span = slice(index * cols, (index + 1) * cols)
            if not first:
                term = total[:, span] + term
            if last:
                out_ref[0, :, span] = term.astype(out_ref.dtype)
            else:
                total[:, span] = term

    groups = count // group
    late = 2 * group + 1

    def step(it, carry):
        @pl.when((me == 0) & (it < count))
        def _():
            lowest(it)

        @pl.when((me == 1) & (it < count))
        def _():
            centre_second(it)

        @pl.when((me == 1) & (it >= 1) & (it <= count))
        def _():
            centre_third(it - 1)

        @pl.when((me == 2) & (it < count))
        def _():
            upper_scores(it)

        @pl.when((me == 2) & (it >= LAG))
        def _():
            upper_help(it - LAG)
            upper_second(it - LAG)

        @pl.when((me == 3) & (it >= LAG))
        def _():
            upper_third(it - LAG)

        turn = lax.rem(it, per_chunk) == 0

        @pl.when(turn & (it >= per_chunk) & (it <= count))
        def _():
            forward_x(it // per_chunk - 1)

        first_y = 3 * per_chunk

        @pl.when(turn & (it >= first_y))
        def _():
            forward_y((it - first_y) // per_chunk)

        for g in range(groups - 1):
            @pl.when(it == g * group + late)
            def _(g=g):
                if g == 0:
                    own_weight.wait()
                project(g, g == 0, False)

        return carry

    steps = count + LAG
    lax.fori_loop(0, steps, step, 0)
    for r in range((steps - 1 - 3 * per_chunk) // per_chunk + 1, chunks):
        forward_y(r)
    project(groups - 1, False, True)

    def drain(h, carry):
        @pl.when(me == 0)
        def _():
            big_to(k_rot, 0, 0, h, 1).wait_send()
            big_to(v_turn, 1, 1, h, 1).wait_send()

        @pl.when(me == 1)
        def _():
            big_to(big_out.at[0], 0, 0, h, 2).wait_send()
            small_to(0, 0, h, 2).wait_send()
            small_to(1, 1, h, 2).wait_send()
            big_to(big_out.at[1], 1, 0, h, 3).wait_send()
            moved(
                small_out.at[1, h], small.at[1, h], small_send.at[2, h], small_recv.at[1, h], {"sp": 3}
            ).wait_send()

        @pl.when(me == 2)
        def _():
            big_to(q_rot, 0, 2, h, 1).wait_send()
            small_to(0, 0, h, 1).wait_send()
            small_to(1, 2, h, 1).wait_send()
            big_to(big_out.at[1], 1, 1, h, 3).wait_send()

        @pl.when(me == 3)
        def _():
            big_to(q_rot, 1, 3, h, 2).wait_send()
            big_to(q_rot, 0, 3, h, 1).wait_send()
            small_to(0, 1, h, 1).wait_send()

        return carry

    lax.fori_loop(0, count, drain, 0)

    def drain_weights(r, carry):
        for xo in range(nx):
            if xo:
                weight_x(xo, r).wait_send()
                if ways > 1:
                    weight_y(xo, r).wait_send()
            if cores > 1:
                for way in range(ways):
                    weight_core(xo, r, way).wait_send()
        return carry

    lax.fori_loop(0, chunks, drain_weights, 0)


def split_local(n, n_dp, n_grp, query_rows, key_rows, value_rows, query_gain, key_gain, lambdas, head_gain, out_weight):
    tok = query_rows.shape[1]
    head_size = query_gain.shape[0]
    width = head_gain.shape[0]
    count = lambdas.shape[0]
    depth, cols = out_weight.shape
    ways = WAYS if n_grp == WAYS else 1
    chunks = count // ways
    cores = CORES if n_dp % CORES == 0 else 1
    nx = n_dp // cores
    cosine, sine = rotation_tables(tok * n, head_size)
    anywhere = pl.BlockSpec(memory_space=pl.ANY)
    vmem = pl.BlockSpec(memory_space=pltpu.VMEM)
    dma = pltpu.SemaphoreType.DMA
    block = (count, tok, width)
    return pl.pallas_call(
        functools.partial(split_kernel, n, n_dp, n_grp, head_size, chunks),
        out_shape=jax.ShapeDtypeStruct((1, tok, n_dp * cols), jnp.bfloat16),
        in_specs=[anywhere] * 3
        + [vmem, vmem, pl.BlockSpec(memory_space=pltpu.SMEM), vmem, anywhere, anywhere, anywhere],
        out_specs=vmem,
        scratch_shapes=[
            pltpu.VMEM((tok, n_dp * cols), jnp.float32),
            pltpu.VMEM((3, tok, count * width), jnp.bfloat16),
            pltpu.VMEM(block, jnp.bfloat16),
            pltpu.VMEM(block, jnp.bfloat16),
            pltpu.VMEM(block, jnp.bfloat16),
            pltpu.VMEM((4,) + block, jnp.bfloat16),
            pltpu.VMEM((3, count, 2, tok), jnp.float32),
            pltpu.VMEM((2,) + block, jnp.bfloat16),
            pltpu.VMEM((2, count, 2, tok), jnp.float32),
            pltpu.VMEM((2, count, tok, 2 * tok), jnp.float32),
            pltpu.VMEM((2, count, 2, tok), jnp.float32),
            pltpu.VMEM((width, tok), jnp.float32),
            pltpu.VMEM((tok, count * width), jnp.bfloat16),
            pltpu.VMEM((n_dp, depth, cols), jnp.bfloat16),
            pltpu.VMEM((tok, width), jnp.float32),
            pltpu.VMEM((tok, width), jnp.float32),
            dma((6,)),
            dma((2, count)),
            dma((4, count)),
            dma((3, count)),
            dma((3, count)),
            dma((nx, chunks)),
            dma((nx, chunks)),
            dma((nx, chunks)),
            dma((nx, chunks)),
            dma((nx, chunks, ways)),
            dma((nx, chunks, ways)),
        ],
        compiler_params=pltpu.CompilerParams(
            collective_id=0, has_side_effects=True, vmem_limit_bytes=56 * 1024 * 1024
        ),
    )(
        query_rows, key_rows, value_rows,
        query_gain[None, :], key_gain[None, :], lambdas, head_gain[None, :],
        out_weight, jnp.asarray(cosine), jnp.asarray(sine),
    )


def plan(n, tok, width, count, n_grp):
    ways = WAYS if n_grp == WAYS else 1
    fits = n == PARTS and tok == width and count % (GROUP * ways) == 0
    return split_local if fits else local


def solution(mesh):
    rows = P(("grp", "dp"), "sp", None)
    n, n_dp, n_grp = mesh.shape["sp"], mesh.shape["dp"], mesh.shape["grp"]

    def body(*args):
        chosen = plan(n, args[0].shape[1], args[6].shape[0], args[5].shape[0], n_grp)
        return chosen(n, n_dp, n_grp, *args)

    return jax.shard_map(
        body,
        mesh=mesh,
        in_specs=(rows, rows, rows, P(), P(), P(), P(), P(None, "dp")),
        out_specs=rows,
        check_vma=False,
    )
```

```python
import functools
import math

import jax
import jax.numpy as jnp
import numpy as np
from jax import lax
from jax.experimental import pallas as pl
from jax.experimental.pallas import tpu as pltpu
from jax.sharding import PartitionSpec as P

EPSILON = 1e-06
OUT_SCALE = 0.8
CORES = 2
CHUNKS = 2
WAYS = 2
PARTS = 4
GROUP = 4
LAG = 5
AHEAD = 2
MESH = pl.DeviceIdType.MESH


def rotation_tables(length, head_size):
    half = head_size // 2
    inverse = np.float32(10000.0) ** (-np.arange(half, dtype=np.float32) / np.float32(half))
    angles = np.arange(length, dtype=np.float32)[:, None] * inverse.astype(np.float32)[None, :]
    cosine, sine = np.cos(angles), np.sin(angles)
    return (
        np.concatenate([cosine] * 4, axis=1).astype(np.float32),
        np.concatenate([-sine, sine] * 2, axis=1).astype(np.float32),
    )


def kernel(
    n, n_dp, n_grp, head_size, q_ref, k_ref, v_ref, qg_ref, kg_ref, lam_ref, hg_ref, w_ref, cos_in, sin_in,
    out_ref, total, rx, rot_q, rot_k, heads_out, hrx, wfull,
    in_send, in_recv, ret_send, ret_recv, wx_send, wx_recv, wy_send, wy_recv, wc_send, wc_recv, own_sem, cos_ref, sin_ref, table_sem,
):
    me = lax.axis_index("sp")
    dp = lax.axis_index("dp")
    ways = WAYS if n_grp == WAYS else 1
    grp = lax.axis_index("grp") if ways > 1 else 0
    cores = CORES if n_dp % CORES == 0 else 1
    nx = n_dp // cores
    xi, core = dp // cores, lax.rem(dp, cores)
    tok = q_ref.shape[1]
    width = 2 * head_size
    local_heads = rx.shape[1]
    length = rx.shape[2]
    depth = w_ref.shape[0]
    cols = w_ref.shape[1]
    piece = depth // (CHUNKS * ways)

    def sp_peer(off):
        return lax.rem(me + off, n)

    def dp_index(xo, co):
        return lax.rem(xi + xo, nx) * cores + lax.rem(core + co, cores)

    barrier = pltpu.get_barrier_semaphore()
    for off in range(1, n):
        pl.semaphore_signal(barrier, inc=1, device_id={"sp": sp_peer(off)}, device_id_type=MESH)
    for xo in range(1, nx):
        pl.semaphore_signal(barrier, inc=1, device_id={"dp": dp_index(xo, 0)}, device_id_type=MESH)
    for co in range(1, cores):
        pl.semaphore_signal(barrier, inc=1, device_id={"dp": dp_index(0, co)}, device_id_type=MESH)

    if ways > 1:
        pl.semaphore_signal(
            barrier, inc=1, device_id={"grp": lax.rem(grp + 1, ways)}, device_id_type=MESH
        )

    sources = (k_ref, q_ref, v_ref)

    def own_rows(t, j):
        column = pl.multiple_of((me * local_heads + j) * width, width)
        return pltpu.make_async_copy(
            sources[t].at[0, :, pl.ds(column, width)],
            rx.at[t, j, pl.ds(pl.multiple_of(me * tok, tok), tok), :],
            in_recv.at[t, j, 0],
        )

    def rows_to(t, j, off):
        peer = sp_peer(off)
        column = pl.multiple_of((peer * local_heads + j) * width, width)
        return pltpu.make_async_remote_copy(
            src_ref=sources[t].at[0, :, pl.ds(column, width)],
            dst_ref=rx.at[t, j, pl.ds(pl.multiple_of(me * tok, tok), tok), :],
            send_sem=in_send.at[t, j, off],
            recv_sem=in_recv.at[t, j, off],
            device_id={"sp": peer},
            device_id_type=MESH,
        )

    def rows_from(t, j, off):
        peer = lax.rem(me + n - off, n)
        block = rx.at[t, j, pl.ds(pl.multiple_of(peer * tok, tok), tok), :]
        return pltpu.make_async_remote_copy(
            src_ref=block, dst_ref=block, send_sem=in_send.at[t, j, off],
            recv_sem=in_recv.at[t, j, off], device_id={"sp": peer}, device_id_type=MESH,
        )

    def piece_rows(r, way):
        first = (r * ways + lax.rem(grp + way, ways)) * piece
        return pl.ds(pl.multiple_of(first, piece), piece)

    def moved(source, target, send_sem, recv_sem, device):
        return pltpu.make_async_remote_copy(
            src_ref=source, dst_ref=target, send_sem=send_sem, recv_sem=recv_sem,
            device_id=device, device_id_type=MESH,
        )

    def weight_x(xo, r):
        rows = piece_rows(r, 0)
        return moved(
            w_ref.at[rows, :], wfull.at[dp, rows, :], wx_send.at[xo, r], wx_recv.at[xo, r],
            {"dp": dp_index(xo, 0)},
        )

    def weight_x_in(xo, r):
        block = wfull.at[dp_index(nx - xo, 0), piece_rows(r, 0), :]
        return moved(block, block, wx_send.at[xo, r], wx_recv.at[xo, r], {"dp": dp_index(xo, 0)})

    def weight_y(xo, r):
        block = wfull.at[dp_index(nx - xo, 0), piece_rows(r, 0), :]
        return moved(block, block, wy_send.at[xo, r], wy_recv.at[xo, r], {"grp": lax.rem(grp + 1, ways)})

    def weight_y_in(xo, r):
        block = wfull.at[dp_index(nx - xo, 0), piece_rows(r, 1), :]
        return moved(block, block, wy_send.at[xo, r], wy_recv.at[xo, r], {"grp": lax.rem(grp + 1, ways)})

    def weight_core(xo, r, way):
        rows = piece_rows(r, way)
        target = wfull.at[dp_index(nx - xo, 0), rows, :]
        return moved(
            w_ref.at[rows, :] if xo == 0 else target, target,
            wc_send.at[xo, r, way], wc_recv.at[xo, r, way], {"dp": dp_index(0, 1)},
        )

    def weight_core_in(xo, r, way):
        block = wfull.at[dp_index(nx - xo, 1), piece_rows(r, way), :]
        return moved(
            block, block, wc_send.at[xo, r, way], wc_recv.at[xo, r, way], {"dp": dp_index(0, 1)}
        )

    own_weight = pltpu.make_async_copy(w_ref, wfull.at[dp], own_sem)
    own_weight.start()
    tables = [
        pltpu.make_async_copy(cos_in, cos_ref, table_sem.at[0]),
        pltpu.make_async_copy(sin_in, sin_ref, table_sem.at[1]),
    ]
    for table in tables:
        table.start()
    for j in range(local_heads):
        for t in range(3):
            own_rows(t, j).start()
    pl.semaphore_wait(barrier, (n - 1) + (nx - 1) + (cores - 1) + (ways - 1))
    for j in range(local_heads):
        for t in range(3):
            for off in range(1, n):
                rows_to(t, j, off).start()
        if j == 0:
            for r in range(CHUNKS):
                for xo in range(1, nx):
                    weight_x(xo, r).start()
            if cores > 1:
                for r in range(CHUNKS):
                    for way in range(ways):
                        weight_core(0, r, way).start()

    lane = lax.broadcasted_iota(jnp.int32, (1, width), 1)
    low_map = lane < head_size
    low_half = lax.rem(lane, head_size) < head_size // 2

    def norm_rotate(block, gain):
        x = block.astype(jnp.float32)
        square = x * x
        low = jnp.sum(jnp.where(low_map, square, 0.0), axis=1, keepdims=True)
        high = jnp.sum(jnp.where(low_map, 0.0, square), axis=1, keepdims=True)
        low = lax.rsqrt(low * (1.0 / head_size) + EPSILON)
        high = lax.rsqrt(high * (1.0 / head_size) + EPSILON)
        y = x * jnp.where(low_map, low, high) * gain
        quarter = head_size // 2
        turned = jnp.where(low_half, pltpu.roll(y, width - quarter, 1), pltpu.roll(y, quarter, 1))
        return (y * cos_ref[...] + turned * sin_ref[...]).astype(jnp.bfloat16)

    def heads_to(j, i):
        column = pl.multiple_of(me * width, width)
        off = lax.rem(i + n - me, n)
        return pltpu.make_async_remote_copy(
            src_ref=heads_out.at[j, i], dst_ref=hrx.at[j, :, pl.ds(column, width)],
            send_sem=ret_send.at[j, off], recv_sem=ret_recv.at[j, off],
            device_id={"sp": i}, device_id_type=MESH,
        )

    def heads_from(j, off):
        peer = lax.rem(me + n - off, n)
        column = pl.multiple_of(peer * width, width)
        block = hrx.at[j, :, pl.ds(column, width)]
        return pltpu.make_async_remote_copy(
            src_ref=block, dst_ref=block, send_sem=ret_send.at[j, off],
            recv_sem=ret_recv.at[j, off], device_id={"sp": peer}, device_id_type=MESH,
        )

    groups = math.gcd(n, 4)
    per_group = n // groups
    segment = length // groups
    factor = head_size ** (-0.5) * math.log2(math.e)
    contract = (((1,), (1,)), ((), ()))

    def query_block(j, g, i, lam):
        rows = pl.ds(i * tok, tok) if isinstance(i, int) else pl.ds(pl.multiple_of(i * tok, tok), tok)
        q = rot_q[rows, :]
        zero = jnp.zeros_like(q)
        both = jnp.concatenate([jnp.where(low_map, q, zero), jnp.where(low_map, zero, q)], axis=0)
        start = g * segment
        spans = ([(0, start)] if g else []) + [(start, segment)]
        parts = []
        for first, size in spans:
            scores = lax.dot_general(
                both, rot_k[first : first + size, :], contract, preferred_element_type=jnp.float32
            )
            if first == start:
                shape = (2 * tok, size)
                row = lax.rem(lax.broadcasted_iota(jnp.int32, shape, 0), tok) + i * tok
                column = lax.broadcasted_iota(jnp.int32, shape, 1) + first
                scores = jnp.where(column <= row, scores, -1e30)
            parts.append(scores)
        top = functools.reduce(jnp.maximum, [jnp.max(s, axis=1, keepdims=True) for s in parts])
        parts = [jnp.exp2((s - top) * factor) for s in parts]
        total = functools.reduce(jnp.add, [jnp.sum(e, axis=1, keepdims=True) for e in parts])
        inverse = 1.0 / total
        one, two = inverse[:tok], inverse[tok:] * lam
        raw = None
        for (first, size), e in zip(spans, parts):
            mixing = (e[:tok] * one - e[tok:] * two).astype(jnp.bfloat16)
            term = jnp.dot(mixing, rx[2, j, first : first + size, :], preferred_element_type=jnp.float32)
            raw = term if raw is None else raw + term
        scaled = raw * lax.rsqrt(jnp.mean(raw * raw, axis=1, keepdims=True) + EPSILON)
        result = (scaled * hg_ref[...] * OUT_SCALE).astype(jnp.bfloat16)

        @pl.when(i == me)
        def _():
            hrx[j, :, pl.ds(pl.multiple_of(me * width, width), width)] = result

        @pl.when(i != me)
        def _():
            heads_out[j, i] = result
            heads_to(j, i).start()

    def forward(stage):
        if stage < CHUNKS:
            for xo in range(1, nx):
                weight_x_in(xo, stage).wait_recv()
                if ways > 1:
                    weight_y(xo, stage).start()
                if cores > 1:
                    weight_core(xo, stage, 0).start()
        elif ways > 1:
            for xo in range(1, nx):
                weight_y_in(xo, stage - CHUNKS).wait_recv()
                if cores > 1:
                    weight_core(xo, stage - CHUNKS, 1).start()

    for table in tables:
        table.wait()
    for j in range(local_heads):
        lam = lam_ref[me * local_heads + j]
        for t, (target, gain) in enumerate(((rot_k, kg_ref), (rot_q, qg_ref), (None, None))):
            own_rows(t, j).wait()
            for off in range(1, n):
                rows_from(t, j, off).wait_recv()
            if target is not None:
                target[...] = norm_rotate(rx[t, j], jnp.concatenate([gain[...]] * 2, axis=1))
        for g in range(groups):
            if per_group == 1:
                query_block(j, g, g, lam)
            else:
                def step(b, carry, j=j, g=g, lam=lam):
                    query_block(j, g, g * per_group + b, lam)
                    return carry
                lax.fori_loop(0, per_group, step, 0)
        for stage in range(2 * CHUNKS):
            if j == min(stage, local_heads - 1):
                forward(stage)

    own_weight.wait()
    if cores > 1:
        for xo in range(nx):
            for r in range(CHUNKS):
                for way in range(ways):
                    weight_core_in(xo, r, way).wait_recv()

    for j in range(local_heads):
        for off in range(1, n):
            heads_from(j, off).wait_recv()
        rows = hrx[j]
        for index in range(n_dp):
            matching = jnp.concatenate(
                [wfull[index, pl.ds((s * local_heads + j) * width, width), :] for s in range(n)], axis=0
            )
            term = jnp.dot(rows, matching, preferred_element_type=jnp.float32)
            span = slice(index * cols, (index + 1) * cols)
            if j:
                term = total[:, span] + term
            if j == local_heads - 1:
                out_ref[0, :, span] = term.astype(out_ref.dtype)
            else:
                total[:, span] = term

    for j in range(local_heads):
        for off in range(1, n):
            for t in range(3):
                rows_to(t, j, off).wait_send()
            heads_to(j, sp_peer(off)).wait_send()
    for r in range(CHUNKS):
        for xo in range(nx):
            if xo:
                weight_x(xo, r).wait_send()
                if ways > 1:
                    weight_y(xo, r).wait_send()
            if cores > 1:
                for way in range(ways):
                    weight_core(xo, r, way).wait_send()


def local(n, n_dp, n_grp, query_rows, key_rows, value_rows, query_gain, key_gain, lambdas, head_gain, out_weight):
    tok = query_rows.shape[1]
    head_size = query_gain.shape[0]
    width = head_gain.shape[0]
    local_heads = lambdas.shape[0] // n
    length = tok * n
    depth, cols = out_weight.shape
    cores = CORES if n_dp % CORES == 0 else 1
    nx = n_dp // cores
    cosine, sine = rotation_tables(length, head_size)
    anywhere = pl.BlockSpec(memory_space=pl.ANY)
    vmem = pl.BlockSpec(memory_space=pltpu.VMEM)
    dma = pltpu.SemaphoreType.DMA
    return pl.pallas_call(
        functools.partial(kernel, n, n_dp, n_grp, head_size),
        out_shape=jax.ShapeDtypeStruct((1, tok, n_dp * cols), jnp.bfloat16),
        in_specs=[anywhere] * 3
        + [vmem, vmem, pl.BlockSpec(memory_space=pltpu.SMEM), vmem, anywhere, anywhere, anywhere],
        out_specs=vmem,
        scratch_shapes=[
            pltpu.VMEM((tok, n_dp * cols), jnp.float32),
            pltpu.VMEM((3, local_heads, length, width), jnp.bfloat16),
            pltpu.VMEM((length, width), jnp.bfloat16),
            pltpu.VMEM((length, width), jnp.bfloat16),
            pltpu.VMEM((local_heads, n, tok, width), jnp.bfloat16),
            pltpu.VMEM((local_heads, tok, n * width), jnp.bfloat16),
            pltpu.VMEM((n_dp, depth, cols), jnp.bfloat16),
            dma((3, local_heads, n)),
            dma((3, local_heads, n)),
            dma((local_heads, n)),
            dma((local_heads, n)),
            dma((nx, CHUNKS)),
            dma((nx, CHUNKS)),
            dma((nx, CHUNKS)),
            dma((nx, CHUNKS)),
            dma((nx, CHUNKS, WAYS)),
            dma((nx, CHUNKS, WAYS)),
            dma(()),
            pltpu.VMEM((length, width), jnp.float32),
            pltpu.VMEM((length, width), jnp.float32),
            dma((2,)),
        ],
        compiler_params=pltpu.CompilerParams(
            collective_id=0, has_side_effects=True, vmem_limit_bytes=56 * 1024 * 1024
        ),
    )(
        query_rows, key_rows, value_rows,
        query_gain[None, :], key_gain[None, :], lambdas, head_gain[None, :],
        out_weight, jnp.asarray(cosine), jnp.asarray(sine),
    )


def split_kernel(
    n, n_dp, n_grp, head_size, chunks, q_in, k_in, v_in, qg_ref, kg_ref, lam_ref, hg_ref, w_ref, cos_in, sin_in,
    out_ref, total, rows_in, q_rot, k_rot, v_turn, big, small, big_out, small_out, kept, kept_top, gain_turn, heads, wfull,
    cos_ref, sin_ref, turn_ref, out_rows, load_sem, out_sem, big_send, big_recv, small_send, small_recv,
    wx_send, wx_recv, wy_send, wy_recv, wc_send, wc_recv,
):
    me = lax.axis_index("sp")
    dp = lax.axis_index("dp")
    ways = WAYS if n_grp == WAYS else 1
    grp = lax.axis_index("grp") if ways > 1 else 0
    cores = CORES if n_dp % CORES == 0 else 1
    nx = n_dp // cores
    xi, core = dp // cores, lax.rem(dp, cores)
    count, tok, width = q_rot.shape
    depth, cols = w_ref.shape
    piece = depth // (chunks * ways)
    factor = head_size ** (-0.5) * math.log2(math.e)

    def dp_index(xo, co):
        return lax.rem(xi + xo, nx) * cores + lax.rem(core + co, cores)

    barrier = pltpu.get_barrier_semaphore()
    for off in range(1, n):
        pl.semaphore_signal(barrier, inc=1, device_id={"sp": lax.rem(me + off, n)}, device_id_type=MESH)
    for xo in range(1, nx):
        pl.semaphore_signal(barrier, inc=1, device_id={"dp": dp_index(xo, 0)}, device_id_type=MESH)
    for co in range(1, cores):
        pl.semaphore_signal(barrier, inc=1, device_id={"dp": dp_index(0, co)}, device_id_type=MESH)
    if ways > 1:
        pl.semaphore_signal(barrier, inc=1, device_id={"grp": lax.rem(grp + 1, ways)}, device_id_type=MESH)

    own = pl.ds(pl.multiple_of(me * tok, tok), tok)
    loads = [
        pltpu.make_async_copy(q_in.at[0], rows_in.at[0], load_sem.at[0]),
        pltpu.make_async_copy(k_in.at[0], rows_in.at[1], load_sem.at[1]),
        pltpu.make_async_copy(v_in.at[0], rows_in.at[2], load_sem.at[2]),
        pltpu.make_async_copy(cos_in.at[own, :], cos_ref, load_sem.at[3]),
        pltpu.make_async_copy(sin_in.at[own, :], sin_ref, load_sem.at[4]),
    ]
    own_weight = pltpu.make_async_copy(w_ref, wfull.at[dp], load_sem.at[5])
    for load in loads:
        load.start()
    own_weight.start()

    def moved(source, target, send_sem, recv_sem, device):
        return pltpu.make_async_remote_copy(
            src_ref=source, dst_ref=target, send_sem=send_sem, recv_sem=recv_sem,
            device_id=device, device_id_type=MESH,
        )

    def piece_rows(r, way):
        first = (r * ways + lax.rem(grp + way, ways)) * piece
        return pl.ds(pl.multiple_of(first, piece), piece)

    def weight_x(xo, r):
        rows = piece_rows(r, 0)
        return moved(
            w_ref.at[rows, :], wfull.at[dp, rows, :], wx_send.at[xo, r], wx_recv.at[xo, r],
            {"dp": dp_index(xo, 0)},
        )

    def weight_x_in(xo, r):
        block = wfull.at[dp_index(nx - xo, 0), piece_rows(r, 0), :]
        return moved(block, block, wx_send.at[xo, r], wx_recv.at[xo, r], {"dp": dp_index(xo, 0)})

    def weight_y(xo, r):
        block = wfull.at[dp_index(nx - xo, 0), piece_rows(r, 0), :]
        return moved(block, block, wy_send.at[xo, r], wy_recv.at[xo, r], {"grp": lax.rem(grp + 1, ways)})

    def weight_y_in(xo, r):
        block = wfull.at[dp_index(nx - xo, 0), piece_rows(r, 1), :]
        return moved(block, block, wy_send.at[xo, r], wy_recv.at[xo, r], {"grp": lax.rem(grp + 1, ways)})

    def weight_core(xo, r, way):
        rows = piece_rows(r, way)
        target = wfull.at[dp_index(nx - xo, 0), rows, :]
        return moved(
            w_ref.at[rows, :] if xo == 0 else target, target,
            wc_send.at[xo, r, way], wc_recv.at[xo, r, way], {"dp": dp_index(0, 1)},
        )

    def weight_core_in(xo, r, way):
        block = wfull.at[dp_index(nx - xo, 1), piece_rows(r, way), :]
        return moved(block, block, wc_send.at[xo, r, way], wc_recv.at[xo, r, way], {"dp": dp_index(0, 1)})

    def forward_x(r):
        for xo in range(1, nx):
            weight_x_in(xo, r).wait_recv()
            if ways > 1:
                weight_y(xo, r).start()
            if cores > 1:
                weight_core(xo, r, 0).start()

    def forward_y(r):
        if ways > 1:
            for xo in range(1, nx):
                weight_y_in(xo, r).wait_recv()
                if cores > 1:
                    weight_core(xo, r, 1).start()

    def big_to(source, lane, slot, h, peer):
        return moved(source.at[h], big.at[slot, h], big_send.at[lane, h], big_recv.at[slot, h], {"sp": peer})

    def small_to(lane, slot, h, peer):
        return moved(
            small_out.at[lane, h], small.at[slot, h], small_send.at[lane, h], small_recv.at[slot, h], {"sp": peer}
        )

    def big_in(slot, h):
        block = big.at[slot, h]
        moved(block, block, big_send.at[0, h], big_recv.at[slot, h], {"sp": lax.rem(me + 1, n)}).wait_recv()

    def small_in(slot, h):
        block = small.at[slot, h]
        moved(block, block, small_send.at[0, h], small_recv.at[slot, h], {"sp": lax.rem(me + 1, n)}).wait_recv()

    pl.semaphore_wait(barrier, (n - 1) + (nx - 1) + (cores - 1) + (ways - 1))
    for r in range(chunks):
        for xo in range(1, nx):
            weight_x(xo, r).start()
    if cores > 1:
        for r in range(chunks):
            for way in range(ways):
                weight_core(0, r, way).start()

    lane = lax.broadcasted_iota(jnp.int32, (1, width), 1)
    low_map = lane < head_size
    half = head_size // 2
    down, across = (lax.broadcasted_iota(jnp.int32, (width, width), axis) for axis in range(2))
    partner = jnp.where(lax.rem(across, head_size) < half, across + half, across - half)
    swap = jnp.where(down == partner, 1.0, 0.0).astype(jnp.bfloat16)
    same_map = jnp.where((down < head_size) == (across < head_size), 1.0, 0.0).astype(jnp.bfloat16)
    sums = jnp.concatenate([same_map, same_map], axis=0)

    def norm_rotate(which, target, first):
        blocks = [rows_in[which, :, head_columns(first + i)] for i in range(GROUP)]
        stacked = jnp.concatenate(blocks, axis=0)
        x = stacked.astype(jnp.float32)
        square = x * x
        coarse = square.astype(jnp.bfloat16)
        fine = (square - coarse.astype(jnp.float32)).astype(jnp.bfloat16)
        total_square = jnp.dot(jnp.concatenate([coarse, fine], axis=1), sums, preferred_element_type=jnp.float32)
        other = jnp.dot(stacked, swap, preferred_element_type=jnp.float32)
        inverse = lax.rsqrt(total_square * (1.0 / head_size) + EPSILON)
        for i in range(GROUP):
            part = slice(i * tok, (i + 1) * tok)
            straight = x[part] * inverse[part] * turn_ref[2 * which]
            turned = other[part] * inverse[part] * turn_ref[2 * which + 1]
            target[first + i] = (straight + turned).astype(jnp.bfloat16)

    for load in loads:
        load.wait()
    gain_turn[...] = jnp.broadcast_to(hg_ref[...], (tok, width)).T
    for which, gain in enumerate((qg_ref, kg_ref)):
        gain = gain[...]
        crossed = jnp.concatenate([gain[:, half:], gain[:, :half]], axis=1)
        turn_ref[2 * which] = cos_ref[...] * jnp.concatenate([gain, gain], axis=1)
        turn_ref[2 * which + 1] = sin_ref[...] * jnp.concatenate([crossed, crossed], axis=1)
    causal = lax.broadcasted_iota(jnp.int32, (tok, 2 * tok), 0) <= lax.rem(
        lax.broadcasted_iota(jnp.int32, (tok, 2 * tok), 1), tok
    )

    def head_columns(h):
        return pl.ds(pl.multiple_of(h * width, width), width)

    def turned_scores(keys, *queries):
        both = []
        for q in queries:
            zero = jnp.zeros_like(q)
            both += [jnp.where(low_map, q, zero), jnp.where(low_map, zero, q)]
        both = jnp.concatenate(both, axis=0)
        return lax.dot_general(keys, both, (((1,), (1,)), ((), ())), preferred_element_type=jnp.float32)

    def exponents(scores):
        top = jnp.max(scores, axis=0, keepdims=True)
        e = jnp.exp2((scores - top) * factor)
        return top * factor, e, jnp.sum(e, axis=0, keepdims=True)

    def mixing_of(e, scale, lam):
        one, two = scale[:, :tok], scale[:, tok:] * lam
        return (e[:, :tok] * one - e[:, tok:] * two).astype(jnp.bfloat16)

    def mixed(e, scale, lam, values):
        return jnp.dot(values, mixing_of(e, scale, lam), preferred_element_type=jnp.float32)

    def put_pair(ref, first, h, pair):
        ref[first, h, 0:1, :] = pair[:, :tok]
        ref[first, h, 1:2, :] = pair[:, tok:]

    def get_pair(ref, first, h):
        return jnp.concatenate([ref[first, h, 0:1, :], ref[first, h, 1:2, :]], axis=1)

    def joined(levels):
        top = functools.reduce(jnp.maximum, levels)
        return top + jnp.log2(functools.reduce(jnp.add, [jnp.exp2(l - top) for l in levels]))

    def finish(raw, h):
        scaled = raw * lax.rsqrt(jnp.mean(raw * raw, axis=0, keepdims=True) + EPSILON)
        result = (scaled * gain_turn[...] * OUT_SCALE).T
        heads[:, head_columns(h)] = result.astype(jnp.bfloat16)

    def partial_scores(keys, queries, slot, first, masked):
        scores = [turned_scores(k, q) for k, q in zip(keys, queries)]
        if masked:
            scores = [jnp.where(causal, s, -1e30) for s in scores]
        parts = [exponents(s) for s in scores]
        for i, (top, e, z) in enumerate(parts):
            kept[slot, first + i] = e
            put_pair(kept_top, slot, first + i, top)
            put_pair(small_out, slot, first + i, top + jnp.log2(z))

    def prepare(j, carry):
        first = j * GROUP
        norm_rotate(0, q_rot, first)

        @pl.when(me == 3)
        def _():
            for i in range(GROUP):
                big_to(q_rot, 1, 3, first + i, 2).start()
                big_to(q_rot, 0, 3, first + i, 1).start()

        @pl.when((me == 2) & (j == 0))
        def _():
            for i in range(AHEAD):
                big_to(q_rot, 0, 2, i, 1).start()

        norm_rotate(1, k_rot, first)
        for i in range(GROUP):
            v_turn[first + i] = rows_in[2, :, head_columns(first + i)].astype(jnp.float32).T.astype(jnp.bfloat16)

        @pl.when(me == 0)
        def _():
            for i in range(GROUP):
                big_to(k_rot, 0, 0, first + i, 1).start()
                big_to(v_turn, 1, 1, first + i, 1).start()

        @pl.when(me >= 2)
        def _():
            heads_of = range(GROUP)
            partial_scores(
                [k_rot[first + i] for i in heads_of], [q_rot[first + i] for i in heads_of], 0, first, True
            )
            for i in heads_of:
                small_to(0, me - 2, first + i, 1).start()

        return carry

    lax.fori_loop(0, count // GROUP, prepare, 0)

    def lowest(h):
        scores = jnp.where(causal, turned_scores(k_rot[h], q_rot[h]), -1e30)
        _, e, z = exponents(scores)
        finish(mixed(e, 1.0 / z, lam_ref[h], v_turn[h]), h)

    def centre(h):
        for slot in range(4):
            big_in(slot, h)
        for slot in range(3):
            small_in(slot, h)
        keys = jnp.concatenate([big[0, h], k_rot[h]], axis=0)
        values = jnp.concatenate([big[1, h], v_turn[h]], axis=1)
        second, third, third_too = (get_pair(small, slot, h) for slot in range(3))
        lam = lam_ref[h]
        pair = 2 * tok
        scores = turned_scores(keys, q_rot[h], big[2, h], big[3, h])
        seen = jnp.concatenate([scores[:tok, :pair], jnp.where(causal, scores[tok:, :pair], -1e30)], axis=0)
        scores = jnp.concatenate([seen, scores[:, pair:]], axis=1)
        top, e, z = exponents(scores)
        level = top + jnp.log2(z)
        level_two = joined([level[:, pair : 2 * pair], second])
        level_three = joined([level[:, 2 * pair :], third, third_too])
        put_pair(small_out, 0, h, level_two)
        put_pair(small_out, 1, h, level_three)
        scales = [
            1.0 / z[:, :pair],
            jnp.exp2(top[:, pair : 2 * pair] - level_two),
            jnp.exp2(top[:, 2 * pair :] - level_three),
        ]
        mixing = [mixing_of(e[:, i * pair : (i + 1) * pair], scale, lam) for i, scale in enumerate(scales)]
        raw = jnp.dot(values, jnp.concatenate(mixing, axis=1), preferred_element_type=jnp.float32)
        big_out[1, h] = raw[:, 2 * tok :].astype(jnp.bfloat16)
        big_out[0, h] = raw[:, tok : 2 * tok].astype(jnp.bfloat16)
        small_to(1, 1, h, 2).start()
        last_level(h).start()
        big_to(big_out.at[1], 1, 0, h, 3).start()
        small_to(0, 0, h, 2).start()
        big_to(big_out.at[0], 0, 0, h, 2).start()
        finish(raw[:, :tok], h)

    def last_level(h):
        return moved(
            small_out.at[1, h], small.at[1, h], small_send.at[2, h], small_recv.at[1, h], {"sp": 3}
        )

    def upper_scores(h):
        big_in(3, h)
        partial_scores([k_rot[h]], [big[3, h]], 1, h, False)
        small_to(1, 2, h, 1).start()

        @pl.when(h + AHEAD < count)
        def _():
            big_to(q_rot, 0, 2, h + AHEAD, 1).start()

    def upper_raw(h, slot, level):
        scale = jnp.exp2(get_pair(kept_top, slot, h) - level)
        return mixed(kept[slot, h], scale, lam_ref[h], v_turn[h])

    def upper_help(h):
        small_in(1, h)
        big_out[1, h] = upper_raw(h, 1, get_pair(small, 1, h)).astype(jnp.bfloat16)
        big_to(big_out.at[1], 1, 1, h, 3).start()

    def upper_second(h):
        big_in(0, h)
        small_in(0, h)
        finish(upper_raw(h, 0, get_pair(small, 0, h)) + big[0, h].astype(jnp.float32), h)

    def upper_third(h):
        big_in(0, h)
        small_in(1, h)
        big_in(1, h)
        raw = upper_raw(h, 0, get_pair(small, 1, h)) + big[0, h].astype(jnp.float32)
        finish(raw + big[1, h].astype(jnp.float32), h)

    group = GROUP
    per_chunk = count // chunks

    def leave(index):
        span = slice(index * cols, (index + 1) * cols)
        return pltpu.make_async_copy(out_rows.at[:, span], out_ref.at[0, :, span], out_sem.at[index])

    def project(g, first, last):
        step = group * width
        rows = pl.ds(g * step, step) if isinstance(g, int) else pl.ds(pl.multiple_of(g * step, step), step)
        if cores > 1:
            for xo in range(nx):
                for r in range(group // per_chunk):
                    for way in range(ways):
                        weight_core_in(xo, g * (group // per_chunk) + r, way).wait_recv()
        block = heads[:, rows]
        for index in range(n_dp):
            term = jnp.dot(block, wfull[index, rows, :], preferred_element_type=jnp.float32)
            span = slice(index * cols, (index + 1) * cols)
            if not first:
                term = total[:, span] + term
            if last:
                out_rows[:, span] = term.astype(out_ref.dtype)
                leave(index).start()
            else:
                total[:, span] = term

    groups = count // group

    def sent(h):
        @pl.when(me == 0)
        def _():
            big_to(k_rot, 0, 0, h, 1).wait_send()
            big_to(v_turn, 1, 1, h, 1).wait_send()

        @pl.when(me == 1)
        def _():
            big_to(big_out.at[0], 0, 0, h, 2).wait_send()
            big_to(big_out.at[1], 1, 0, h, 3).wait_send()
            small_to(0, 0, h, 2).wait_send()
            small_to(1, 1, h, 2).wait_send()
            last_level(h).wait_send()

        @pl.when(me == 2)
        def _():
            big_to(q_rot, 0, 2, h, 1).wait_send()
            small_to(0, 0, h, 1).wait_send()
            small_to(1, 2, h, 1).wait_send()

        @pl.when(me == 3)
        def _():
            big_to(q_rot, 1, 3, h, 2).wait_send()
            big_to(q_rot, 0, 3, h, 1).wait_send()
            small_to(0, 1, h, 1).wait_send()

    first_y = 2 * per_chunk

    def step(it, carry):
        @pl.when((me == 0) & (it < count))
        def _():
            lowest(it)

        @pl.when((me == 1) & (it < count))
        def _():
            centre(it)

        @pl.when((me == 2) & (it < count))
        def _():
            upper_scores(it)

        turn = lax.rem(it, per_chunk) == 0

        @pl.when(turn & (it < count))
        def _():
            forward_x(it // per_chunk)

        @pl.when(turn & (it >= first_y) & (it < first_y + count))
        def _():
            forward_y((it - first_y) // per_chunk)

        @pl.when((me == 2) & (it >= LAG))
        def _():
            upper_help(it - LAG)
            upper_second(it - LAG)

        @pl.when((me == 3) & (it >= LAG))
        def _():
            upper_third(it - LAG)

        @pl.when(it >= LAG)
        def _():
            sent(it - LAG)

        for g in range(groups - 1):
            @pl.when(it == (g + 1) * group - 1 + LAG)
            def _(g=g):
                if g == 0:
                    own_weight.wait()
                project(g, g == 0, False)

        return carry

    lax.fori_loop(0, count + LAG, step, 0)
    project(groups - 1, False, True)

    def drain(h, carry):
        @pl.when(me == 2)
        def _():
            big_to(big_out.at[1], 1, 1, h, 3).wait_send()

        return carry

    lax.fori_loop(0, count, drain, 0)

    def drain_weights(r, carry):
        for xo in range(nx):
            if xo:
                weight_x(xo, r).wait_send()
                if ways > 1:
                    weight_y(xo, r).wait_send()
            if cores > 1:
                for way in range(ways):
                    weight_core(xo, r, way).wait_send()
        return carry

    lax.fori_loop(0, chunks, drain_weights, 0)
    for index in range(n_dp):
        leave(index).wait()


def split_local(n, n_dp, n_grp, query_rows, key_rows, value_rows, query_gain, key_gain, lambdas, head_gain, out_weight):
    tok = query_rows.shape[1]
    head_size = query_gain.shape[0]
    width = head_gain.shape[0]
    count = lambdas.shape[0]
    depth, cols = out_weight.shape
    ways = WAYS if n_grp == WAYS else 1
    chunks = count // ways
    cores = CORES if n_dp % CORES == 0 else 1
    nx = n_dp // cores
    cosine, sine = rotation_tables(tok * n, head_size)
    anywhere = pl.BlockSpec(memory_space=pl.ANY)
    vmem = pl.BlockSpec(memory_space=pltpu.VMEM)
    dma = pltpu.SemaphoreType.DMA
    block = (count, tok, width)
    return pl.pallas_call(
        functools.partial(split_kernel, n, n_dp, n_grp, head_size, chunks),
        out_shape=jax.ShapeDtypeStruct((1, tok, n_dp * cols), jnp.bfloat16),
        in_specs=[anywhere] * 3
        + [vmem, vmem, pl.BlockSpec(memory_space=pltpu.SMEM), vmem, anywhere, anywhere, anywhere],
        out_specs=anywhere,
        scratch_shapes=[
            pltpu.VMEM((tok, n_dp * cols), jnp.float32),
            pltpu.VMEM((3, tok, count * width), jnp.bfloat16),
            pltpu.VMEM(block, jnp.bfloat16),
            pltpu.VMEM(block, jnp.bfloat16),
            pltpu.VMEM(block, jnp.bfloat16),
            pltpu.VMEM((4,) + block, jnp.bfloat16),
            pltpu.VMEM((3, count, 2, tok), jnp.float32),
            pltpu.VMEM((2,) + block, jnp.bfloat16),
            pltpu.VMEM((2, count, 2, tok), jnp.float32),
            pltpu.VMEM((2, count, tok, 2 * tok), jnp.float32),
            pltpu.VMEM((2, count, 2, tok), jnp.float32),
            pltpu.VMEM((width, tok), jnp.float32),
            pltpu.VMEM((tok, count * width), jnp.bfloat16),
            pltpu.VMEM((n_dp, depth, cols), jnp.bfloat16),
            pltpu.VMEM((tok, width), jnp.float32),
            pltpu.VMEM((tok, width), jnp.float32),
            pltpu.VMEM((4, tok, width), jnp.float32),
            pltpu.VMEM((tok, n_dp * cols), jnp.bfloat16),
            dma((6,)),
            dma((n_dp,)),
            dma((2, count)),
            dma((4, count)),
            dma((3, count)),
            dma((3, count)),
            dma((nx, chunks)),
            dma((nx, chunks)),
            dma((nx, chunks)),
            dma((nx, chunks)),
            dma((nx, chunks, ways)),
            dma((nx, chunks, ways)),
        ],
        compiler_params=pltpu.CompilerParams(
            collective_id=0, has_side_effects=True, vmem_limit_bytes=56 * 1024 * 1024
        ),
    )(
        query_rows, key_rows, value_rows,
        query_gain[None, :], key_gain[None, :], lambdas, head_gain[None, :],
        out_weight, jnp.asarray(cosine), jnp.asarray(sine),
    )


def plan(n, tok, width, count, n_grp):
    ways = WAYS if n_grp == WAYS else 1
    fits = n == PARTS and tok == width and count % (GROUP * ways) == 0
    return split_local if fits else local


def solution(mesh):
    rows = P(("grp", "dp"), "sp", None)
    n, n_dp, n_grp = mesh.shape["sp"], mesh.shape["dp"], mesh.shape["grp"]

    def body(*args):
        chosen = plan(n, args[0].shape[1], args[6].shape[0], args[5].shape[0], n_grp)
        return chosen(n, n_dp, n_grp, *args)

    return jax.shard_map(
        body,
        mesh=mesh,
        in_specs=(rows, rows, rows, P(), P(), P(), P(), P(None, "dp")),
        out_specs=rows,
        check_vma=False,
    )
```

```python
import functools
import math

import jax
import jax.numpy as jnp
import numpy as np
from jax import lax
from jax.experimental import pallas as pl
from jax.experimental.pallas import tpu as pltpu
from jax.sharding import PartitionSpec as P

EPSILON = 1e-06
OUT_SCALE = 0.8
CORES = 2
CHUNKS = 2
WAYS = 2
PARTS = 4
GROUP = 4
LAG = 5
AHEAD = 3
DEEP = 3
SPREAD = 3
TALKS = ((0, 1), (1, 2), (1, 3), (2, 3))
MESH = pl.DeviceIdType.MESH


def rotation_tables(length, head_size):
    half = head_size // 2
    inverse = np.float32(10000.0) ** (-np.arange(half, dtype=np.float32) / np.float32(half))
    angles = np.arange(length, dtype=np.float32)[:, None] * inverse.astype(np.float32)[None, :]
    cosine, sine = np.cos(angles), np.sin(angles)
    return (
        np.concatenate([cosine] * 4, axis=1).astype(np.float32),
        np.concatenate([-sine, sine] * 2, axis=1).astype(np.float32),
    )


def kernel(
    n, n_dp, n_grp, head_size, q_ref, k_ref, v_ref, qg_ref, kg_ref, lam_ref, hg_ref, w_ref, cos_in, sin_in,
    out_ref, total, rx, rot_q, rot_k, heads_out, hrx, wfull,
    in_send, in_recv, ret_send, ret_recv, wx_send, wx_recv, wy_send, wy_recv, wc_send, wc_recv, own_sem, cos_ref, sin_ref, table_sem,
):
    me = lax.axis_index("sp")
    dp = lax.axis_index("dp")
    ways = WAYS if n_grp == WAYS else 1
    grp = lax.axis_index("grp") if ways > 1 else 0
    cores = CORES if n_dp % CORES == 0 else 1
    nx = n_dp // cores
    xi, core = dp // cores, lax.rem(dp, cores)
    tok = q_ref.shape[1]
    width = 2 * head_size
    local_heads = rx.shape[1]
    length = rx.shape[2]
    depth = w_ref.shape[0]
    cols = w_ref.shape[1]
    piece = depth // (CHUNKS * ways)

    def sp_peer(off):
        return lax.rem(me + off, n)

    def dp_index(xo, co):
        return lax.rem(xi + xo, nx) * cores + lax.rem(core + co, cores)

    barrier = pltpu.get_barrier_semaphore()
    for off in range(1, n):
        pl.semaphore_signal(barrier, inc=1, device_id={"sp": sp_peer(off)}, device_id_type=MESH)
    for xo in range(1, nx):
        pl.semaphore_signal(barrier, inc=1, device_id={"dp": dp_index(xo, 0)}, device_id_type=MESH)
    for co in range(1, cores):
        pl.semaphore_signal(barrier, inc=1, device_id={"dp": dp_index(0, co)}, device_id_type=MESH)

    if ways > 1:
        pl.semaphore_signal(
            barrier, inc=1, device_id={"grp": lax.rem(grp + 1, ways)}, device_id_type=MESH
        )

    sources = (k_ref, q_ref, v_ref)

    def own_rows(t, j):
        column = pl.multiple_of((me * local_heads + j) * width, width)
        return pltpu.make_async_copy(
            sources[t].at[0, :, pl.ds(column, width)],
            rx.at[t, j, pl.ds(pl.multiple_of(me * tok, tok), tok), :],
            in_recv.at[t, j, 0],
        )

    def rows_to(t, j, off):
        peer = sp_peer(off)
        column = pl.multiple_of((peer * local_heads + j) * width, width)
        return pltpu.make_async_remote_copy(
            src_ref=sources[t].at[0, :, pl.ds(column, width)],
            dst_ref=rx.at[t, j, pl.ds(pl.multiple_of(me * tok, tok), tok), :],
            send_sem=in_send.at[t, j, off],
            recv_sem=in_recv.at[t, j, off],
            device_id={"sp": peer},
            device_id_type=MESH,
        )

    def rows_from(t, j, off):
        peer = lax.rem(me + n - off, n)
        block = rx.at[t, j, pl.ds(pl.multiple_of(peer * tok, tok), tok), :]
        return pltpu.make_async_remote_copy(
            src_ref=block, dst_ref=block, send_sem=in_send.at[t, j, off],
            recv_sem=in_recv.at[t, j, off], device_id={"sp": peer}, device_id_type=MESH,
        )

    def piece_rows(r, way):
        first = (r * ways + lax.rem(grp + way, ways)) * piece
        return pl.ds(pl.multiple_of(first, piece), piece)

    def moved(source, target, send_sem, recv_sem, device):
        return pltpu.make_async_remote_copy(
            src_ref=source, dst_ref=target, send_sem=send_sem, recv_sem=recv_sem,
            device_id=device, device_id_type=MESH,
        )

    def weight_x(xo, r):
        rows = piece_rows(r, 0)
        return moved(
            w_ref.at[rows, :], wfull.at[dp, rows, :], wx_send.at[xo, r], wx_recv.at[xo, r],
            {"dp": dp_index(xo, 0)},
        )

    def weight_x_in(xo, r):
        block = wfull.at[dp_index(nx - xo, 0), piece_rows(r, 0), :]
        return moved(block, block, wx_send.at[xo, r], wx_recv.at[xo, r], {"dp": dp_index(xo, 0)})

    def weight_y(xo, r):
        block = wfull.at[dp_index(nx - xo, 0), piece_rows(r, 0), :]
        return moved(block, block, wy_send.at[xo, r], wy_recv.at[xo, r], {"grp": lax.rem(grp + 1, ways)})

    def weight_y_in(xo, r):
        block = wfull.at[dp_index(nx - xo, 0), piece_rows(r, 1), :]
        return moved(block, block, wy_send.at[xo, r], wy_recv.at[xo, r], {"grp": lax.rem(grp + 1, ways)})

    def weight_core(xo, r, way):
        rows = piece_rows(r, way)
        target = wfull.at[dp_index(nx - xo, 0), rows, :]
        return moved(
            w_ref.at[rows, :] if xo == 0 else target, target,
            wc_send.at[xo, r, way], wc_recv.at[xo, r, way], {"dp": dp_index(0, 1)},
        )

    def weight_core_in(xo, r, way):
        block = wfull.at[dp_index(nx - xo, 1), piece_rows(r, way), :]
        return moved(
            block, block, wc_send.at[xo, r, way], wc_recv.at[xo, r, way], {"dp": dp_index(0, 1)}
        )

    own_weight = pltpu.make_async_copy(w_ref, wfull.at[dp], own_sem)
    own_weight.start()
    tables = [
        pltpu.make_async_copy(cos_in, cos_ref, table_sem.at[0]),
        pltpu.make_async_copy(sin_in, sin_ref, table_sem.at[1]),
    ]
    for table in tables:
        table.start()
    for j in range(local_heads):
        for t in range(3):
            own_rows(t, j).start()
    pl.semaphore_wait(barrier, (n - 1) + (nx - 1) + (cores - 1) + (ways - 1))
    for j in range(local_heads):
        for t in range(3):
            for off in range(1, n):
                rows_to(t, j, off).start()
        if j == 0:
            for r in range(CHUNKS):
                for xo in range(1, nx):
                    weight_x(xo, r).start()
            if cores > 1:
                for r in range(CHUNKS):
                    for way in range(ways):
                        weight_core(0, r, way).start()

    lane = lax.broadcasted_iota(jnp.int32, (1, width), 1)
    low_map = lane < head_size
    low_half = lax.rem(lane, head_size) < head_size // 2

    def norm_rotate(block, gain):
        x = block.astype(jnp.float32)
        square = x * x
        low = jnp.sum(jnp.where(low_map, square, 0.0), axis=1, keepdims=True)
        high = jnp.sum(jnp.where(low_map, 0.0, square), axis=1, keepdims=True)
        low = lax.rsqrt(low * (1.0 / head_size) + EPSILON)
        high = lax.rsqrt(high * (1.0 / head_size) + EPSILON)
        y = x * jnp.where(low_map, low, high) * gain
        quarter = head_size // 2
        turned = jnp.where(low_half, pltpu.roll(y, width - quarter, 1), pltpu.roll(y, quarter, 1))
        return (y * cos_ref[...] + turned * sin_ref[...]).astype(jnp.bfloat16)

    def heads_to(j, i):
        column = pl.multiple_of(me * width, width)
        off = lax.rem(i + n - me, n)
        return pltpu.make_async_remote_copy(
            src_ref=heads_out.at[j, i], dst_ref=hrx.at[j, :, pl.ds(column, width)],
            send_sem=ret_send.at[j, off], recv_sem=ret_recv.at[j, off],
            device_id={"sp": i}, device_id_type=MESH,
        )

    def heads_from(j, off):
        peer = lax.rem(me + n - off, n)
        column = pl.multiple_of(peer * width, width)
        block = hrx.at[j, :, pl.ds(column, width)]
        return pltpu.make_async_remote_copy(
            src_ref=block, dst_ref=block, send_sem=ret_send.at[j, off],
            recv_sem=ret_recv.at[j, off], device_id={"sp": peer}, device_id_type=MESH,
        )

    groups = math.gcd(n, 4)
    per_group = n // groups
    segment = length // groups
    factor = head_size ** (-0.5) * math.log2(math.e)
    contract = (((1,), (1,)), ((), ()))

    def query_block(j, g, i, lam):
        rows = pl.ds(i * tok, tok) if isinstance(i, int) else pl.ds(pl.multiple_of(i * tok, tok), tok)
        q = rot_q[rows, :]
        zero = jnp.zeros_like(q)
        both = jnp.concatenate([jnp.where(low_map, q, zero), jnp.where(low_map, zero, q)], axis=0)
        start = g * segment
        spans = ([(0, start)] if g else []) + [(start, segment)]
        parts = []
        for first, size in spans:
            scores = lax.dot_general(
                both, rot_k[first : first + size, :], contract, preferred_element_type=jnp.float32
            )
            if first == start:
                shape = (2 * tok, size)
                row = lax.rem(lax.broadcasted_iota(jnp.int32, shape, 0), tok) + i * tok
                column = lax.broadcasted_iota(jnp.int32, shape, 1) + first
                scores = jnp.where(column <= row, scores, -1e30)
            parts.append(scores)
        top = functools.reduce(jnp.maximum, [jnp.max(s, axis=1, keepdims=True) for s in parts])
        parts = [jnp.exp2((s - top) * factor) for s in parts]
        total = functools.reduce(jnp.add, [jnp.sum(e, axis=1, keepdims=True) for e in parts])
        inverse = 1.0 / total
        one, two = inverse[:tok], inverse[tok:] * lam
        raw = None
        for (first, size), e in zip(spans, parts):
            mixing = (e[:tok] * one - e[tok:] * two).astype(jnp.bfloat16)
            term = jnp.dot(mixing, rx[2, j, first : first + size, :], preferred_element_type=jnp.float32)
            raw = term if raw is None else raw + term
        scaled = raw * lax.rsqrt(jnp.mean(raw * raw, axis=1, keepdims=True) + EPSILON)
        result = (scaled * hg_ref[...] * OUT_SCALE).astype(jnp.bfloat16)

        @pl.when(i == me)
        def _():
            hrx[j, :, pl.ds(pl.multiple_of(me * width, width), width)] = result

        @pl.when(i != me)
        def _():
            heads_out[j, i] = result
            heads_to(j, i).start()

    def forward(stage):
        if stage < CHUNKS:
            for xo in range(1, nx):
                weight_x_in(xo, stage).wait_recv()
                if ways > 1:
                    weight_y(xo, stage).start()
                if cores > 1:
                    weight_core(xo, stage, 0).start()
        elif ways > 1:
            for xo in range(1, nx):
                weight_y_in(xo, stage - CHUNKS).wait_recv()
                if cores > 1:
                    weight_core(xo, stage - CHUNKS, 1).start()

    for table in tables:
        table.wait()
    for j in range(local_heads):
        lam = lam_ref[me * local_heads + j]
        for t, (target, gain) in enumerate(((rot_k, kg_ref), (rot_q, qg_ref), (None, None))):
            own_rows(t, j).wait()
            for off in range(1, n):
                rows_from(t, j, off).wait_recv()
            if target is not None:
                target[...] = norm_rotate(rx[t, j], jnp.concatenate([gain[...]] * 2, axis=1))
        for g in range(groups):
            if per_group == 1:
                query_block(j, g, g, lam)
            else:
                def step(b, carry, j=j, g=g, lam=lam):
                    query_block(j, g, g * per_group + b, lam)
                    return carry
                lax.fori_loop(0, per_group, step, 0)
        for stage in range(2 * CHUNKS):
            if j == min(stage, local_heads - 1):
                forward(stage)

    own_weight.wait()
    if cores > 1:
        for xo in range(nx):
            for r in range(CHUNKS):
                for way in range(ways):
                    weight_core_in(xo, r, way).wait_recv()

    for j in range(local_heads):
        for off in range(1, n):
            heads_from(j, off).wait_recv()
        rows = hrx[j]
        for index in range(n_dp):
            matching = jnp.concatenate(
                [wfull[index, pl.ds((s * local_heads + j) * width, width), :] for s in range(n)], axis=0
            )
            term = jnp.dot(rows, matching, preferred_element_type=jnp.float32)
            span = slice(index * cols, (index + 1) * cols)
            if j:
                term = total[:, span] + term
            if j == local_heads - 1:
                out_ref[0, :, span] = term.astype(out_ref.dtype)
            else:
                total[:, span] = term

    for j in range(local_heads):
        for off in range(1, n):
            for t in range(3):
                rows_to(t, j, off).wait_send()
            heads_to(j, sp_peer(off)).wait_send()
    for r in range(CHUNKS):
        for xo in range(nx):
            if xo:
                weight_x(xo, r).wait_send()
                if ways > 1:
                    weight_y(xo, r).wait_send()
            if cores > 1:
                for way in range(ways):
                    weight_core(xo, r, way).wait_send()


def local(n, n_dp, n_grp, query_rows, key_rows, value_rows, query_gain, key_gain, lambdas, head_gain, out_weight):
    tok = query_rows.shape[1]
    head_size = query_gain.shape[0]
    width = head_gain.shape[0]
    local_heads = lambdas.shape[0] // n
    length = tok * n
    depth, cols = out_weight.shape
    cores = CORES if n_dp % CORES == 0 else 1
    nx = n_dp // cores
    cosine, sine = rotation_tables(length, head_size)
    anywhere = pl.BlockSpec(memory_space=pl.ANY)
    vmem = pl.BlockSpec(memory_space=pltpu.VMEM)
    dma = pltpu.SemaphoreType.DMA
    return pl.pallas_call(
        functools.partial(kernel, n, n_dp, n_grp, head_size),
        out_shape=jax.ShapeDtypeStruct((1, tok, n_dp * cols), jnp.bfloat16),
        in_specs=[anywhere] * 3
        + [vmem, vmem, pl.BlockSpec(memory_space=pltpu.SMEM), vmem, anywhere, anywhere, anywhere],
        out_specs=vmem,
        scratch_shapes=[
            pltpu.VMEM((tok, n_dp * cols), jnp.float32),
            pltpu.VMEM((3, local_heads, length, width), jnp.bfloat16),
            pltpu.VMEM((length, width), jnp.bfloat16),
            pltpu.VMEM((length, width), jnp.bfloat16),
            pltpu.VMEM((local_heads, n, tok, width), jnp.bfloat16),
            pltpu.VMEM((local_heads, tok, n * width), jnp.bfloat16),
            pltpu.VMEM((n_dp, depth, cols), jnp.bfloat16),
            dma((3, local_heads, n)),
            dma((3, local_heads, n)),
            dma((local_heads, n)),
            dma((local_heads, n)),
            dma((nx, CHUNKS)),
            dma((nx, CHUNKS)),
            dma((nx, CHUNKS)),
            dma((nx, CHUNKS)),
            dma((nx, CHUNKS, WAYS)),
            dma((nx, CHUNKS, WAYS)),
            dma(()),
            pltpu.VMEM((length, width), jnp.float32),
            pltpu.VMEM((length, width), jnp.float32),
            dma((2,)),
        ],
        compiler_params=pltpu.CompilerParams(
            collective_id=0, has_side_effects=True, vmem_limit_bytes=56 * 1024 * 1024
        ),
    )(
        query_rows, key_rows, value_rows,
        query_gain[None, :], key_gain[None, :], lambdas, head_gain[None, :],
        out_weight, jnp.asarray(cosine), jnp.asarray(sine),
    )


def split_kernel(
    n, n_dp, n_grp, head_size, chunks, q_in, k_in, v_in, qg_ref, kg_ref, lam_ref, hg_ref, w_ref, cos_in, sin_in,
    out_ref, total, rows_in, rot, v_turn, big, small, big_out, small_out, kept, kept_top, gain_turn, heads, wfull,
    cos_ref, sin_ref, turn_ref, load_sem, big_send, small_send, came, wx_send, wx_recv, wy_send, wy_recv, wc_send, wc_recv,
):
    me = lax.axis_index("sp")
    dp = lax.axis_index("dp")
    ways = WAYS if n_grp == WAYS else 1
    grp = lax.axis_index("grp") if ways > 1 else 0
    cores = CORES if n_dp % CORES == 0 else 1
    nx = n_dp // cores
    xi, core = dp // cores, lax.rem(dp, cores)
    count, tok, width = v_turn.shape
    q_rot, k_rot = rot.at[0], rot.at[1]
    depth, cols = w_ref.shape
    piece = depth // (chunks * ways)
    per_chunk = count // chunks
    factor = head_size ** (-0.5) * math.log2(math.e)

    def dp_index(xo, co):
        return lax.rem(xi + xo, nx) * cores + lax.rem(core + co, cores)

    direct = chunks - 1
    alone = count - GROUP

    barrier = pltpu.get_barrier_semaphore()
    for here, there in TALKS:
        for one, other in ((here, there), (there, here)):
            @pl.when(me == one)
            def _(other=other):
                pl.semaphore_signal(barrier, inc=1, device_id={"sp": other}, device_id_type=MESH)
    talkers = sum(jnp.where((me == here) | (me == there), 1, 0) for here, there in TALKS)
    for xo in range(1, nx):
        pl.semaphore_signal(barrier, inc=1, device_id={"dp": dp_index(xo, 0)}, device_id_type=MESH)
    for co in range(1, cores):
        pl.semaphore_signal(barrier, inc=1, device_id={"dp": dp_index(0, co)}, device_id_type=MESH)
    if ways > 1:
        pl.semaphore_signal(barrier, inc=1, device_id={"grp": lax.rem(grp + 1, ways)}, device_id_type=MESH)

    own = pl.ds(pl.multiple_of(me * tok, tok), tok)
    loads = [
        pltpu.make_async_copy(cos_in.at[own, :], cos_ref, load_sem.at[3]),
        pltpu.make_async_copy(sin_in.at[own, :], sin_ref, load_sem.at[4]),
        pltpu.make_async_copy(q_in.at[0], rows_in.at[0], load_sem.at[0]),
        pltpu.make_async_copy(k_in.at[0], rows_in.at[1], load_sem.at[1]),
        pltpu.make_async_copy(v_in.at[0], rows_in.at[2], load_sem.at[2]),
    ]
    own_weight = pltpu.make_async_copy(w_ref, wfull.at[dp], load_sem.at[5])
    for load in loads:
        load.start()
    own_weight.start()

    def moved(source, target, send_sem, recv_sem, device):
        return pltpu.make_async_remote_copy(
            src_ref=source, dst_ref=target, send_sem=send_sem, recv_sem=recv_sem,
            device_id=device, device_id_type=MESH,
        )

    def piece_rows(r, way):
        first = (r * ways + lax.rem(grp + way, ways)) * piece
        return pl.ds(pl.multiple_of(first, piece), piece)

    def weight_x(xo, r, way=0):
        rows = piece_rows(r, way)
        return moved(
            w_ref.at[rows, :], wfull.at[dp, rows, :], wx_send.at[xo - 1], wx_recv.at[xo - 1, r + way],
            {"dp": dp_index(xo, 0)},
        )

    def weight_x_in(xo, r, way=0):
        block = wfull.at[dp_index(nx - xo, 0), piece_rows(r, way), :]
        return moved(block, block, wx_send.at[xo - 1], wx_recv.at[xo - 1, r + way], {"dp": dp_index(xo, 0)})

    def weight_y(xo, r):
        block = wfull.at[dp_index(nx - xo, 0), piece_rows(r, 0), :]
        return moved(
            block, block, wy_send.at[xo - 1], wy_recv.at[xo - 1, r], {"grp": lax.rem(grp + 1, ways)}
        )

    def weight_y_in(xo, r):
        block = wfull.at[dp_index(nx - xo, 0), piece_rows(r, 1), :]
        return moved(
            block, block, wy_send.at[xo - 1], wy_recv.at[xo - 1, r], {"grp": lax.rem(grp + 1, ways)}
        )

    def weight_core(xo, r, way):
        rows = piece_rows(r, way)
        target = wfull.at[dp_index(nx - xo, 0), rows, :]
        return moved(
            w_ref.at[rows, :] if xo == 0 else target, target,
            wc_send.at[xo], wc_recv.at[xo, r * per_chunk // GROUP], {"dp": dp_index(0, 1)},
        )

    def weight_core_in(xo, g, rows):
        block = wfull.at[dp_index(nx - xo, 1), rows, :]
        return moved(block, block, wc_send.at[xo], wc_recv.at[xo, g], {"dp": dp_index(0, 1)})

    def forward_x(r):
        for xo in range(1, nx):
            weight_x_in(xo, r).wait_recv()
            if ways > 1:
                weight_y(xo, r).start()
            if cores > 1:
                weight_core(xo, r, 0).start()

            @pl.when(r + DEEP < direct)
            def _(xo=xo):
                weight_x(xo, r + DEEP).start()

            for way in range(ways):
                @pl.when(r == max(direct - DEEP, 0) + way)
                def _(xo=xo, way=way):
                    weight_x(xo, direct, way).start()

    def forward_y(r):
        if ways > 1:
            for xo in range(1, nx):
                weight_y_in(xo, r).wait_recv()
                if cores > 1:
                    weight_core(xo, r, 1).start()

    def forward_direct():
        for way in range(ways):
            for xo in range(1, nx):
                weight_x_in(xo, direct, way).wait_recv()
                if cores > 1:
                    weight_core(xo, direct, way).start()

    def big_to(source, lane, slot, h, peer, what=0):
        return moved(source.at[h], big.at[h, slot], big_send.at[lane], came.at[what, h], {"sp": peer})

    def small_to(lane, slot, h, peer):
        source = small_out.at[h, min(lane, 1)]
        return moved(source, small.at[h, slot], small_send.at[lane], came.at[1, h], {"sp": peer})

    def came_in(block, what, h):
        moved(block, block, big_send.at[0], came.at[what, h], {"sp": lax.rem(me + 1, n)}).wait_recv()

    def gone(block, sem):
        moved(block, block, sem, came.at[0, 0], {"sp": lax.rem(me + 1, n)}).wait_send()

    pl.semaphore_wait(barrier, talkers + (nx - 1) + (cores - 1) + (ways - 1))
    for r in range(min(DEEP, direct)):
        for xo in range(1, nx):
            weight_x(xo, r).start()
    if cores > 1:
        for r in range(chunks):
            for way in range(ways):
                weight_core(0, r, way).start()

    lane = lax.broadcasted_iota(jnp.int32, (1, width), 1)
    low_map = lane < head_size
    half = head_size // 2
    down, across = (lax.broadcasted_iota(jnp.int32, (width, width), axis) for axis in range(2))
    partner = jnp.where(lax.rem(across, head_size) < half, across + half, across - half)
    swap = jnp.where(down == partner, 1.0, 0.0).astype(jnp.bfloat16)
    same_map = jnp.where((down < head_size) == (across < head_size), 1.0, 0.0).astype(jnp.bfloat16)
    sums = jnp.concatenate([same_map, same_map], axis=0)

    def norm_rotate(which, first):
        blocks = [rows_in[which, :, head_columns(first + i)] for i in range(GROUP)]
        stacked = jnp.concatenate(blocks, axis=0)
        x = stacked.astype(jnp.float32)
        square = x * x
        coarse = square.astype(jnp.bfloat16)
        fine = (square - coarse.astype(jnp.float32)).astype(jnp.bfloat16)
        total_square = jnp.dot(jnp.concatenate([coarse, fine], axis=1), sums, preferred_element_type=jnp.float32)
        other = jnp.dot(stacked, swap, preferred_element_type=jnp.float32)
        inverse = lax.rsqrt(total_square * (1.0 / head_size) + EPSILON)
        for i in range(GROUP):
            part = slice(i * tok, (i + 1) * tok)
            straight = x[part] * inverse[part] * turn_ref[2 * which]
            turned = other[part] * inverse[part] * turn_ref[2 * which + 1]
            rot[which, first + i] = (straight + turned).astype(jnp.bfloat16)

    for load in loads[:3]:
        load.wait()
    gain_turn[...] = jnp.broadcast_to(hg_ref[...], (tok, width)).T
    for which, gain in enumerate((qg_ref, kg_ref)):
        gain = gain[...]
        crossed = jnp.concatenate([gain[:, half:], gain[:, :half]], axis=1)
        turn_ref[2 * which] = cos_ref[...] * jnp.concatenate([gain, gain], axis=1)
        turn_ref[2 * which + 1] = sin_ref[...] * jnp.concatenate([crossed, crossed], axis=1)
    causal = lax.broadcasted_iota(jnp.int32, (tok, 2 * tok), 0) <= lax.rem(
        lax.broadcasted_iota(jnp.int32, (tok, 2 * tok), 1), tok
    )

    def head_columns(h):
        return pl.ds(pl.multiple_of(h * width, width), width)

    def turned_scores(keys, *queries):
        both = []
        for q in queries:
            zero = jnp.zeros_like(q)
            both += [jnp.where(low_map, q, zero), jnp.where(low_map, zero, q)]
        both = jnp.concatenate(both, axis=0)
        return lax.dot_general(keys, both, (((1,), (1,)), ((), ())), preferred_element_type=jnp.float32)

    def exponents(scores):
        top = jnp.max(scores, axis=0, keepdims=True)
        e = jnp.exp2((scores - top) * factor)
        return top * factor, e, jnp.sum(e, axis=0, keepdims=True)

    def mixing_of(e, scale, lam):
        one, two = scale[:, :tok], scale[:, tok:] * lam
        return (e[:, :tok] * one - e[:, tok:] * two).astype(jnp.bfloat16)

    def mixed(e, scale, lam, values):
        return jnp.dot(values, mixing_of(e, scale, lam), preferred_element_type=jnp.float32)

    def put_pair(ref, h, slot, pair):
        ref[h, slot, 0:1, :] = pair[:, :tok]
        ref[h, slot, 1:2, :] = pair[:, tok:]

    def get_pair(ref, h, slot):
        return jnp.concatenate([ref[h, slot, 0:1, :], ref[h, slot, 1:2, :]], axis=1)

    def joined(levels):
        top = functools.reduce(jnp.maximum, levels)
        return top + jnp.log2(functools.reduce(jnp.add, [jnp.exp2(l - top) for l in levels]))

    def finish(raw, h):
        scaled = raw * lax.rsqrt(jnp.mean(raw * raw, axis=0, keepdims=True) + EPSILON)
        result = (scaled * gain_turn[...] * OUT_SCALE).T
        heads[:, head_columns(h)] = result.astype(jnp.bfloat16)

    def partial_scores(keys, queries, slot, first, masked):
        scores = [turned_scores(k, q) for k, q in zip(keys, queries)]
        if masked:
            scores = [jnp.where(causal, s, -1e30) for s in scores]
        parts = [exponents(s) for s in scores]
        for i, (top, e, z) in enumerate(parts):
            kept[first + i, slot] = e
            put_pair(kept_top, first + i, slot, top)
            put_pair(small_out, first + i, slot, top + jnp.log2(z))

    def third_queries(h):
        big_to(q_rot, 1, 3, h, 2).start()
        big_to(q_rot, 0, 3, h, 1).start()

    def prepare(j, carry):
        first = j * GROUP
        members = range(GROUP)

        @pl.when((me == 0) & (j == 0))
        def _():
            loads[3].wait()
            loads[4].wait()

        def turn_values():
            for i in members:
                v_turn[first + i] = rows_in[2, :, head_columns(first + i)].astype(jnp.float32).T.astype(jnp.bfloat16)

        ahead = jnp.where(me == 0, 1, 0)
        norm_rotate(ahead, first)

        @pl.when((me == 3) & (j == 0))
        def _():
            third_queries(0)

        @pl.when((me == 2) & (j == 0))
        def _():
            for i in range(AHEAD):
                big_to(q_rot, 0, 2, i, 1).start()

        @pl.when((me > 0) & (j == 0))
        def _():
            loads[3].wait()
            loads[4].wait()

        turn_values()

        @pl.when(me == 0)
        def _():
            for i in members:
                big_to(k_rot, 0, 0, first + i, 1).start()
                big_to(v_turn, 1, 1, first + i, 1).start()

        norm_rotate(1 - ahead, first)

        @pl.when((me == 2) & (first >= alone))
        def _():
            for i in members:
                big_to(k_rot, 2, 2, first + i, 3, 2).start()
                big_to(v_turn, 2, 3, first + i, 3, 2).start()

        @pl.when((me == 2) | ((me == 3) & (first < alone)))
        def _():
            partial_scores([k_rot[first + i] for i in members], [q_rot[first + i] for i in members], 0, first, True)

        @pl.when(me == 2)
        def _():
            for i in members:
                small_to(0, 0, first + i, 1).start()

        @pl.when((me == 3) & (first < alone))
        def _():
            for i in members:
                if i:
                    third_queries(first + i)
                else:
                    @pl.when(j > 0)
                    def _():
                        third_queries(first)
                small_to(0, 1, first + i, 1).start()

        return carry

    lax.fori_loop(0, count // GROUP, prepare, 0)

    @pl.when(me == 1)
    def _():
        for h in range(alone, count):
            small[h, 2] = jnp.full((2, tok), -1e30, jnp.float32)

    def lowest(h):
        scores = jnp.where(causal, turned_scores(k_rot[h], q_rot[h]), -1e30)
        _, e, z = exponents(scores)
        finish(mixed(e, 1.0 / z, lam_ref[h], v_turn[h]), h)

    def centre(h):
        came_in(big.at[h], 0, h)

        @pl.when(h < alone)
        def _():
            came_in(small.at[h], 1, h)

        @pl.when(h >= alone)
        def _():
            came_in(small.at[h, 0:2], 1, h)

        keys = jnp.concatenate([big[h, 0], k_rot[h]], axis=0)
        values = jnp.concatenate([big[h, 1], v_turn[h]], axis=1)
        second, third, third_too = (get_pair(small, h, slot) for slot in range(3))
        lam = lam_ref[h]
        pair = 2 * tok
        scores = turned_scores(keys, q_rot[h], big[h, 2], big[h, 3])
        seen = jnp.concatenate([scores[:tok, :pair], jnp.where(causal, scores[tok:, :pair], -1e30)], axis=0)
        scores = jnp.concatenate([seen, scores[:, pair:]], axis=1)
        top, e, z = exponents(scores)
        level = top + jnp.log2(z)
        level_two = joined([level[:, pair : 2 * pair], second])
        level_three = joined([level[:, 2 * pair :], third, third_too])
        put_pair(small_out, h, 0, level_two)
        put_pair(small_out, h, 1, level_three)
        scales = [
            1.0 / z[:, :pair],
            jnp.exp2(top[:, pair : 2 * pair] - level_two),
            jnp.exp2(top[:, 2 * pair :] - level_three),
        ]
        mixing = [mixing_of(e[:, i * pair : (i + 1) * pair], scale, lam) for i, scale in enumerate(scales)]
        raw = jnp.dot(values, jnp.concatenate(mixing, axis=1), preferred_element_type=jnp.float32)
        big_out[1, h] = raw[:, 2 * tok :].astype(jnp.bfloat16)
        big_out[0, h] = raw[:, tok : 2 * tok].astype(jnp.bfloat16)

        @pl.when(h < alone)
        def _():
            small_to(1, 1, h, 2).start()

        small_to(0, 0, h, 2).start()
        small_to(2, 1, h, 3).start()
        big_to(big_out.at[1], 1, 0, h, 3).start()
        big_to(big_out.at[0], 0, 0, h, 2, 2).start()
        finish(raw[:, :tok], h)

    def upper_scores(h):
        @pl.when(h < alone)
        def _():
            came_in(big.at[h, 3], 0, h)
            partial_scores([k_rot[h]], [big[h, 3]], 1, h, False)
            small_to(1, 2, h, 1).start()

        @pl.when(h + AHEAD < alone)
        def _():
            big_to(q_rot, 0, 2, h + AHEAD, 1).start()

        @pl.when(h == alone - 2)
        def _():
            big_to(q_rot, 0, 2, alone, 1).start()

        @pl.when(h == alone - 1)
        def _():
            for i in range(1, GROUP):
                big_to(q_rot, 0, 2, alone + i, 1).start()

    def upper_raw(h, slot, level):
        scale = jnp.exp2(get_pair(kept_top, h, slot) - level)
        return mixed(kept[h, slot], scale, lam_ref[h], v_turn[h])

    def upper_second(h):
        @pl.when(h < alone)
        def _():
            came_in(small.at[h, 0:2], 1, h)
            big_out[1, h] = upper_raw(h, 1, get_pair(small, h, 1)).astype(jnp.bfloat16)
            big_to(big_out.at[1], 1, 1, h, 3).start()

        @pl.when(h >= alone)
        def _():
            came_in(small.at[h, 0:1], 1, h)

        came_in(big.at[h, 0], 2, h)
        finish(upper_raw(h, 0, get_pair(small, h, 0)) + big[h, 0].astype(jnp.float32), h)

    def joint_scores(h):
        came_in(big.at[h, 2:4], 2, h)
        scores = turned_scores(jnp.concatenate([big[h, 2], k_rot[h]], axis=0), q_rot[h])
        scores = jnp.concatenate([scores[:tok], jnp.where(causal, scores[tok:], -1e30)], axis=0)
        top, e, z = exponents(scores)
        kept[h, 0] = e[:tok]
        kept[h, 1] = e[tok:]
        put_pair(kept_top, h, 0, top)
        put_pair(small_out, h, 0, top + jnp.log2(z))

    def upper_third(h):
        came_in(small.at[h, 1], 1, h)

        @pl.when(h < alone)
        def _():
            came_in(big.at[h, 0:2], 0, h)
            raw = upper_raw(h, 0, get_pair(small, h, 1)) + big[h, 0].astype(jnp.float32)
            finish(raw + big[h, 1].astype(jnp.float32), h)

        @pl.when(h >= alone)
        def _():
            came_in(big.at[h, 0], 0, h)
            scale = jnp.exp2(get_pair(kept_top, h, 0) - get_pair(small, h, 1))
            e = jnp.concatenate([kept[h, 0], kept[h, 1]], axis=0)
            values = jnp.concatenate([big[h, 3], v_turn[h]], axis=1)
            finish(mixed(e, scale, lam_ref[h], values) + big[h, 0].astype(jnp.float32), h)

    group = GROUP

    def project(g, first, last):
        step = group * width
        rows = pl.ds(g * step, step) if isinstance(g, int) else pl.ds(pl.multiple_of(g * step, step), step)
        if cores > 1:
            for xo in range(nx):
                weight_core_in(xo, g, rows).wait_recv()
        block = heads[:, rows]
        for index in range(n_dp):
            term = jnp.dot(block, wfull[index, rows, :], preferred_element_type=jnp.float32)
            span = slice(index * cols, (index + 1) * cols)
            if not first:
                term = total[:, span] + term
            if last:
                out_ref[0, :, span] = term.astype(out_ref.dtype)
            else:
                total[:, span] = term

    groups = count // group

    first_x = jnp.where(me == 1, 0, 1)
    first_y = first_x + 2 * per_chunk
    last_x = first_x + direct * per_chunk

    def step(it, carry):
        @pl.when((me == 2) & (it < count))
        def _():
            upper_scores(it)

        turn = lax.rem(it - first_x + per_chunk, per_chunk) == 0

        @pl.when(turn & (it >= first_x) & (it < last_x))
        def _():
            forward_x((it - first_x) // per_chunk)

        @pl.when(turn & (it >= first_y) & (it < first_y + direct * per_chunk))
        def _():
            forward_y((it - first_y) // per_chunk)

        @pl.when(it == jnp.where(me == 1, count, last_x))
        def _():
            forward_direct()

        @pl.when((me == 0) & (it < count))
        def _():
            lowest(it)

        @pl.when((me == 1) & (it < count))
        def _():
            centre(it)

        @pl.when((me == 3) & (it < GROUP))
        def _():
            joint_scores(alone + it)

        @pl.when((me == 2) & (it >= LAG))
        def _():
            upper_second(it - LAG)

        @pl.when((me == 3) & (it >= LAG + SPREAD) & (it < LAG + SPREAD + GROUP))
        def _():
            h = alone + it - (LAG + SPREAD)
            big_to(q_rot, 0, 3, h, 1).start()
            small_to(0, 1, h, 1).start()

        @pl.when((me == 3) & (it >= LAG))
        def _():
            upper_third(it - LAG)

        for g in range(groups - 1):
            @pl.when(it == (g + 1) * group + 1 + jnp.where(me == 1, LAG - 2, LAG))
            def _(g=g):
                if g == 0:
                    own_weight.wait()
                project(g, g == 0, False)

        return carry

    lax.fori_loop(0, count + LAG, step, 0)
    project(groups - 1, False, True)

    whole, most = q_rot.at[:], q_rot.at[0:alone]
    rows = small_out.at[:, 0]
    most_rows = small_out.at[0:alone, 0]

    @pl.when(me == 0)
    def _():
        gone(whole, big_send.at[0])
        gone(whole, big_send.at[1])

    @pl.when(me == 1)
    def _():
        gone(whole, big_send.at[0])
        gone(whole, big_send.at[1])
        gone(rows, small_send.at[0])
        gone(most_rows, small_send.at[1])
        gone(rows, small_send.at[2])

    @pl.when(me == 2)
    def _():
        gone(whole, big_send.at[0])
        gone(most, big_send.at[1])
        gone(q_rot.at[0 : 2 * GROUP], big_send.at[2])
        gone(rows, small_send.at[0])
        gone(most_rows, small_send.at[1])

    @pl.when(me == 3)
    def _():
        gone(whole, big_send.at[0])
        gone(most, big_send.at[1])
        gone(rows, small_send.at[0])

    for xo in range(nx):
        if xo:
            sent_x = wfull.at[0, 0 : (direct + ways) * piece, :]
            moved(sent_x, sent_x, wx_send.at[xo - 1], wx_recv.at[0, 0], {"dp": dp_index(xo, 0)}).wait_send()
            if ways > 1:
                sent_y = wfull.at[0, 0 : direct * piece, :]
                moved(sent_y, sent_y, wy_send.at[xo - 1], wy_recv.at[0, 0], {"dp": dp_index(xo, 0)}).wait_send()
        if cores > 1:
            sent_core = wfull.at[0]
            moved(sent_core, sent_core, wc_send.at[xo], wc_recv.at[0, 0], {"dp": dp_index(0, 1)}).wait_send()


def split_local(n, n_dp, n_grp, query_rows, key_rows, value_rows, query_gain, key_gain, lambdas, head_gain, out_weight):
    tok = query_rows.shape[1]
    head_size = query_gain.shape[0]
    width = head_gain.shape[0]
    count = lambdas.shape[0]
    depth, cols = out_weight.shape
    ways = WAYS if n_grp == WAYS else 1
    chunks = count // ways
    cores = CORES if n_dp % CORES == 0 else 1
    nx = n_dp // cores
    cosine, sine = rotation_tables(tok * n, head_size)
    anywhere = pl.BlockSpec(memory_space=pl.ANY)
    vmem = pl.BlockSpec(memory_space=pltpu.VMEM)
    dma = pltpu.SemaphoreType.DMA
    across = max(nx - 1, 1)
    return pl.pallas_call(
        functools.partial(split_kernel, n, n_dp, n_grp, head_size, chunks),
        out_shape=pltpu.VMEM((1, tok, n_dp * cols), jnp.bfloat16),
        in_specs=[anywhere] * 3
        + [vmem, vmem, pl.BlockSpec(memory_space=pltpu.SMEM), vmem, anywhere, anywhere, anywhere],
        out_specs=vmem,
        scratch_shapes=[
            pltpu.VMEM((tok, n_dp * cols), jnp.float32),
            pltpu.VMEM((3, tok, count * width), jnp.bfloat16),
            pltpu.VMEM((2, count, tok, width), jnp.bfloat16),
            pltpu.VMEM((count, tok, width), jnp.bfloat16),
            pltpu.VMEM((count, 4, tok, width), jnp.bfloat16),
            pltpu.VMEM((count, 3, 2, tok), jnp.float32),
            pltpu.VMEM((2, count, tok, width), jnp.bfloat16),
            pltpu.VMEM((count, 2, 2, tok), jnp.float32),
            pltpu.VMEM((count, 2, tok, 2 * tok), jnp.float32),
            pltpu.VMEM((count, 2, 2, tok), jnp.float32),
            pltpu.VMEM((width, tok), jnp.float32),
            pltpu.VMEM((tok, count * width), jnp.bfloat16),
            pltpu.VMEM((n_dp, depth, cols), jnp.bfloat16),
            pltpu.VMEM((tok, width), jnp.float32),
            pltpu.VMEM((tok, width), jnp.float32),
            pltpu.VMEM((4, tok, width), jnp.float32),
            dma((6,)),
            dma((3,)),
            dma((3,)),
            dma((3, count)),
            dma((across,)),
            dma((across, chunks - 1 + ways)),
            dma((across,)),
            dma((across, chunks)),
            dma((nx,)),
            dma((nx, count // GROUP)),
        ],
        compiler_params=pltpu.CompilerParams(
            collective_id=0, has_side_effects=True, vmem_limit_bytes=56 * 1024 * 1024
        ),
    )(
        query_rows, key_rows, value_rows,
        query_gain[None, :], key_gain[None, :], lambdas, head_gain[None, :],
        out_weight, jnp.asarray(cosine), jnp.asarray(sine),
    )


def plan(n, tok, width, count, n_grp):
    ways = WAYS if n_grp == WAYS else 1
    fits = n == PARTS and tok == width and count % (GROUP * ways) == 0
    return split_local if fits else local


def solution(mesh):
    rows = P(("grp", "dp"), "sp", None)
    n, n_dp, n_grp = mesh.shape["sp"], mesh.shape["dp"], mesh.shape["grp"]

    def body(*args):
        chosen = plan(n, args[0].shape[1], args[6].shape[0], args[5].shape[0], n_grp)
        return chosen(n, n_dp, n_grp, *args)

    return jax.shard_map(
        body,
        mesh=mesh,
        in_specs=(rows, rows, rows, P(), P(), P(), P(), P(None, "dp")),
        out_specs=rows,
        check_vma=False,
    )
```

```python
import functools
import math

import jax
import jax.numpy as jnp
import numpy as np
from jax import lax
from jax.experimental import pallas as pl
from jax.experimental.pallas import tpu as pltpu
from jax.sharding import PartitionSpec as P

EPSILON = 1e-06
OUT_SCALE = 0.8
CORES = 2
CHUNKS = 2
WAYS = 2
PARTS = 4
GROUP = 4
LAG = 7
AHEAD = 3
DEEP = 3
SPREAD = 4
BEHIND = 2
NEAR = 4
HELP = 5
PROJECT = 10
SWAP = 2
PACED = 2
TALKS = ((0, 1), (1, 2), (1, 3), (2, 3))
MESH = pl.DeviceIdType.MESH


def rotation_tables(length, head_size):
    half = head_size // 2
    inverse = np.float32(10000.0) ** (-np.arange(half, dtype=np.float32) / np.float32(half))
    angles = np.arange(length, dtype=np.float32)[:, None] * inverse.astype(np.float32)[None, :]
    cosine, sine = np.cos(angles), np.sin(angles)
    return (
        np.concatenate([cosine] * 4, axis=1).astype(np.float32),
        np.concatenate([-sine, sine] * 2, axis=1).astype(np.float32),
    )


def kernel(
    n, n_dp, n_grp, head_size, q_ref, k_ref, v_ref, qg_ref, kg_ref, lam_ref, hg_ref, w_ref, cos_in, sin_in,
    out_ref, total, rx, rot_q, rot_k, heads_out, hrx, wfull,
    in_send, in_recv, ret_send, ret_recv, wx_send, wx_recv, wy_send, wy_recv, wc_send, wc_recv, own_sem, cos_ref, sin_ref, table_sem,
):
    me = lax.axis_index("sp")
    dp = lax.axis_index("dp")
    ways = WAYS if n_grp == WAYS else 1
    grp = lax.axis_index("grp") if ways > 1 else 0
    cores = CORES if n_dp % CORES == 0 else 1
    nx = n_dp // cores
    xi, core = dp // cores, lax.rem(dp, cores)
    tok = q_ref.shape[1]
    width = 2 * head_size
    local_heads = rx.shape[1]
    length = rx.shape[2]
    depth = w_ref.shape[0]
    cols = w_ref.shape[1]
    piece = depth // (CHUNKS * ways)

    def sp_peer(off):
        return lax.rem(me + off, n)

    def dp_index(xo, co):
        return lax.rem(xi + xo, nx) * cores + lax.rem(core + co, cores)

    barrier = pltpu.get_barrier_semaphore()
    for off in range(1, n):
        pl.semaphore_signal(barrier, inc=1, device_id={"sp": sp_peer(off)}, device_id_type=MESH)
    for xo in range(1, nx):
        pl.semaphore_signal(barrier, inc=1, device_id={"dp": dp_index(xo, 0)}, device_id_type=MESH)
    for co in range(1, cores):
        pl.semaphore_signal(barrier, inc=1, device_id={"dp": dp_index(0, co)}, device_id_type=MESH)

    if ways > 1:
        pl.semaphore_signal(
            barrier, inc=1, device_id={"grp": lax.rem(grp + 1, ways)}, device_id_type=MESH
        )

    sources = (k_ref, q_ref, v_ref)

    def own_rows(t, j):
        column = pl.multiple_of((me * local_heads + j) * width, width)
        return pltpu.make_async_copy(
            sources[t].at[0, :, pl.ds(column, width)],
            rx.at[t, j, pl.ds(pl.multiple_of(me * tok, tok), tok), :],
            in_recv.at[t, j, 0],
        )

    def rows_to(t, j, off):
        peer = sp_peer(off)
        column = pl.multiple_of((peer * local_heads + j) * width, width)
        return pltpu.make_async_remote_copy(
            src_ref=sources[t].at[0, :, pl.ds(column, width)],
            dst_ref=rx.at[t, j, pl.ds(pl.multiple_of(me * tok, tok), tok), :],
            send_sem=in_send.at[t, j, off],
            recv_sem=in_recv.at[t, j, off],
            device_id={"sp": peer},
            device_id_type=MESH,
        )

    def rows_from(t, j, off):
        peer = lax.rem(me + n - off, n)
        block = rx.at[t, j, pl.ds(pl.multiple_of(peer * tok, tok), tok), :]
        return pltpu.make_async_remote_copy(
            src_ref=block, dst_ref=block, send_sem=in_send.at[t, j, off],
            recv_sem=in_recv.at[t, j, off], device_id={"sp": peer}, device_id_type=MESH,
        )

    def piece_rows(r, way):
        first = (r * ways + lax.rem(grp + way, ways)) * piece
        return pl.ds(pl.multiple_of(first, piece), piece)

    def moved(source, target, send_sem, recv_sem, device):
        return pltpu.make_async_remote_copy(
            src_ref=source, dst_ref=target, send_sem=send_sem, recv_sem=recv_sem,
            device_id=device, device_id_type=MESH,
        )

    def weight_x(xo, r):
        rows = piece_rows(r, 0)
        return moved(
            w_ref.at[rows, :], wfull.at[dp, rows, :], wx_send.at[xo, r], wx_recv.at[xo, r],
            {"dp": dp_index(xo, 0)},
        )

    def weight_x_in(xo, r):
        block = wfull.at[dp_index(nx - xo, 0), piece_rows(r, 0), :]
        return moved(block, block, wx_send.at[xo, r], wx_recv.at[xo, r], {"dp": dp_index(xo, 0)})

    def weight_y(xo, r):
        block = wfull.at[dp_index(nx - xo, 0), piece_rows(r, 0), :]
        return moved(block, block, wy_send.at[xo, r], wy_recv.at[xo, r], {"grp": lax.rem(grp + 1, ways)})

    def weight_y_in(xo, r):
        block = wfull.at[dp_index(nx - xo, 0), piece_rows(r, 1), :]
        return moved(block, block, wy_send.at[xo, r], wy_recv.at[xo, r], {"grp": lax.rem(grp + 1, ways)})

    def weight_core(xo, r, way):
        rows = piece_rows(r, way)
        target = wfull.at[dp_index(nx - xo, 0), rows, :]
        return moved(
            w_ref.at[rows, :] if xo == 0 else target, target,
            wc_send.at[xo, r, way], wc_recv.at[xo, r, way], {"dp": dp_index(0, 1)},
        )

    def weight_core_in(xo, r, way):
        block = wfull.at[dp_index(nx - xo, 1), piece_rows(r, way), :]
        return moved(
            block, block, wc_send.at[xo, r, way], wc_recv.at[xo, r, way], {"dp": dp_index(0, 1)}
        )

    own_weight = pltpu.make_async_copy(w_ref, wfull.at[dp], own_sem)
    own_weight.start()
    tables = [
        pltpu.make_async_copy(cos_in, cos_ref, table_sem.at[0]),
        pltpu.make_async_copy(sin_in, sin_ref, table_sem.at[1]),
    ]
    for table in tables:
        table.start()
    for j in range(local_heads):
        for t in range(3):
            own_rows(t, j).start()
    pl.semaphore_wait(barrier, (n - 1) + (nx - 1) + (cores - 1) + (ways - 1))
    for j in range(local_heads):
        for t in range(3):
            for off in range(1, n):
                rows_to(t, j, off).start()
        if j == 0:
            for r in range(CHUNKS):
                for xo in range(1, nx):
                    weight_x(xo, r).start()
            if cores > 1:
                for r in range(CHUNKS):
                    for way in range(ways):
                        weight_core(0, r, way).start()

    lane = lax.broadcasted_iota(jnp.int32, (1, width), 1)
    low_map = lane < head_size
    low_half = lax.rem(lane, head_size) < head_size // 2

    def norm_rotate(block, gain):
        x = block.astype(jnp.float32)
        square = x * x
        low = jnp.sum(jnp.where(low_map, square, 0.0), axis=1, keepdims=True)
        high = jnp.sum(jnp.where(low_map, 0.0, square), axis=1, keepdims=True)
        low = lax.rsqrt(low * (1.0 / head_size) + EPSILON)
        high = lax.rsqrt(high * (1.0 / head_size) + EPSILON)
        y = x * jnp.where(low_map, low, high) * gain
        quarter = head_size // 2
        turned = jnp.where(low_half, pltpu.roll(y, width - quarter, 1), pltpu.roll(y, quarter, 1))
        return (y * cos_ref[...] + turned * sin_ref[...]).astype(jnp.bfloat16)

    def heads_to(j, i):
        column = pl.multiple_of(me * width, width)
        off = lax.rem(i + n - me, n)
        return pltpu.make_async_remote_copy(
            src_ref=heads_out.at[j, i], dst_ref=hrx.at[j, :, pl.ds(column, width)],
            send_sem=ret_send.at[j, off], recv_sem=ret_recv.at[j, off],
            device_id={"sp": i}, device_id_type=MESH,
        )

    def heads_from(j, off):
        peer = lax.rem(me + n - off, n)
        column = pl.multiple_of(peer * width, width)
        block = hrx.at[j, :, pl.ds(column, width)]
        return pltpu.make_async_remote_copy(
            src_ref=block, dst_ref=block, send_sem=ret_send.at[j, off],
            recv_sem=ret_recv.at[j, off], device_id={"sp": peer}, device_id_type=MESH,
        )

    groups = math.gcd(n, 4)
    per_group = n // groups
    segment = length // groups
    factor = head_size ** (-0.5) * math.log2(math.e)
    contract = (((1,), (1,)), ((), ()))

    def query_block(j, g, i, lam):
        rows = pl.ds(i * tok, tok) if isinstance(i, int) else pl.ds(pl.multiple_of(i * tok, tok), tok)
        q = rot_q[rows, :]
        zero = jnp.zeros_like(q)
        both = jnp.concatenate([jnp.where(low_map, q, zero), jnp.where(low_map, zero, q)], axis=0)
        start = g * segment
        spans = ([(0, start)] if g else []) + [(start, segment)]
        parts = []
        for first, size in spans:
            scores = lax.dot_general(
                both, rot_k[first : first + size, :], contract, preferred_element_type=jnp.float32
            )
            if first == start:
                shape = (2 * tok, size)
                row = lax.rem(lax.broadcasted_iota(jnp.int32, shape, 0), tok) + i * tok
                column = lax.broadcasted_iota(jnp.int32, shape, 1) + first
                scores = jnp.where(column <= row, scores, -1e30)
            parts.append(scores)
        top = functools.reduce(jnp.maximum, [jnp.max(s, axis=1, keepdims=True) for s in parts])
        parts = [jnp.exp2((s - top) * factor) for s in parts]
        total = functools.reduce(jnp.add, [jnp.sum(e, axis=1, keepdims=True) for e in parts])
        inverse = 1.0 / total
        one, two = inverse[:tok], inverse[tok:] * lam
        raw = None
        for (first, size), e in zip(spans, parts):
            mixing = (e[:tok] * one - e[tok:] * two).astype(jnp.bfloat16)
            term = jnp.dot(mixing, rx[2, j, first : first + size, :], preferred_element_type=jnp.float32)
            raw = term if raw is None else raw + term
        scaled = raw * lax.rsqrt(jnp.mean(raw * raw, axis=1, keepdims=True) + EPSILON)
        result = (scaled * hg_ref[...] * OUT_SCALE).astype(jnp.bfloat16)

        @pl.when(i == me)
        def _():
            hrx[j, :, pl.ds(pl.multiple_of(me * width, width), width)] = result

        @pl.when(i != me)
        def _():
            heads_out[j, i] = result
            heads_to(j, i).start()

    def forward(stage):
        if stage < CHUNKS:
            for xo in range(1, nx):
                weight_x_in(xo, stage).wait_recv()
                if ways > 1:
                    weight_y(xo, stage).start()
                if cores > 1:
                    weight_core(xo, stage, 0).start()
        elif ways > 1:
            for xo in range(1, nx):
                weight_y_in(xo, stage - CHUNKS).wait_recv()
                if cores > 1:
                    weight_core(xo, stage - CHUNKS, 1).start()

    for table in tables:
        table.wait()
    for j in range(local_heads):
        lam = lam_ref[me * local_heads + j]
        for t, (target, gain) in enumerate(((rot_k, kg_ref), (rot_q, qg_ref), (None, None))):
            own_rows(t, j).wait()
            for off in range(1, n):
                rows_from(t, j, off).wait_recv()
            if target is not None:
                target[...] = norm_rotate(rx[t, j], jnp.concatenate([gain[...]] * 2, axis=1))
        for g in range(groups):
            if per_group == 1:
                query_block(j, g, g, lam)
            else:
                def step(b, carry, j=j, g=g, lam=lam):
                    query_block(j, g, g * per_group + b, lam)
                    return carry
                lax.fori_loop(0, per_group, step, 0)
        for stage in range(2 * CHUNKS):
            if j == min(stage, local_heads - 1):
                forward(stage)

    own_weight.wait()
    if cores > 1:
        for xo in range(nx):
            for r in range(CHUNKS):
                for way in range(ways):
                    weight_core_in(xo, r, way).wait_recv()

    for j in range(local_heads):
        for off in range(1, n):
            heads_from(j, off).wait_recv()
        rows = hrx[j]
        for index in range(n_dp):
            matching = jnp.concatenate(
                [wfull[index, pl.ds((s * local_heads + j) * width, width), :] for s in range(n)], axis=0
            )
            term = jnp.dot(rows, matching, preferred_element_type=jnp.float32)
            span = slice(index * cols, (index + 1) * cols)
            if j:
                term = total[:, span] + term
            if j == local_heads - 1:
                out_ref[0, :, span] = term.astype(out_ref.dtype)
            else:
                total[:, span] = term

    for j in range(local_heads):
        for off in range(1, n):
            for t in range(3):
                rows_to(t, j, off).wait_send()
            heads_to(j, sp_peer(off)).wait_send()
    for r in range(CHUNKS):
        for xo in range(nx):
            if xo:
                weight_x(xo, r).wait_send()
                if ways > 1:
                    weight_y(xo, r).wait_send()
            if cores > 1:
                for way in range(ways):
                    weight_core(xo, r, way).wait_send()


def local(n, n_dp, n_grp, query_rows, key_rows, value_rows, query_gain, key_gain, lambdas, head_gain, out_weight):
    tok = query_rows.shape[1]
    head_size = query_gain.shape[0]
    width = head_gain.shape[0]
    local_heads = lambdas.shape[0] // n
    length = tok * n
    depth, cols = out_weight.shape
    cores = CORES if n_dp % CORES == 0 else 1
    nx = n_dp // cores
    cosine, sine = rotation_tables(length, head_size)
    anywhere = pl.BlockSpec(memory_space=pl.ANY)
    vmem = pl.BlockSpec(memory_space=pltpu.VMEM)
    dma = pltpu.SemaphoreType.DMA
    return pl.pallas_call(
        functools.partial(kernel, n, n_dp, n_grp, head_size),
        out_shape=jax.ShapeDtypeStruct((1, tok, n_dp * cols), jnp.bfloat16),
        in_specs=[anywhere] * 3
        + [vmem, vmem, pl.BlockSpec(memory_space=pltpu.SMEM), vmem, anywhere, anywhere, anywhere],
        out_specs=vmem,
        scratch_shapes=[
            pltpu.VMEM((tok, n_dp * cols), jnp.float32),
            pltpu.VMEM((3, local_heads, length, width), jnp.bfloat16),
            pltpu.VMEM((length, width), jnp.bfloat16),
            pltpu.VMEM((length, width), jnp.bfloat16),
            pltpu.VMEM((local_heads, n, tok, width), jnp.bfloat16),
            pltpu.VMEM((local_heads, tok, n * width), jnp.bfloat16),
            pltpu.VMEM((n_dp, depth, cols), jnp.bfloat16),
            dma((3, local_heads, n)),
            dma((3, local_heads, n)),
            dma((local_heads, n)),
            dma((local_heads, n)),
            dma((nx, CHUNKS)),
            dma((nx, CHUNKS)),
            dma((nx, CHUNKS)),
            dma((nx, CHUNKS)),
            dma((nx, CHUNKS, WAYS)),
            dma((nx, CHUNKS, WAYS)),
            dma(()),
            pltpu.VMEM((length, width), jnp.float32),
            pltpu.VMEM((length, width), jnp.float32),
            dma((2,)),
        ],
        compiler_params=pltpu.CompilerParams(
            collective_id=0, has_side_effects=True, vmem_limit_bytes=56 * 1024 * 1024
        ),
    )(
        query_rows, key_rows, value_rows,
        query_gain[None, :], key_gain[None, :], lambdas, head_gain[None, :],
        out_weight, jnp.asarray(cosine), jnp.asarray(sine),
    )


def split_kernel(
    n, n_dp, n_grp, head_size, chunks, q_in, k_in, v_in, qg_in, kg_in, lam_in, hg_in, w_ref, cos_in, sin_in,
    out_ref, total, rows_in, rot, v_turn, big, small, big_out, small_out, kept, kept_top, gain_turn, heads, wfull,
    cos_ref, sin_ref, turn_ref, qg_ref, kg_ref, lam_ref, hg_ref, load_sem, big_send, small_send, came, wx_send, wx_recv, wy_send, wy_recv, wc_send, wc_recv,
):
    me = lax.axis_index("sp")
    dp = lax.axis_index("dp")
    ways = WAYS if n_grp == WAYS else 1
    grp = lax.axis_index("grp") if ways > 1 else 0
    cores = CORES if n_dp % CORES == 0 else 1
    nx = n_dp // cores
    xi, core = dp // cores, lax.rem(dp, cores)
    count, tok, width = v_turn.shape
    q_rot, k_rot = rot.at[0], rot.at[1]
    depth, cols = w_ref.shape
    piece = depth // (chunks * ways)
    per_chunk = count // chunks
    factor = head_size ** (-0.5) * math.log2(math.e)

    def dp_index(xo, co):
        return lax.rem(xi + xo, nx) * cores + lax.rem(core + co, cores)

    direct = chunks - 1
    alone = count - GROUP

    barrier = pltpu.get_barrier_semaphore()
    for here, there in TALKS:
        for one, other in ((here, there), (there, here)):
            @pl.when(me == one)
            def _(other=other):
                pl.semaphore_signal(barrier, inc=1, device_id={"sp": other}, device_id_type=MESH)
    talkers = sum(jnp.where((me == here) | (me == there), 1, 0) for here, there in TALKS)
    for xo in range(1, nx):
        pl.semaphore_signal(barrier, inc=1, device_id={"dp": dp_index(xo, 0)}, device_id_type=MESH)
    for co in range(1, cores):
        pl.semaphore_signal(barrier, inc=1, device_id={"dp": dp_index(0, co)}, device_id_type=MESH)
    if ways > 1:
        pl.semaphore_signal(barrier, inc=1, device_id={"grp": lax.rem(grp + 1, ways)}, device_id_type=MESH)

    own = pl.ds(pl.multiple_of(me * tok, tok), tok)
    loads = [
        pltpu.make_async_copy(qg_in, qg_ref, load_sem.at[6]),
        pltpu.make_async_copy(kg_in, kg_ref, load_sem.at[7]),
        pltpu.make_async_copy(hg_in, hg_ref, load_sem.at[8]),
        pltpu.make_async_copy(lam_in, lam_ref, load_sem.at[9]),
        pltpu.make_async_copy(cos_in.at[own, :], cos_ref, load_sem.at[3]),
        pltpu.make_async_copy(sin_in.at[own, :], sin_ref, load_sem.at[4]),
        pltpu.make_async_copy(q_in.at[0], rows_in.at[0], load_sem.at[0]),
        pltpu.make_async_copy(k_in.at[0], rows_in.at[1], load_sem.at[1]),
        pltpu.make_async_copy(v_in.at[0], rows_in.at[2], load_sem.at[2]),
    ]
    own_weight = pltpu.make_async_copy(w_ref, wfull.at[dp], load_sem.at[5])
    for load in loads:
        load.start()
    own_weight.start()

    def moved(source, target, send_sem, recv_sem, device):
        return pltpu.make_async_remote_copy(
            src_ref=source, dst_ref=target, send_sem=send_sem, recv_sem=recv_sem,
            device_id=device, device_id_type=MESH,
        )

    def piece_rows(r, way):
        first = (r * ways + lax.rem(grp + way, ways)) * piece
        return pl.ds(pl.multiple_of(first, piece), piece)

    def weight_x(xo, r, way=0):
        rows = piece_rows(r, way)
        return moved(
            w_ref.at[rows, :], wfull.at[dp, rows, :], wx_send.at[xo - 1], wx_recv.at[xo - 1, r + way],
            {"dp": dp_index(xo, 0)},
        )

    def weight_x_in(xo, r, way=0):
        block = wfull.at[dp_index(nx - xo, 0), piece_rows(r, way), :]
        return moved(block, block, wx_send.at[xo - 1], wx_recv.at[xo - 1, r + way], {"dp": dp_index(xo, 0)})

    def weight_y(xo, r):
        block = wfull.at[dp_index(nx - xo, 0), piece_rows(r, 0), :]
        return moved(
            block, block, wy_send.at[xo - 1], wy_recv.at[xo - 1, r], {"grp": lax.rem(grp + 1, ways)}
        )

    def weight_y_in(xo, r):
        block = wfull.at[dp_index(nx - xo, 0), piece_rows(r, 1), :]
        return moved(
            block, block, wy_send.at[xo - 1], wy_recv.at[xo - 1, r], {"grp": lax.rem(grp + 1, ways)}
        )

    def weight_core(xo, r, way):
        rows = piece_rows(r, way)
        target = wfull.at[dp_index(nx - xo, 0), rows, :]
        return moved(
            w_ref.at[rows, :] if xo == 0 else target, target,
            wc_send.at[xo], wc_recv.at[xo, r * per_chunk // GROUP], {"dp": dp_index(0, 1)},
        )

    def weight_core_in(xo, g, rows):
        block = wfull.at[dp_index(nx - xo, 1), rows, :]
        return moved(block, block, wc_send.at[xo], wc_recv.at[xo, g], {"dp": dp_index(0, 1)})

    def forward_x(r):
        for xo in range(1, nx):
            weight_x_in(xo, r).wait_recv()
            if ways > 1:
                weight_y(xo, r).start()
            if cores > 1:
                weight_core(xo, r, 0).start()

            @pl.when(r + DEEP < direct)
            def _(xo=xo):
                weight_x(xo, r + DEEP).start()

            for way in range(ways):
                @pl.when(r == max(direct - DEEP, 0) + way)
                def _(xo=xo, way=way):
                    weight_x(xo, direct, way).start()

    def forward_y(r):
        if ways > 1:
            for xo in range(1, nx):
                weight_y_in(xo, r).wait_recv()
                if cores > 1:
                    weight_core(xo, r, 1).start()

    def forward_direct():
        for way in range(ways):
            for xo in range(1, nx):
                weight_x_in(xo, direct, way).wait_recv()
                if cores > 1:
                    weight_core(xo, direct, way).start()

    def big_to(source, lane, slot, h, peer, what=0):
        return moved(source.at[h], big.at[h, slot], big_send.at[lane], came.at[what, h], {"sp": peer})

    def small_to(lane, slot, h, peer, what):
        source = small_out.at[h, min(lane, 1)]
        return moved(source, small.at[h, slot], small_send.at[lane], came.at[what, h], {"sp": peer})

    def came_in(block, what, h):
        moved(block, block, big_send.at[0], came.at[what, h], {"sp": lax.rem(me + 1, n)}).wait_recv()

    def gone(block, sem):
        moved(block, block, sem, came.at[0, 0], {"sp": lax.rem(me + 1, n)}).wait_send()

    lane = lax.broadcasted_iota(jnp.int32, (1, width), 1)
    low_map = lane < head_size
    half = head_size // 2
    down, across = (lax.broadcasted_iota(jnp.int32, (width, width), axis) for axis in range(2))
    partner = jnp.where(lax.rem(across, head_size) < half, across + half, across - half)
    swap = jnp.where(down == partner, 1.0, 0.0).astype(jnp.bfloat16)
    same_map = jnp.where((down < head_size) == (across < head_size), 1.0, 0.0).astype(jnp.bfloat16)
    sums = jnp.concatenate([same_map, same_map], axis=0)

    def norm_rotate(which, first):
        blocks = [rows_in[which, :, head_columns(first + i)] for i in range(GROUP)]
        stacked = jnp.concatenate(blocks, axis=0)
        x = stacked.astype(jnp.float32)
        square = x * x
        coarse = square.astype(jnp.bfloat16)
        fine = (square - coarse.astype(jnp.float32)).astype(jnp.bfloat16)
        total_square = jnp.dot(jnp.concatenate([coarse, fine], axis=1), sums, preferred_element_type=jnp.float32)
        other = jnp.dot(stacked, swap, preferred_element_type=jnp.float32)
        inverse = lax.rsqrt(total_square * (1.0 / head_size) + EPSILON)
        for i in range(GROUP):
            part = slice(i * tok, (i + 1) * tok)
            straight = x[part] * inverse[part] * turn_ref[2 * which]
            turned = other[part] * inverse[part] * turn_ref[2 * which + 1]
            rot[which, first + i] = (straight + turned).astype(jnp.bfloat16)

    for load in loads[:7]:
        load.wait()
    gain_turn[...] = jnp.broadcast_to(hg_ref[...], (tok, width)).T
    for which, gain in enumerate((qg_ref, kg_ref)):
        gain = gain[...]
        crossed = jnp.concatenate([gain[:, half:], gain[:, :half]], axis=1)
        turn_ref[2 * which] = cos_ref[...] * jnp.concatenate([gain, gain], axis=1)
        turn_ref[2 * which + 1] = sin_ref[...] * jnp.concatenate([crossed, crossed], axis=1)
    causal = lax.broadcasted_iota(jnp.int32, (tok, 2 * tok), 0) <= lax.rem(
        lax.broadcasted_iota(jnp.int32, (tok, 2 * tok), 1), tok
    )

    def head_columns(h):
        return pl.ds(pl.multiple_of(h * width, width), width)

    def turned_scores(keys, *queries):
        both = []
        for q in queries:
            zero = jnp.zeros_like(q)
            both += [jnp.where(low_map, q, zero), jnp.where(low_map, zero, q)]
        both = jnp.concatenate(both, axis=0)
        return lax.dot_general(keys, both, (((1,), (1,)), ((), ())), preferred_element_type=jnp.float32)

    def exponents(scores):
        top = jnp.max(scores, axis=0, keepdims=True)
        e = jnp.exp2((scores - top) * factor)
        return top * factor, e, jnp.sum(e, axis=0, keepdims=True)

    def mixing_of(e, scale, lam):
        one, two = scale[:, :tok], scale[:, tok:] * lam
        return (e[:, :tok] * one - e[:, tok:] * two).astype(jnp.bfloat16)

    def mixed(e, scale, lam, values):
        return jnp.dot(values, mixing_of(e, scale, lam), preferred_element_type=jnp.float32)

    def put_pair(ref, h, slot, pair):
        ref[h, slot, 0:1, :] = pair[:, :tok]
        ref[h, slot, 1:2, :] = pair[:, tok:]

    def get_pair(ref, h, slot):
        return jnp.concatenate([ref[h, slot, 0:1, :], ref[h, slot, 1:2, :]], axis=1)

    def joined(levels):
        top = functools.reduce(jnp.maximum, levels)
        return top + jnp.log2(functools.reduce(jnp.add, [jnp.exp2(l - top) for l in levels]))

    def finish(raw, h):
        scaled = raw * lax.rsqrt(jnp.mean(raw * raw, axis=0, keepdims=True) + EPSILON)
        result = (scaled * gain_turn[...] * OUT_SCALE).T
        heads[:, head_columns(h)] = result.astype(jnp.bfloat16)

    def partial_scores(keys, queries, slot, first, masked):
        scores = [turned_scores(k, q) for k, q in zip(keys, queries)]
        if masked:
            scores = [jnp.where(causal, s, -1e30) for s in scores]
        parts = [exponents(s) for s in scores]
        for i, (top, e, z) in enumerate(parts):
            kept[first + i, slot] = e
            put_pair(kept_top, first + i, slot, top)
            put_pair(small_out, first + i, slot, top + jnp.log2(z))

    def third_queries(h):
        big_to(q_rot, 1, 3, h, 2).start()
        big_to(q_rot, 0, 3, h, 1, 2).start()

    members = range(GROUP)
    ahead = jnp.where(me == 0, 1, 0)

    def begin(j, carry):
        first = j * GROUP

        @pl.when(j == 0)
        def _():
            loads[7].wait()
            loads[8].wait()

        norm_rotate(ahead, first)
        for i in members:
            v_turn[first + i] = rows_in[2, :, head_columns(first + i)].astype(jnp.float32).T.astype(jnp.bfloat16)
        return carry

    def spread(j, carry):
        first = j * GROUP

        @pl.when((me == 3) & (j == 0))
        def _():
            third_queries(0)

        @pl.when((me == 2) & (j == 0))
        def _():
            big_to(q_rot, 0, 2, 0, 1).start()

        @pl.when(me == 0)
        def _():
            for i in members:
                big_to(k_rot, 0, 0, first + i, 1).start()
                big_to(v_turn, 1, 1, first + i, 1).start()

        norm_rotate(1 - ahead, first)

        @pl.when((me == 2) & (first >= alone))
        def _():
            for i in members:
                big_to(k_rot, 2, 2, first + i, 3, 2).start()
                big_to(v_turn, 2, 3, first + i, 3, 2).start()

        @pl.when((me == 2) | ((me == 3) & (first < alone)))
        def _():
            partial_scores([k_rot[first + i] for i in members], [q_rot[first + i] for i in members], 0, first, True)

        @pl.when(me == 2)
        def _():
            for i in members:
                small_to(0, 0, first + i, 1, 1).start()

        @pl.when((me == 2) & (j == 0))
        def _():
            for i in range(1, AHEAD):
                big_to(q_rot, 0, 2, i, 1).start()

        @pl.when((me == 3) & (first < alone))
        def _():
            for i in members:
                if i:
                    third_queries(first + i)
                else:
                    @pl.when(j > 0)
                    def _():
                        third_queries(first)
                small_to(0, 1, first + i, 1, 3).start()

        return carry

    lax.fori_loop(0, 1, begin, 0)
    pl.semaphore_wait(barrier, talkers + (nx - 1) + (cores - 1) + (ways - 1))
    for r in range(min(DEEP, direct)):
        for xo in range(1, nx):
            weight_x(xo, r).start()
    if cores > 1:
        for r in range(chunks):
            for way in range(ways):
                weight_core(0, r, way).start()

    lax.fori_loop(0, 1, spread, 0)
    lax.fori_loop(1, count // GROUP, lambda j, carry: spread(j, begin(j, carry)), 0)

    @pl.when(me == 1)
    def _():
        for h in range(alone, count):
            small[h, 2] = jnp.full((2, tok), -1e30, jnp.float32)

    def lowest(h):
        scores = jnp.where(causal, turned_scores(k_rot[h], q_rot[h]), -1e30)
        _, e, z = exponents(scores)
        finish(mixed(e, 1.0 / z, lam_ref[h], v_turn[h]), h)

    def centre(h, third):
        if h is not None:
            came_in(big.at[h, 0:3], 0, h)
            came_in(small.at[h, 0], 1, h)
        if third is not None:
            came_in(big.at[third, 3], 2, third)

            @pl.when(third < alone)
            def _():
                came_in(small.at[third, 1:3], 3, third)

            @pl.when(third >= alone)
            def _():
                came_in(small.at[third, 1], 3, third)

        pair = 2 * tok
        scores, levels, places, values = [], [], [], []
        for place, x in ((1, h), (2, h), (3, third)):
            if x is None:
                continue
            keys = jnp.concatenate([big[x, 0], k_rot[x]], axis=0)
            values.append(jnp.concatenate([big[x, 1], v_turn[x]], axis=1))
            part = turned_scores(keys, q_rot[x] if place == 1 else big[x, place])
            if place == 1:
                part = jnp.concatenate([part[:tok], jnp.where(causal, part[tok:], -1e30)], axis=0)
            scores.append(part)
            levels.append([get_pair(small, x, slot) for slot in ((), (0,), (1, 2))[place - 1]])
            places.append((place, x))
        parts = [exponents(part) for part in scores]
        scales = []
        for (place, x), (top, e, z), others in zip(places, parts, levels):
            if place == 1:
                scales.append(1.0 / z)
            else:
                level = joined([top + jnp.log2(z)] + others)
                put_pair(small_out, x, place - 2, level)
                scales.append(jnp.exp2(top - level))
        mixing = [mixing_of(e, scale, lam_ref[x]) for (_, x), (_, e, _), scale in zip(places, parts, scales)]
        raws = [jnp.dot(v, m, preferred_element_type=jnp.float32) for v, m in zip(values, mixing)]
        for (place, x), raw in zip(places, raws):
            if place > 1:
                big_out[place - 2, x] = raw.astype(jnp.bfloat16)
        if third is not None:
            @pl.when(third < alone)
            def _():
                small_to(1, 1, third, 2, 3).start()

            small_to(2, 1, third, 3, 1).start()
        if h is not None:
            small_to(0, 0, h, 2, 1).start()
        if third is not None:
            big_to(big_out.at[1], 1, 0, third, 3).start()
        if h is not None:
            big_to(big_out.at[0], 0, 0, h, 2, 2).start()
            finish(raws[0], h)

    def upper_scores(h):
        @pl.when(h < alone)
        def _():
            came_in(big.at[h, 3], 0, h)
            partial_scores([k_rot[h]], [big[h, 3]], 1, h, False)
            small_to(1, 2, h, 1, 3).start()

        @pl.when(h + AHEAD < count)
        def _():
            big_to(q_rot, 0, 2, h + AHEAD, 1).start()

    def upper_raw(h, slot, level):
        scale = jnp.exp2(get_pair(kept_top, h, slot) - level)
        return mixed(kept[h, slot], scale, lam_ref[h], v_turn[h])

    def upper_help(h):
        came_in(small.at[h, 1], 3, h)
        big_out[1, h] = upper_raw(h, 1, get_pair(small, h, 1)).astype(jnp.bfloat16)
        big_to(big_out.at[1], 1, 1, h, 3).start()

    def upper_second(h):
        came_in(small.at[h, 0], 1, h)
        came_in(big.at[h, 0], 2, h)
        finish(upper_raw(h, 0, get_pair(small, h, 0)) + big[h, 0].astype(jnp.float32), h)

    def joint_scores(h):
        came_in(big.at[h, 2:4], 2, h)
        scores = turned_scores(jnp.concatenate([big[h, 2], k_rot[h]], axis=0), q_rot[h])
        scores = jnp.concatenate([scores[:tok], jnp.where(causal, scores[tok:], -1e30)], axis=0)
        top, e, z = exponents(scores)
        kept[h, 0] = e[:tok]
        kept[h, 1] = e[tok:]
        put_pair(kept_top, h, 0, top)
        put_pair(small_out, h, 0, top + jnp.log2(z))

    def upper_third(h):
        came_in(small.at[h, 1], 1, h)

        @pl.when(h < alone)
        def _():
            came_in(big.at[h, 0:2], 0, h)
            raw = upper_raw(h, 0, get_pair(small, h, 1)) + big[h, 0].astype(jnp.float32)
            finish(raw + big[h, 1].astype(jnp.float32), h)

        @pl.when(h >= alone)
        def _():
            came_in(big.at[h, 0], 0, h)
            scale = jnp.exp2(get_pair(kept_top, h, 0) - get_pair(small, h, 1))
            e = jnp.concatenate([kept[h, 0], kept[h, 1]], axis=0)
            values = jnp.concatenate([big[h, 3], v_turn[h]], axis=1)
            finish(mixed(e, scale, lam_ref[h], values) + big[h, 0].astype(jnp.float32), h)

    group = GROUP

    def project(g, first, last):
        step = group * width
        rows = pl.ds(g * step, step) if isinstance(g, int) else pl.ds(pl.multiple_of(g * step, step), step)
        if cores > 1:
            for xo in range(nx):
                weight_core_in(xo, g, rows).wait_recv()
        block = heads[:, rows]
        for index in range(n_dp):
            term = jnp.dot(block, wfull[index, rows, :], preferred_element_type=jnp.float32)
            span = slice(index * cols, (index + 1) * cols)
            if not first:
                term = total[:, span] + term
            if last:
                out_ref[0, :, span] = term.astype(out_ref.dtype)
            else:
                total[:, span] = term

    groups = count // group

    def turned_order(at):
        early = (at >= alone - SWAP) & (at < alone)
        late = (at >= alone) & (at < alone + SWAP)
        return at + jnp.where(early, SWAP, jnp.where(late, -SWAP, 0))


    first_x = jnp.where(me == 1, 2, 1)
    first_y = first_x + 2 * per_chunk
    last_x = first_x + direct * per_chunk

    def step(it, carry):
        @pl.when((me == 2) & (it < count))
        def _():
            upper_scores(it)

        turn = lax.rem(it - first_x + per_chunk, per_chunk) == 0

        @pl.when(turn & (it >= first_x) & (it < last_x))
        def _():
            forward_x((it - first_x) // per_chunk)

        @pl.when(turn & (it >= first_y) & (it < first_y + direct * per_chunk))
        def _():
            forward_y((it - first_y) // per_chunk)

        @pl.when(it == jnp.where(me < 2, last_x, HELP + alone + 1))
        def _():
            forward_direct()

        @pl.when((me == 0) & (it < count))
        def _():
            lowest(it)

        @pl.when((me == 1) & (it < BEHIND))
        def _():
            centre(it, None)

        @pl.when((me == 1) & (it >= BEHIND) & (it < count))
        def _():
            centre(it, jnp.where(it == count - 1, it - 1, it - BEHIND))

        @pl.when((me == 1) & (it >= count - BEHIND) & (it < count))
        def _():
            centre(None, jnp.where(it == count - 1, it, it - 1))

        @pl.when((me == 2) & (it >= HELP) & (it < HELP + alone))
        def _():
            upper_help(it - HELP)

        @pl.when((me == 2) & (it >= NEAR) & (it < NEAR + count))
        def _():
            upper_second(it - NEAR)

        @pl.when((me == 3) & (it >= GROUP) & (it < 2 * GROUP))
        def _():
            joint_scores(alone + it - GROUP)

        for i in range(GROUP):
            @pl.when((me == 3) & (it == LAG + SPREAD + min(i, PACED)))
            def _(i=i):
                big_to(q_rot, 0, 3, alone + i, 1, 2).start()
                small_to(0, 1, alone + i, 1, 3).start()

        @pl.when((me == 3) & (it >= LAG))
        def _():
            upper_third(turned_order(it - LAG))

        for g in range(groups - 1):
            @pl.when(it == g * group + PROJECT + jnp.where(me == 3, 3, jnp.where((me == 1) & (g == 1), 2, 0)))
            def _(g=g):
                if g == 0:
                    own_weight.wait()
                project(g, g == 0, False)

        return carry

    lax.fori_loop(0, count + LAG, step, 0)
    project(groups - 1, False, True)

    whole, most = q_rot.at[:], q_rot.at[0:alone]
    rows = small_out.at[:, 0]
    most_rows = small_out.at[0:alone, 0]

    @pl.when(me == 0)
    def _():
        gone(whole, big_send.at[0])
        gone(whole, big_send.at[1])

    @pl.when(me == 1)
    def _():
        gone(whole, big_send.at[0])
        gone(whole, big_send.at[1])
        gone(rows, small_send.at[0])
        gone(most_rows, small_send.at[1])
        gone(rows, small_send.at[2])

    @pl.when(me == 2)
    def _():
        gone(whole, big_send.at[0])
        gone(most, big_send.at[1])
        gone(q_rot.at[0 : 2 * GROUP], big_send.at[2])
        gone(rows, small_send.at[0])
        gone(most_rows, small_send.at[1])

    @pl.when(me == 3)
    def _():
        gone(whole, big_send.at[0])
        gone(most, big_send.at[1])
        gone(rows, small_send.at[0])

    for xo in range(nx):
        if xo:
            sent_x = wfull.at[0, 0 : (direct + ways) * piece, :]
            moved(sent_x, sent_x, wx_send.at[xo - 1], wx_recv.at[0, 0], {"dp": dp_index(xo, 0)}).wait_send()
            if ways > 1:
                sent_y = wfull.at[0, 0 : direct * piece, :]
                moved(sent_y, sent_y, wy_send.at[xo - 1], wy_recv.at[0, 0], {"dp": dp_index(xo, 0)}).wait_send()
        if cores > 1:
            sent_core = wfull.at[0]
            moved(sent_core, sent_core, wc_send.at[xo], wc_recv.at[0, 0], {"dp": dp_index(0, 1)}).wait_send()


def split_local(n, n_dp, n_grp, query_rows, key_rows, value_rows, query_gain, key_gain, lambdas, head_gain, out_weight):
    tok = query_rows.shape[1]
    head_size = query_gain.shape[0]
    width = head_gain.shape[0]
    count = lambdas.shape[0]
    depth, cols = out_weight.shape
    ways = WAYS if n_grp == WAYS else 1
    chunks = count // ways
    cores = CORES if n_dp % CORES == 0 else 1
    nx = n_dp // cores
    cosine, sine = rotation_tables(tok * n, head_size)
    anywhere = pl.BlockSpec(memory_space=pl.ANY)
    vmem = pl.BlockSpec(memory_space=pltpu.VMEM)
    dma = pltpu.SemaphoreType.DMA
    across = max(nx - 1, 1)
    return pl.pallas_call(
        functools.partial(split_kernel, n, n_dp, n_grp, head_size, chunks),
        out_shape=pltpu.VMEM((1, tok, n_dp * cols), jnp.bfloat16),
        in_specs=[anywhere] * 3
        + [anywhere] * 7,
        out_specs=vmem,
        scratch_shapes=[
            pltpu.VMEM((tok, n_dp * cols), jnp.float32),
            pltpu.VMEM((3, tok, count * width), jnp.bfloat16),
            pltpu.VMEM((2, count, tok, width), jnp.bfloat16),
            pltpu.VMEM((count, tok, width), jnp.bfloat16),
            pltpu.VMEM((count, 4, tok, width), jnp.bfloat16),
            pltpu.VMEM((count, 3, 2, tok), jnp.float32),
            pltpu.VMEM((2, count, tok, width), jnp.bfloat16),
            pltpu.VMEM((count, 2, 2, tok), jnp.float32),
            pltpu.VMEM((count, 2, tok, 2 * tok), jnp.float32),
            pltpu.VMEM((count, 2, 2, tok), jnp.float32),
            pltpu.VMEM((width, tok), jnp.float32),
            pltpu.VMEM((tok, count * width), jnp.bfloat16),
            pltpu.VMEM((n_dp, depth, cols), jnp.bfloat16),
            pltpu.VMEM((tok, width), jnp.float32),
            pltpu.VMEM((tok, width), jnp.float32),
            pltpu.VMEM((4, tok, width), jnp.float32),
            pltpu.VMEM((1, head_size), jnp.float32),
            pltpu.VMEM((1, head_size), jnp.float32),
            pltpu.SMEM((count,), jnp.float32),
            pltpu.VMEM((1, width), jnp.float32),
            dma((10,)),
            dma((3,)),
            dma((3,)),
            dma((4, count)),
            dma((across,)),
            dma((across, chunks - 1 + ways)),
            dma((across,)),
            dma((across, chunks)),
            dma((nx,)),
            dma((nx, count // GROUP)),
        ],
        compiler_params=pltpu.CompilerParams(
            collective_id=0, has_side_effects=True, vmem_limit_bytes=56 * 1024 * 1024
        ),
    )(
        query_rows, key_rows, value_rows,
        query_gain[None, :], key_gain[None, :], lambdas, head_gain[None, :],
        out_weight, jnp.asarray(cosine), jnp.asarray(sine),
    )


def plan(n, tok, width, count, n_grp):
    ways = WAYS if n_grp == WAYS else 1
    fits = n == PARTS and tok == width and count % (GROUP * ways) == 0
    return split_local if fits else local


def solution(mesh):
    rows = P(("grp", "dp"), "sp", None)
    n, n_dp, n_grp = mesh.shape["sp"], mesh.shape["dp"], mesh.shape["grp"]

    def body(*args):
        chosen = plan(n, args[0].shape[1], args[6].shape[0], args[5].shape[0], n_grp)
        return chosen(n, n_dp, n_grp, *args)

    return jax.shard_map(
        body,
        mesh=mesh,
        in_specs=(rows, rows, rows, P(), P(), P(), P(), P(None, "dp")),
        out_specs=rows,
        check_vma=False,
    )
```

```python
import functools
import math

import jax
import jax.numpy as jnp
import numpy as np
from jax import lax
from jax.experimental import pallas as pl
from jax.experimental.pallas import tpu as pltpu
from jax.sharding import PartitionSpec as P

EPSILON = 1e-06
OUT_SCALE = 0.8
CORES = 2
CHUNKS = 2
WAYS = 2
PARTS = 4
GROUP = 4
LAG = 7
AHEAD = 3
DEEP = 3
PACES = (4, 4, 5, 6)
BEHIND = 2
NEAR = 4
HELP = 4
PROJECT = 10
SWAP = 0
LATE = 0
TALKS = ((0, 1), (1, 2), (1, 3), (2, 3))
MESH = pl.DeviceIdType.MESH


def rotation_tables(length, head_size):
    half = head_size // 2
    inverse = np.float32(10000.0) ** (-np.arange(half, dtype=np.float32) / np.float32(half))
    angles = np.arange(length, dtype=np.float32)[:, None] * inverse.astype(np.float32)[None, :]
    cosine, sine = np.cos(angles), np.sin(angles)
    return (
        np.concatenate([cosine] * 4, axis=1).astype(np.float32),
        np.concatenate([-sine, sine] * 2, axis=1).astype(np.float32),
    )


def kernel(
    n, n_dp, n_grp, head_size, q_ref, k_ref, v_ref, qg_ref, kg_ref, lam_ref, hg_ref, w_ref, cos_in, sin_in,
    out_ref, total, rx, rot_q, rot_k, heads_out, hrx, wfull,
    in_send, in_recv, ret_send, ret_recv, wx_send, wx_recv, wy_send, wy_recv, wc_send, wc_recv, own_sem, cos_ref, sin_ref, table_sem,
):
    me = lax.axis_index("sp")
    dp = lax.axis_index("dp")
    ways = WAYS if n_grp == WAYS else 1
    grp = lax.axis_index("grp") if ways > 1 else 0
    cores = CORES if n_dp % CORES == 0 else 1
    nx = n_dp // cores
    xi, core = dp // cores, lax.rem(dp, cores)
    tok = q_ref.shape[1]
    width = 2 * head_size
    local_heads = rx.shape[1]
    length = rx.shape[2]
    depth = w_ref.shape[0]
    cols = w_ref.shape[1]
    piece = depth // (CHUNKS * ways)

    def sp_peer(off):
        return lax.rem(me + off, n)

    def dp_index(xo, co):
        return lax.rem(xi + xo, nx) * cores + lax.rem(core + co, cores)

    barrier = pltpu.get_barrier_semaphore()
    for off in range(1, n):
        pl.semaphore_signal(barrier, inc=1, device_id={"sp": sp_peer(off)}, device_id_type=MESH)
    for xo in range(1, nx):
        pl.semaphore_signal(barrier, inc=1, device_id={"dp": dp_index(xo, 0)}, device_id_type=MESH)
    for co in range(1, cores):
        pl.semaphore_signal(barrier, inc=1, device_id={"dp": dp_index(0, co)}, device_id_type=MESH)

    if ways > 1:
        pl.semaphore_signal(
            barrier, inc=1, device_id={"grp": lax.rem(grp + 1, ways)}, device_id_type=MESH
        )

    sources = (k_ref, q_ref, v_ref)

    def own_rows(t, j):
        column = pl.multiple_of((me * local_heads + j) * width, width)
        return pltpu.make_async_copy(
            sources[t].at[0, :, pl.ds(column, width)],
            rx.at[t, j, pl.ds(pl.multiple_of(me * tok, tok), tok), :],
            in_recv.at[t, j, 0],
        )

    def rows_to(t, j, off):
        peer = sp_peer(off)
        column = pl.multiple_of((peer * local_heads + j) * width, width)
        return pltpu.make_async_remote_copy(
            src_ref=sources[t].at[0, :, pl.ds(column, width)],
            dst_ref=rx.at[t, j, pl.ds(pl.multiple_of(me * tok, tok), tok), :],
            send_sem=in_send.at[t, j, off],
            recv_sem=in_recv.at[t, j, off],
            device_id={"sp": peer},
            device_id_type=MESH,
        )

    def rows_from(t, j, off):
        peer = lax.rem(me + n - off, n)
        block = rx.at[t, j, pl.ds(pl.multiple_of(peer * tok, tok), tok), :]
        return pltpu.make_async_remote_copy(
            src_ref=block, dst_ref=block, send_sem=in_send.at[t, j, off],
            recv_sem=in_recv.at[t, j, off], device_id={"sp": peer}, device_id_type=MESH,
        )

    def piece_rows(r, way):
        first = (r * ways + lax.rem(grp + way, ways)) * piece
        return pl.ds(pl.multiple_of(first, piece), piece)

    def moved(source, target, send_sem, recv_sem, device):
        return pltpu.make_async_remote_copy(
            src_ref=source, dst_ref=target, send_sem=send_sem, recv_sem=recv_sem,
            device_id=device, device_id_type=MESH,
        )

    def weight_x(xo, r):
        rows = piece_rows(r, 0)
        return moved(
            w_ref.at[rows, :], wfull.at[dp, rows, :], wx_send.at[xo, r], wx_recv.at[xo, r],
            {"dp": dp_index(xo, 0)},
        )

    def weight_x_in(xo, r):
        block = wfull.at[dp_index(nx - xo, 0), piece_rows(r, 0), :]
        return moved(block, block, wx_send.at[xo, r], wx_recv.at[xo, r], {"dp": dp_index(xo, 0)})

    def weight_y(xo, r):
        block = wfull.at[dp_index(nx - xo, 0), piece_rows(r, 0), :]
        return moved(block, block, wy_send.at[xo, r], wy_recv.at[xo, r], {"grp": lax.rem(grp + 1, ways)})

    def weight_y_in(xo, r):
        block = wfull.at[dp_index(nx - xo, 0), piece_rows(r, 1), :]
        return moved(block, block, wy_send.at[xo, r], wy_recv.at[xo, r], {"grp": lax.rem(grp + 1, ways)})

    def weight_core(xo, r, way):
        rows = piece_rows(r, way)
        target = wfull.at[dp_index(nx - xo, 0), rows, :]
        return moved(
            w_ref.at[rows, :] if xo == 0 else target, target,
            wc_send.at[xo, r, way], wc_recv.at[xo, r, way], {"dp": dp_index(0, 1)},
        )

    def weight_core_in(xo, r, way):
        block = wfull.at[dp_index(nx - xo, 1), piece_rows(r, way), :]
        return moved(
            block, block, wc_send.at[xo, r, way], wc_recv.at[xo, r, way], {"dp": dp_index(0, 1)}
        )

    own_weight = pltpu.make_async_copy(w_ref, wfull.at[dp], own_sem)
    own_weight.start()
    tables = [
        pltpu.make_async_copy(cos_in, cos_ref, table_sem.at[0]),
        pltpu.make_async_copy(sin_in, sin_ref, table_sem.at[1]),
    ]
    for table in tables:
        table.start()
    for j in range(local_heads):
        for t in range(3):
            own_rows(t, j).start()
    pl.semaphore_wait(barrier, (n - 1) + (nx - 1) + (cores - 1) + (ways - 1))
    for j in range(local_heads):
        for t in range(3):
            for off in range(1, n):
                rows_to(t, j, off).start()
        if j == 0:
            for r in range(CHUNKS):
                for xo in range(1, nx):
                    weight_x(xo, r).start()
            if cores > 1:
                for r in range(CHUNKS):
                    for way in range(ways):
                        weight_core(0, r, way).start()

    lane = lax.broadcasted_iota(jnp.int32, (1, width), 1)
    low_map = lane < head_size
    low_half = lax.rem(lane, head_size) < head_size // 2

    def norm_rotate(block, gain):
        x = block.astype(jnp.float32)
        square = x * x
        low = jnp.sum(jnp.where(low_map, square, 0.0), axis=1, keepdims=True)
        high = jnp.sum(jnp.where(low_map, 0.0, square), axis=1, keepdims=True)
        low = lax.rsqrt(low * (1.0 / head_size) + EPSILON)
        high = lax.rsqrt(high * (1.0 / head_size) + EPSILON)
        y = x * jnp.where(low_map, low, high) * gain
        quarter = head_size // 2
        turned = jnp.where(low_half, pltpu.roll(y, width - quarter, 1), pltpu.roll(y, quarter, 1))
        return (y * cos_ref[...] + turned * sin_ref[...]).astype(jnp.bfloat16)

    def heads_to(j, i):
        column = pl.multiple_of(me * width, width)
        off = lax.rem(i + n - me, n)
        return pltpu.make_async_remote_copy(
            src_ref=heads_out.at[j, i], dst_ref=hrx.at[j, :, pl.ds(column, width)],
            send_sem=ret_send.at[j, off], recv_sem=ret_recv.at[j, off],
            device_id={"sp": i}, device_id_type=MESH,
        )

    def heads_from(j, off):
        peer = lax.rem(me + n - off, n)
        column = pl.multiple_of(peer * width, width)
        block = hrx.at[j, :, pl.ds(column, width)]
        return pltpu.make_async_remote_copy(
            src_ref=block, dst_ref=block, send_sem=ret_send.at[j, off],
            recv_sem=ret_recv.at[j, off], device_id={"sp": peer}, device_id_type=MESH,
        )

    groups = math.gcd(n, 4)
    per_group = n // groups
    segment = length // groups
    factor = head_size ** (-0.5) * math.log2(math.e)
    contract = (((1,), (1,)), ((), ()))

    def query_block(j, g, i, lam):
        rows = pl.ds(i * tok, tok) if isinstance(i, int) else pl.ds(pl.multiple_of(i * tok, tok), tok)
        q = rot_q[rows, :]
        zero = jnp.zeros_like(q)
        both = jnp.concatenate([jnp.where(low_map, q, zero), jnp.where(low_map, zero, q)], axis=0)
        start = g * segment
        spans = ([(0, start)] if g else []) + [(start, segment)]
        parts = []
        for first, size in spans:
            scores = lax.dot_general(
                both, rot_k[first : first + size, :], contract, preferred_element_type=jnp.float32
            )
            if first == start:
                shape = (2 * tok, size)
                row = lax.rem(lax.broadcasted_iota(jnp.int32, shape, 0), tok) + i * tok
                column = lax.broadcasted_iota(jnp.int32, shape, 1) + first
                scores = jnp.where(column <= row, scores, -1e30)
            parts.append(scores)
        top = functools.reduce(jnp.maximum, [jnp.max(s, axis=1, keepdims=True) for s in parts])
        parts = [jnp.exp2((s - top) * factor) for s in parts]
        total = functools.reduce(jnp.add, [jnp.sum(e, axis=1, keepdims=True) for e in parts])
        inverse = 1.0 / total
        one, two = inverse[:tok], inverse[tok:] * lam
        raw = None
        for (first, size), e in zip(spans, parts):
            mixing = (e[:tok] * one - e[tok:] * two).astype(jnp.bfloat16)
            term = jnp.dot(mixing, rx[2, j, first : first + size, :], preferred_element_type=jnp.float32)
            raw = term if raw is None else raw + term
        scaled = raw * lax.rsqrt(jnp.mean(raw * raw, axis=1, keepdims=True) + EPSILON)
        result = (scaled * hg_ref[...] * OUT_SCALE).astype(jnp.bfloat16)

        @pl.when(i == me)
        def _():
            hrx[j, :, pl.ds(pl.multiple_of(me * width, width), width)] = result

        @pl.when(i != me)
        def _():
            heads_out[j, i] = result
            heads_to(j, i).start()

    def forward(stage):
        if stage < CHUNKS:
            for xo in range(1, nx):
                weight_x_in(xo, stage).wait_recv()
                if ways > 1:
                    weight_y(xo, stage).start()
                if cores > 1:
                    weight_core(xo, stage, 0).start()
        elif ways > 1:
            for xo in range(1, nx):
                weight_y_in(xo, stage - CHUNKS).wait_recv()
                if cores > 1:
                    weight_core(xo, stage - CHUNKS, 1).start()

    for table in tables:
        table.wait()
    for j in range(local_heads):
        lam = lam_ref[me * local_heads + j]
        for t, (target, gain) in enumerate(((rot_k, kg_ref), (rot_q, qg_ref), (None, None))):
            own_rows(t, j).wait()
            for off in range(1, n):
                rows_from(t, j, off).wait_recv()
            if target is not None:
                target[...] = norm_rotate(rx[t, j], jnp.concatenate([gain[...]] * 2, axis=1))
        for g in range(groups):
            if per_group == 1:
                query_block(j, g, g, lam)
            else:
                def step(b, carry, j=j, g=g, lam=lam):
                    query_block(j, g, g * per_group + b, lam)
                    return carry
                lax.fori_loop(0, per_group, step, 0)
        for stage in range(2 * CHUNKS):
            if j == min(stage, local_heads - 1):
                forward(stage)

    own_weight.wait()
    if cores > 1:
        for xo in range(nx):
            for r in range(CHUNKS):
                for way in range(ways):
                    weight_core_in(xo, r, way).wait_recv()

    for j in range(local_heads):
        for off in range(1, n):
            heads_from(j, off).wait_recv()
        rows = hrx[j]
        for index in range(n_dp):
            matching = jnp.concatenate(
                [wfull[index, pl.ds((s * local_heads + j) * width, width), :] for s in range(n)], axis=0
            )
            term = jnp.dot(rows, matching, preferred_element_type=jnp.float32)
            span = slice(index * cols, (index + 1) * cols)
            if j:
                term = total[:, span] + term
            if j == local_heads - 1:
                out_ref[0, :, span] = term.astype(out_ref.dtype)
            else:
                total[:, span] = term

    for j in range(local_heads):
        for off in range(1, n):
            for t in range(3):
                rows_to(t, j, off).wait_send()
            heads_to(j, sp_peer(off)).wait_send()
    for r in range(CHUNKS):
        for xo in range(nx):
            if xo:
                weight_x(xo, r).wait_send()
                if ways > 1:
                    weight_y(xo, r).wait_send()
            if cores > 1:
                for way in range(ways):
                    weight_core(xo, r, way).wait_send()


def local(n, n_dp, n_grp, query_rows, key_rows, value_rows, query_gain, key_gain, lambdas, head_gain, out_weight):
    tok = query_rows.shape[1]
    head_size = query_gain.shape[0]
    width = head_gain.shape[0]
    local_heads = lambdas.shape[0] // n
    length = tok * n
    depth, cols = out_weight.shape
    cores = CORES if n_dp % CORES == 0 else 1
    nx = n_dp // cores
    cosine, sine = rotation_tables(length, head_size)
    anywhere = pl.BlockSpec(memory_space=pl.ANY)
    vmem = pl.BlockSpec(memory_space=pltpu.VMEM)
    dma = pltpu.SemaphoreType.DMA
    return pl.pallas_call(
        functools.partial(kernel, n, n_dp, n_grp, head_size),
        out_shape=jax.ShapeDtypeStruct((1, tok, n_dp * cols), jnp.bfloat16),
        in_specs=[anywhere] * 3
        + [vmem, vmem, pl.BlockSpec(memory_space=pltpu.SMEM), vmem, anywhere, anywhere, anywhere],
        out_specs=vmem,
        scratch_shapes=[
            pltpu.VMEM((tok, n_dp * cols), jnp.float32),
            pltpu.VMEM((3, local_heads, length, width), jnp.bfloat16),
            pltpu.VMEM((length, width), jnp.bfloat16),
            pltpu.VMEM((length, width), jnp.bfloat16),
            pltpu.VMEM((local_heads, n, tok, width), jnp.bfloat16),
            pltpu.VMEM((local_heads, tok, n * width), jnp.bfloat16),
            pltpu.VMEM((n_dp, depth, cols), jnp.bfloat16),
            dma((3, local_heads, n)),
            dma((3, local_heads, n)),
            dma((local_heads, n)),
            dma((local_heads, n)),
            dma((nx, CHUNKS)),
            dma((nx, CHUNKS)),
            dma((nx, CHUNKS)),
            dma((nx, CHUNKS)),
            dma((nx, CHUNKS, WAYS)),
            dma((nx, CHUNKS, WAYS)),
            dma(()),
            pltpu.VMEM((length, width), jnp.float32),
            pltpu.VMEM((length, width), jnp.float32),
            dma((2,)),
        ],
        compiler_params=pltpu.CompilerParams(
            collective_id=0, has_side_effects=True, vmem_limit_bytes=56 * 1024 * 1024
        ),
    )(
        query_rows, key_rows, value_rows,
        query_gain[None, :], key_gain[None, :], lambdas, head_gain[None, :],
        out_weight, jnp.asarray(cosine), jnp.asarray(sine),
    )


def split_kernel(
    n, n_dp, n_grp, head_size, chunks, q_in, k_in, v_in, qg_in, kg_in, lam_in, hg_in, w_ref, cos_in, sin_in,
    out_ref, total, rows_in, rot, v_turn, big, small, big_out, small_out, kept, kept_top, gain_turn, heads, wfull,
    cos_ref, sin_ref, turn_ref, qg_ref, kg_ref, lam_ref, hg_ref, load_sem, big_send, small_send, came, wx_send, wx_recv, wy_send, wy_recv, wc_send, wc_recv,
):
    me = lax.axis_index("sp")
    dp = lax.axis_index("dp")
    ways = WAYS if n_grp == WAYS else 1
    grp = lax.axis_index("grp") if ways > 1 else 0
    cores = CORES if n_dp % CORES == 0 else 1
    nx = n_dp // cores
    xi, core = dp // cores, lax.rem(dp, cores)
    count, tok, width = v_turn.shape
    q_rot, k_rot = rot.at[0], rot.at[1]
    depth, cols = w_ref.shape
    piece = depth // (chunks * ways)
    per_chunk = count // chunks
    factor = head_size ** (-0.5) * math.log2(math.e)

    def dp_index(xo, co):
        return lax.rem(xi + xo, nx) * cores + lax.rem(core + co, cores)

    direct = chunks - 1
    alone = count - GROUP

    barrier = pltpu.get_barrier_semaphore()
    for here, there in TALKS:
        for one, other in ((here, there), (there, here)):
            @pl.when(me == one)
            def _(other=other):
                pl.semaphore_signal(barrier, inc=1, device_id={"sp": other}, device_id_type=MESH)
    talkers = sum(jnp.where((me == here) | (me == there), 1, 0) for here, there in TALKS)
    for xo in range(1, nx):
        pl.semaphore_signal(barrier, inc=1, device_id={"dp": dp_index(xo, 0)}, device_id_type=MESH)
    for co in range(1, cores):
        pl.semaphore_signal(barrier, inc=1, device_id={"dp": dp_index(0, co)}, device_id_type=MESH)
    if ways > 1:
        pl.semaphore_signal(barrier, inc=1, device_id={"grp": lax.rem(grp + 1, ways)}, device_id_type=MESH)

    own = pl.ds(pl.multiple_of(me * tok, tok), tok)
    loads = [
        pltpu.make_async_copy(qg_in, qg_ref, load_sem.at[6]),
        pltpu.make_async_copy(kg_in, kg_ref, load_sem.at[7]),
        pltpu.make_async_copy(hg_in, hg_ref, load_sem.at[8]),
        pltpu.make_async_copy(lam_in, lam_ref, load_sem.at[9]),
        pltpu.make_async_copy(cos_in.at[own, :], cos_ref, load_sem.at[3]),
        pltpu.make_async_copy(sin_in.at[own, :], sin_ref, load_sem.at[4]),
        pltpu.make_async_copy(q_in.at[0], rows_in.at[0], load_sem.at[0]),
        pltpu.make_async_copy(k_in.at[0], rows_in.at[1], load_sem.at[1]),
        pltpu.make_async_copy(v_in.at[0], rows_in.at[2], load_sem.at[2]),
    ]
    own_weight = pltpu.make_async_copy(w_ref, wfull.at[dp], load_sem.at[5])
    for load in loads:
        load.start()
    own_weight.start()

    def moved(source, target, send_sem, recv_sem, device):
        return pltpu.make_async_remote_copy(
            src_ref=source, dst_ref=target, send_sem=send_sem, recv_sem=recv_sem,
            device_id=device, device_id_type=MESH,
        )

    def piece_rows(r, way):
        first = (r * ways + lax.rem(grp + way, ways)) * piece
        return pl.ds(pl.multiple_of(first, piece), piece)

    def weight_x(xo, r, way=0):
        rows = piece_rows(r, way)
        return moved(
            w_ref.at[rows, :], wfull.at[dp, rows, :], wx_send.at[xo - 1], wx_recv.at[xo - 1, r + way],
            {"dp": dp_index(xo, 0)},
        )

    def weight_x_in(xo, r, way=0):
        block = wfull.at[dp_index(nx - xo, 0), piece_rows(r, way), :]
        return moved(block, block, wx_send.at[xo - 1], wx_recv.at[xo - 1, r + way], {"dp": dp_index(xo, 0)})

    def weight_y(xo, r):
        block = wfull.at[dp_index(nx - xo, 0), piece_rows(r, 0), :]
        return moved(
            block, block, wy_send.at[xo - 1], wy_recv.at[xo - 1, r], {"grp": lax.rem(grp + 1, ways)}
        )

    def weight_y_in(xo, r):
        block = wfull.at[dp_index(nx - xo, 0), piece_rows(r, 1), :]
        return moved(
            block, block, wy_send.at[xo - 1], wy_recv.at[xo - 1, r], {"grp": lax.rem(grp + 1, ways)}
        )

    def weight_core(xo, r, way):
        rows = piece_rows(r, way)
        target = wfull.at[dp_index(nx - xo, 0), rows, :]
        return moved(
            w_ref.at[rows, :] if xo == 0 else target, target,
            wc_send.at[xo], wc_recv.at[xo, r * per_chunk // GROUP], {"dp": dp_index(0, 1)},
        )

    def weight_core_in(xo, g, rows):
        block = wfull.at[dp_index(nx - xo, 1), rows, :]
        return moved(block, block, wc_send.at[xo], wc_recv.at[xo, g], {"dp": dp_index(0, 1)})

    def forward_x(r):
        for xo in range(1, nx):
            weight_x_in(xo, r).wait_recv()
            if ways > 1:
                weight_y(xo, r).start()
            if cores > 1:
                weight_core(xo, r, 0).start()

            @pl.when(r + DEEP < direct)
            def _(xo=xo):
                weight_x(xo, r + DEEP).start()

            for way in range(ways):
                @pl.when(r == max(direct - DEEP, 0) + way)
                def _(xo=xo, way=way):
                    weight_x(xo, direct, way).start()

    def forward_y(r):
        if ways > 1:
            for xo in range(1, nx):
                weight_y_in(xo, r).wait_recv()
                if cores > 1:
                    weight_core(xo, r, 1).start()

    def forward_direct():
        for way in range(ways):
            for xo in range(1, nx):
                weight_x_in(xo, direct, way).wait_recv()
                if cores > 1:
                    weight_core(xo, direct, way).start()

    def big_to(source, lane, slot, h, peer, what=0):
        return moved(source.at[h], big.at[h, slot], big_send.at[lane], came.at[what, h], {"sp": peer})

    def small_to(lane, slot, h, peer, what):
        source = small_out.at[h, min(lane, 1)]
        return moved(source, small.at[h, slot], small_send.at[lane], came.at[what, h], {"sp": peer})

    def came_in(block, what, h):
        moved(block, block, big_send.at[0], came.at[what, h], {"sp": lax.rem(me + 1, n)}).wait_recv()

    def gone(block, sem):
        moved(block, block, sem, came.at[0, 0], {"sp": lax.rem(me + 1, n)}).wait_send()

    lane = lax.broadcasted_iota(jnp.int32, (1, width), 1)
    low_map = lane < head_size
    half = head_size // 2
    down, across = (lax.broadcasted_iota(jnp.int32, (width, width), axis) for axis in range(2))
    partner = jnp.where(lax.rem(across, head_size) < half, across + half, across - half)
    swap = jnp.where(down == partner, 1.0, 0.0).astype(jnp.bfloat16)
    same_map = jnp.where((down < head_size) == (across < head_size), 1.0, 0.0).astype(jnp.bfloat16)
    sums = jnp.concatenate([same_map, same_map], axis=0)

    def norm_rotate(which, first):
        blocks = [rows_in[which, :, head_columns(first + i)] for i in range(GROUP)]
        stacked = jnp.concatenate(blocks, axis=0)
        x = stacked.astype(jnp.float32)
        square = x * x
        coarse = square.astype(jnp.bfloat16)
        fine = (square - coarse.astype(jnp.float32)).astype(jnp.bfloat16)
        total_square = jnp.dot(jnp.concatenate([coarse, fine], axis=1), sums, preferred_element_type=jnp.float32)
        other = jnp.dot(stacked, swap, preferred_element_type=jnp.float32)
        inverse = lax.rsqrt(total_square * (1.0 / head_size) + EPSILON)
        for i in range(GROUP):
            part = slice(i * tok, (i + 1) * tok)
            straight = x[part] * inverse[part] * turn_ref[2 * which]
            turned = other[part] * inverse[part] * turn_ref[2 * which + 1]
            rot[which, first + i] = (straight + turned).astype(jnp.bfloat16)

    for load in loads[:7]:
        load.wait()
    gain_turn[...] = jnp.broadcast_to(hg_ref[...], (tok, width)).T
    for which, gain in enumerate((qg_ref, kg_ref)):
        gain = gain[...]
        crossed = jnp.concatenate([gain[:, half:], gain[:, :half]], axis=1)
        turn_ref[2 * which] = cos_ref[...] * jnp.concatenate([gain, gain], axis=1)
        turn_ref[2 * which + 1] = sin_ref[...] * jnp.concatenate([crossed, crossed], axis=1)
    causal = lax.broadcasted_iota(jnp.int32, (tok, 2 * tok), 0) <= lax.rem(
        lax.broadcasted_iota(jnp.int32, (tok, 2 * tok), 1), tok
    )

    def head_columns(h):
        return pl.ds(pl.multiple_of(h * width, width), width)

    def turned_scores(keys, *queries):
        both = []
        for q in queries:
            zero = jnp.zeros_like(q)
            both += [jnp.where(low_map, q, zero), jnp.where(low_map, zero, q)]
        both = jnp.concatenate(both, axis=0)
        return lax.dot_general(keys, both, (((1,), (1,)), ((), ())), preferred_element_type=jnp.float32)

    def exponents(scores):
        top = jnp.max(scores, axis=0, keepdims=True)
        e = jnp.exp2((scores - top) * factor)
        return top * factor, e, jnp.sum(e, axis=0, keepdims=True)

    def mixing_of(e, scale, lam):
        one, two = scale[:, :tok], scale[:, tok:] * lam
        return (e[:, :tok] * one - e[:, tok:] * two).astype(jnp.bfloat16)

    def mixed(e, scale, lam, values):
        return jnp.dot(values, mixing_of(e, scale, lam), preferred_element_type=jnp.float32)

    def put_pair(ref, h, slot, pair):
        ref[h, slot, 0:1, :] = pair[:, :tok]
        ref[h, slot, 1:2, :] = pair[:, tok:]

    def get_pair(ref, h, slot):
        return jnp.concatenate([ref[h, slot, 0:1, :], ref[h, slot, 1:2, :]], axis=1)

    def joined(levels):
        top = functools.reduce(jnp.maximum, levels)
        return top + jnp.log2(functools.reduce(jnp.add, [jnp.exp2(l - top) for l in levels]))

    def finish(raw, h):
        scaled = raw * lax.rsqrt(jnp.mean(raw * raw, axis=0, keepdims=True) + EPSILON)
        result = (scaled * gain_turn[...] * OUT_SCALE).T
        heads[:, head_columns(h)] = result.astype(jnp.bfloat16)

    def partial_scores(keys, queries, slot, first, masked):
        scores = [turned_scores(k, q) for k, q in zip(keys, queries)]
        if masked:
            scores = [jnp.where(causal, s, -1e30) for s in scores]
        parts = [exponents(s) for s in scores]
        for i, (top, e, z) in enumerate(parts):
            kept[first + i, slot] = e
            put_pair(kept_top, first + i, slot, top)
            put_pair(small_out, first + i, slot, top + jnp.log2(z))

    def third_queries(h):
        big_to(q_rot, 1, 3, h, 2).start()
        big_to(q_rot, 0, 3, h, 1, 2).start()

    members = range(GROUP)
    ahead = jnp.where(me == 0, 1, 0)

    def begin(j, carry):
        first = j * GROUP

        @pl.when(j == 0)
        def _():
            loads[7].wait()
            loads[8].wait()

        norm_rotate(ahead, first)
        for i in members:
            v_turn[first + i] = rows_in[2, :, head_columns(first + i)].astype(jnp.float32).T.astype(jnp.bfloat16)
        return carry

    def spread(j, carry):
        first = j * GROUP

        @pl.when((me == 3) & (j == 0))
        def _():
            third_queries(0)

        @pl.when((me == 2) & (j == 0))
        def _():
            big_to(q_rot, 0, 2, 0, 1).start()

        @pl.when(me == 0)
        def _():
            for i in members:
                big_to(k_rot, 0, 0, first + i, 1).start()
                big_to(v_turn, 1, 1, first + i, 1).start()

        norm_rotate(1 - ahead, first)

        @pl.when((me == 2) & (first >= alone))
        def _():
            for i in members:
                big_to(k_rot, 2, 2, first + i, 3, 2).start()
                big_to(v_turn, 2, 3, first + i, 3, 2).start()

        @pl.when((me == 2) | ((me == 3) & (first < alone)))
        def _():
            partial_scores([k_rot[first + i] for i in members], [q_rot[first + i] for i in members], 0, first, True)

        @pl.when(me == 2)
        def _():
            for i in members:
                small_to(0, 0, first + i, 1, 1).start()

        @pl.when((me == 2) & (j == 0))
        def _():
            for i in range(1, AHEAD):
                big_to(q_rot, 0, 2, i, 1).start()

        @pl.when((me == 3) & (first < alone))
        def _():
            for i in members:
                if i:
                    third_queries(first + i)
                else:
                    @pl.when(j > 0)
                    def _():
                        third_queries(first)
                small_to(0, 1, first + i, 1, 3).start()

        return carry

    lax.fori_loop(0, 1, begin, 0)
    pl.semaphore_wait(barrier, talkers + (nx - 1) + (cores - 1) + (ways - 1))
    for r in range(min(DEEP, direct)):
        for xo in range(1, nx):
            weight_x(xo, r).start()
    if cores > 1:
        for r in range(chunks):
            for way in range(ways):
                weight_core(0, r, way).start()

    lax.fori_loop(0, 1, spread, 0)
    lax.fori_loop(1, count // GROUP, lambda j, carry: spread(j, begin(j, carry)), 0)

    @pl.when(me == 1)
    def _():
        for h in range(alone, count):
            small[h, 2] = jnp.full((2, tok), -1e30, jnp.float32)

    def lowest(h):
        scores = jnp.where(causal, turned_scores(k_rot[h], q_rot[h]), -1e30)
        _, e, z = exponents(scores)
        finish(mixed(e, 1.0 / z, lam_ref[h], v_turn[h]), h)

    def centre(h, third):
        if h is not None:
            came_in(big.at[h, 0:3], 0, h)
            came_in(small.at[h, 0], 1, h)
        if third is not None:
            came_in(big.at[third, 3], 2, third)

            @pl.when(third < alone)
            def _():
                came_in(small.at[third, 1:3], 3, third)

            @pl.when(third >= alone)
            def _():
                came_in(small.at[third, 1], 3, third)

        pair = 2 * tok
        scores, levels, places, values = [], [], [], []
        for place, x in ((1, h), (2, h), (3, third)):
            if x is None:
                continue
            keys = jnp.concatenate([big[x, 0], k_rot[x]], axis=0)
            values.append(jnp.concatenate([big[x, 1], v_turn[x]], axis=1))
            part = turned_scores(keys, q_rot[x] if place == 1 else big[x, place])
            if place == 1:
                part = jnp.concatenate([part[:tok], jnp.where(causal, part[tok:], -1e30)], axis=0)
            scores.append(part)
            levels.append([get_pair(small, x, slot) for slot in ((), (0,), (1, 2))[place - 1]])
            places.append((place, x))
        parts = [exponents(part) for part in scores]
        scales = []
        for (place, x), (top, e, z), others in zip(places, parts, levels):
            if place == 1:
                scales.append(1.0 / z)
            else:
                level = joined([top + jnp.log2(z)] + others)
                put_pair(small_out, x, place - 2, level)
                scales.append(jnp.exp2(top - level))
        mixing = [mixing_of(e, scale, lam_ref[x]) for (_, x), (_, e, _), scale in zip(places, parts, scales)]
        raws = [jnp.dot(v, m, preferred_element_type=jnp.float32) for v, m in zip(values, mixing)]
        for (place, x), raw in zip(places, raws):
            if place > 1:
                big_out[place - 2, x] = raw.astype(jnp.bfloat16)
        if third is not None:
            @pl.when(third < alone)
            def _():
                small_to(1, 1, third, 2, 3).start()

            small_to(2, 1, third, 3, 1).start()
        if h is not None:
            small_to(0, 0, h, 2, 1).start()
        if third is not None:
            big_to(big_out.at[1], 1, 0, third, 3).start()
        if h is not None:
            big_to(big_out.at[0], 0, 0, h, 2, 2).start()
            finish(raws[0], h)

    def upper_scores(h):
        @pl.when(h < alone)
        def _():
            came_in(big.at[h, 3], 0, h)
            partial_scores([k_rot[h]], [big[h, 3]], 1, h, False)
            small_to(1, 2, h, 1, 3).start()

        @pl.when(h + AHEAD < count)
        def _():
            big_to(q_rot, 0, 2, h + AHEAD, 1).start()

    def upper_raw(h, slot, level):
        scale = jnp.exp2(get_pair(kept_top, h, slot) - level)
        return mixed(kept[h, slot], scale, lam_ref[h], v_turn[h])

    def upper_help(h):
        came_in(small.at[h, 1], 3, h)
        big_out[1, h] = upper_raw(h, 1, get_pair(small, h, 1)).astype(jnp.bfloat16)
        big_to(big_out.at[1], 1, 1, h, 3).start()

    def upper_second(h):
        came_in(small.at[h, 0], 1, h)
        came_in(big.at[h, 0], 2, h)
        finish(upper_raw(h, 0, get_pair(small, h, 0)) + big[h, 0].astype(jnp.float32), h)

    def joint_scores(h):
        came_in(big.at[h, 2:4], 2, h)
        scores = turned_scores(jnp.concatenate([big[h, 2], k_rot[h]], axis=0), q_rot[h])
        scores = jnp.concatenate([scores[:tok], jnp.where(causal, scores[tok:], -1e30)], axis=0)
        top, e, z = exponents(scores)
        kept[h, 0] = e[:tok]
        kept[h, 1] = e[tok:]
        put_pair(kept_top, h, 0, top)
        put_pair(small_out, h, 0, top + jnp.log2(z))

    def upper_third(h):
        came_in(small.at[h, 1], 1, h)

        @pl.when(h < alone)
        def _():
            came_in(big.at[h, 0:2], 0, h)
            raw = upper_raw(h, 0, get_pair(small, h, 1)) + big[h, 0].astype(jnp.float32)
            finish(raw + big[h, 1].astype(jnp.float32), h)

        @pl.when(h >= alone)
        def _():
            came_in(big.at[h, 0], 0, h)
            scale = jnp.exp2(get_pair(kept_top, h, 0) - get_pair(small, h, 1))
            e = jnp.concatenate([kept[h, 0], kept[h, 1]], axis=0)
            values = jnp.concatenate([big[h, 3], v_turn[h]], axis=1)
            finish(mixed(e, scale, lam_ref[h], values) + big[h, 0].astype(jnp.float32), h)

    group = GROUP

    def project(g, first, last, parts=((0, GROUP),)):
        arrived = pl.ds(g * group * width, group * width)
        if cores > 1:
            for xo in range(nx):
                weight_core_in(xo, g, arrived).wait_recv()
        for low, high in parts:
            add_heads(g * group + low, high - low, first, last and high == group)

    def add_heads(low, number, first, last):
        rows = pl.ds(low * width, number * width)
        block = heads[:, rows]
        for index in range(n_dp):
            term = jnp.dot(block, wfull[index, rows, :], preferred_element_type=jnp.float32)
            span = slice(index * cols, (index + 1) * cols)
            if not first:
                term = total[:, span] + term
            if last:
                out_ref[0, :, span] = term.astype(out_ref.dtype)
            else:
                total[:, span] = term

    groups = count // group

    def turned_order(at):
        early = (at >= alone - SWAP) & (at < alone)
        late = (at >= alone) & (at < alone + SWAP)
        return at + jnp.where(early, SWAP, jnp.where(late, -SWAP, 0))


    first_x = jnp.where(me == 1, 2, 1)
    first_y = first_x + 2 * per_chunk
    last_x = first_x + direct * per_chunk

    def step(it, carry):
        @pl.when((me == 2) & (it < count))
        def _():
            upper_scores(it)

        turn = lax.rem(it - first_x + per_chunk, per_chunk) == 0

        @pl.when(turn & (it >= first_x) & (it < last_x))
        def _():
            forward_x((it - first_x) // per_chunk)

        @pl.when(turn & (it >= first_y) & (it < first_y + direct * per_chunk))
        def _():
            forward_y((it - first_y) // per_chunk)

        @pl.when(it == jnp.where(me < 2, last_x, HELP + alone + 1))
        def _():
            forward_direct()

        @pl.when((me == 0) & (it < count))
        def _():
            lowest(it)

        @pl.when((me == 1) & (it < BEHIND))
        def _():
            centre(it, None)

        @pl.when((me == 1) & (it >= BEHIND) & (it < count))
        def _():
            centre(it, jnp.where(it == count - 1, it - 1, it - BEHIND))

        @pl.when((me == 1) & (it >= count - BEHIND) & (it < count))
        def _():
            centre(None, jnp.where(it == count - 1, it, it - 1))

        @pl.when((me == 2) & (it >= HELP) & (it < HELP + alone))
        def _():
            upper_help(it - HELP)

        @pl.when((me == 2) & (it >= NEAR) & (it < NEAR + count))
        def _():
            upper_second(it - NEAR)

        @pl.when((me == 3) & (it >= GROUP) & (it < 2 * GROUP))
        def _():
            joint_scores(alone + it - GROUP)

        for i in range(GROUP):
            @pl.when((me == 3) & (it == LAG + PACES[i]))
            def _(i=i):
                big_to(q_rot, 0, 3, alone + i, 1, 2).start()
                small_to(0, 1, alone + i, 1, 3).start()

        @pl.when((me == 3) & (it >= LAG))
        def _():
            upper_third(turned_order(it - LAG))

        for g in range(groups - 1):
            @pl.when(it == g * group + PROJECT + jnp.where(me == 3, LATE, jnp.where((me == 1) & (g == 1), 2, 0)))
            def _(g=g):
                if g == 0:
                    own_weight.wait()
                project(g, g == 0, False)

        return carry

    steps = count + NEAR
    lax.fori_loop(0, steps, step, 0)

    @pl.when(me == 3)
    def _():
        for h in range(steps - LAG, count - 2):
            upper_third(h)

    project(groups - 1, False, False, ((0, GROUP - 2),))

    @pl.when(me == 3)
    def _():
        for h in range(max(steps - LAG, count - 2), count):
            upper_third(h)

    add_heads(count - 2, 2, False, True)

    whole, most = q_rot.at[:], q_rot.at[0:alone]
    rows = small_out.at[:, 0]
    most_rows = small_out.at[0:alone, 0]

    @pl.when(me == 0)
    def _():
        gone(whole, big_send.at[0])
        gone(whole, big_send.at[1])

    @pl.when(me == 1)
    def _():
        gone(whole, big_send.at[0])
        gone(whole, big_send.at[1])
        gone(rows, small_send.at[0])
        gone(most_rows, small_send.at[1])
        gone(rows, small_send.at[2])

    @pl.when(me == 2)
    def _():
        gone(whole, big_send.at[0])
        gone(most, big_send.at[1])
        gone(q_rot.at[0 : 2 * GROUP], big_send.at[2])
        gone(rows, small_send.at[0])
        gone(most_rows, small_send.at[1])

    @pl.when(me == 3)
    def _():
        gone(whole, big_send.at[0])
        gone(most, big_send.at[1])
        gone(rows, small_send.at[0])

    for xo in range(nx):
        if xo:
            sent_x = wfull.at[0, 0 : (direct + ways) * piece, :]
            moved(sent_x, sent_x, wx_send.at[xo - 1], wx_recv.at[0, 0], {"dp": dp_index(xo, 0)}).wait_send()
            if ways > 1:
                sent_y = wfull.at[0, 0 : direct * piece, :]
                moved(sent_y, sent_y, wy_send.at[xo - 1], wy_recv.at[0, 0], {"dp": dp_index(xo, 0)}).wait_send()
        if cores > 1:
            sent_core = wfull.at[0]
            moved(sent_core, sent_core, wc_send.at[xo], wc_recv.at[0, 0], {"dp": dp_index(0, 1)}).wait_send()


def split_local(n, n_dp, n_grp, query_rows, key_rows, value_rows, query_gain, key_gain, lambdas, head_gain, out_weight):
    tok = query_rows.shape[1]
    head_size = query_gain.shape[0]
    width = head_gain.shape[0]
    count = lambdas.shape[0]
    depth, cols = out_weight.shape
    ways = WAYS if n_grp == WAYS else 1
    chunks = count // ways
    cores = CORES if n_dp % CORES == 0 else 1
    nx = n_dp // cores
    cosine, sine = rotation_tables(tok * n, head_size)
    anywhere = pl.BlockSpec(memory_space=pl.ANY)
    vmem = pl.BlockSpec(memory_space=pltpu.VMEM)
    dma = pltpu.SemaphoreType.DMA
    across = max(nx - 1, 1)
    return pl.pallas_call(
        functools.partial(split_kernel, n, n_dp, n_grp, head_size, chunks),
        out_shape=pltpu.VMEM((1, tok, n_dp * cols), jnp.bfloat16),
        in_specs=[anywhere] * 3
        + [anywhere] * 7,
        out_specs=vmem,
        scratch_shapes=[
            pltpu.VMEM((tok, n_dp * cols), jnp.float32),
            pltpu.VMEM((3, tok, count * width), jnp.bfloat16),
            pltpu.VMEM((2, count, tok, width), jnp.bfloat16),
            pltpu.VMEM((count, tok, width), jnp.bfloat16),
            pltpu.VMEM((count, 4, tok, width), jnp.bfloat16),
            pltpu.VMEM((count, 3, 2, tok), jnp.float32),
            pltpu.VMEM((2, count, tok, width), jnp.bfloat16),
            pltpu.VMEM((count, 2, 2, tok), jnp.float32),
            pltpu.VMEM((count, 2, tok, 2 * tok), jnp.float32),
            pltpu.VMEM((count, 2, 2, tok), jnp.float32),
            pltpu.VMEM((width, tok), jnp.float32),
            pltpu.VMEM((tok, count * width), jnp.bfloat16),
            pltpu.VMEM((n_dp, depth, cols), jnp.bfloat16),
            pltpu.VMEM((tok, width), jnp.float32),
            pltpu.VMEM((tok, width), jnp.float32),
            pltpu.VMEM((4, tok, width), jnp.float32),
            pltpu.VMEM((1, head_size), jnp.float32),
            pltpu.VMEM((1, head_size), jnp.float32),
            pltpu.SMEM((count,), jnp.float32),
            pltpu.VMEM((1, width), jnp.float32),
            dma((10,)),
            dma((3,)),
            dma((3,)),
            dma((4, count)),
            dma((across,)),
            dma((across, chunks - 1 + ways)),
            dma((across,)),
            dma((across, chunks)),
            dma((nx,)),
            dma((nx, count // GROUP)),
        ],
        compiler_params=pltpu.CompilerParams(
            collective_id=0, has_side_effects=True, vmem_limit_bytes=56 * 1024 * 1024
        ),
    )(
        query_rows, key_rows, value_rows,
        query_gain[None, :], key_gain[None, :], lambdas, head_gain[None, :],
        out_weight, jnp.asarray(cosine), jnp.asarray(sine),
    )


def plan(n, tok, width, count, n_grp):
    ways = WAYS if n_grp == WAYS else 1
    fits = n == PARTS and tok == width and count % (GROUP * ways) == 0
    return split_local if fits else local


def solution(mesh):
    rows = P(("grp", "dp"), "sp", None)
    n, n_dp, n_grp = mesh.shape["sp"], mesh.shape["dp"], mesh.shape["grp"]

    def body(*args):
        chosen = plan(n, args[0].shape[1], args[6].shape[0], args[5].shape[0], n_grp)
        return chosen(n, n_dp, n_grp, *args)

    return jax.shard_map(
        body,
        mesh=mesh,
        in_specs=(rows, rows, rows, P(), P(), P(), P(), P(None, "dp")),
        out_specs=rows,
        check_vma=False,
    )
```

```python
import functools
import math

import jax
import jax.numpy as jnp
import numpy as np
from jax import lax
from jax.experimental import pallas as pl
from jax.experimental.pallas import tpu as pltpu
from jax.sharding import PartitionSpec as P

EPSILON = 1e-06
OUT_SCALE = 0.8
CORES = 2
CHUNKS = 2
WAYS = 2
PARTS = 4
GROUP = 4
LAG = 7
AHEAD = 3
DEEP = 3
PACES = (4, 4, 6, 6)
BEHIND = 2
NEAR = 4
HELP = 4
PROJECT = 10
SWAP = 0
LATE = 0
TALKS = ((0, 1), (1, 2), (1, 3), (2, 3))
MESH = pl.DeviceIdType.MESH


def rotation_tables(length, head_size):
    half = head_size // 2
    inverse = np.float32(10000.0) ** (-np.arange(half, dtype=np.float32) / np.float32(half))
    angles = np.arange(length, dtype=np.float32)[:, None] * inverse.astype(np.float32)[None, :]
    cosine, sine = np.cos(angles), np.sin(angles)
    return (
        np.concatenate([cosine] * 4, axis=1).astype(np.float32),
        np.concatenate([-sine, sine] * 2, axis=1).astype(np.float32),
    )


def kernel(
    n, n_dp, n_grp, head_size, q_ref, k_ref, v_ref, qg_ref, kg_ref, lam_ref, hg_ref, w_ref, cos_in, sin_in,
    out_ref, total, rx, rot_q, rot_k, heads_out, hrx, wfull,
    in_send, in_recv, ret_send, ret_recv, wx_send, wx_recv, wy_send, wy_recv, wc_send, wc_recv, own_sem, cos_ref, sin_ref, table_sem,
):
    me = lax.axis_index("sp")
    dp = lax.axis_index("dp")
    ways = WAYS if n_grp == WAYS else 1
    grp = lax.axis_index("grp") if ways > 1 else 0
    cores = CORES if n_dp % CORES == 0 else 1
    nx = n_dp // cores
    xi, core = dp // cores, lax.rem(dp, cores)
    tok = q_ref.shape[1]
    width = 2 * head_size
    local_heads = rx.shape[1]
    length = rx.shape[2]
    depth = w_ref.shape[0]
    cols = w_ref.shape[1]
    piece = depth // (CHUNKS * ways)

    def sp_peer(off):
        return lax.rem(me + off, n)

    def dp_index(xo, co):
        return lax.rem(xi + xo, nx) * cores + lax.rem(core + co, cores)

    barrier = pltpu.get_barrier_semaphore()
    for off in range(1, n):
        pl.semaphore_signal(barrier, inc=1, device_id={"sp": sp_peer(off)}, device_id_type=MESH)
    for xo in range(1, nx):
        pl.semaphore_signal(barrier, inc=1, device_id={"dp": dp_index(xo, 0)}, device_id_type=MESH)
    for co in range(1, cores):
        pl.semaphore_signal(barrier, inc=1, device_id={"dp": dp_index(0, co)}, device_id_type=MESH)

    if ways > 1:
        pl.semaphore_signal(
            barrier, inc=1, device_id={"grp": lax.rem(grp + 1, ways)}, device_id_type=MESH
        )

    sources = (k_ref, q_ref, v_ref)

    def own_rows(t, j):
        column = pl.multiple_of((me * local_heads + j) * width, width)
        return pltpu.make_async_copy(
            sources[t].at[0, :, pl.ds(column, width)],
            rx.at[t, j, pl.ds(pl.multiple_of(me * tok, tok), tok), :],
            in_recv.at[t, j, 0],
        )

    def rows_to(t, j, off):
        peer = sp_peer(off)
        column = pl.multiple_of((peer * local_heads + j) * width, width)
        return pltpu.make_async_remote_copy(
            src_ref=sources[t].at[0, :, pl.ds(column, width)],
            dst_ref=rx.at[t, j, pl.ds(pl.multiple_of(me * tok, tok), tok), :],
            send_sem=in_send.at[t, j, off],
            recv_sem=in_recv.at[t, j, off],
            device_id={"sp": peer},
            device_id_type=MESH,
        )

    def rows_from(t, j, off):
        peer = lax.rem(me + n - off, n)
        block = rx.at[t, j, pl.ds(pl.multiple_of(peer * tok, tok), tok), :]
        return pltpu.make_async_remote_copy(
            src_ref=block, dst_ref=block, send_sem=in_send.at[t, j, off],
            recv_sem=in_recv.at[t, j, off], device_id={"sp": peer}, device_id_type=MESH,
        )

    def piece_rows(r, way):
        first = (r * ways + lax.rem(grp + way, ways)) * piece
        return pl.ds(pl.multiple_of(first, piece), piece)

    def moved(source, target, send_sem, recv_sem, device):
        return pltpu.make_async_remote_copy(
            src_ref=source, dst_ref=target, send_sem=send_sem, recv_sem=recv_sem,
            device_id=device, device_id_type=MESH,
        )

    def weight_x(xo, r):
        rows = piece_rows(r, 0)
        return moved(
            w_ref.at[rows, :], wfull.at[dp, rows, :], wx_send.at[xo, r], wx_recv.at[xo, r],
            {"dp": dp_index(xo, 0)},
        )

    def weight_x_in(xo, r):
        block = wfull.at[dp_index(nx - xo, 0), piece_rows(r, 0), :]
        return moved(block, block, wx_send.at[xo, r], wx_recv.at[xo, r], {"dp": dp_index(xo, 0)})

    def weight_y(xo, r):
        block = wfull.at[dp_index(nx - xo, 0), piece_rows(r, 0), :]
        return moved(block, block, wy_send.at[xo, r], wy_recv.at[xo, r], {"grp": lax.rem(grp + 1, ways)})

    def weight_y_in(xo, r):
        block = wfull.at[dp_index(nx - xo, 0), piece_rows(r, 1), :]
        return moved(block, block, wy_send.at[xo, r], wy_recv.at[xo, r], {"grp": lax.rem(grp + 1, ways)})

    def weight_core(xo, r, way):
        rows = piece_rows(r, way)
        target = wfull.at[dp_index(nx - xo, 0), rows, :]
        return moved(
            w_ref.at[rows, :] if xo == 0 else target, target,
            wc_send.at[xo, r, way], wc_recv.at[xo, r, way], {"dp": dp_index(0, 1)},
        )

    def weight_core_in(xo, r, way):
        block = wfull.at[dp_index(nx - xo, 1), piece_rows(r, way), :]
        return moved(
            block, block, wc_send.at[xo, r, way], wc_recv.at[xo, r, way], {"dp": dp_index(0, 1)}
        )

    own_weight = pltpu.make_async_copy(w_ref, wfull.at[dp], own_sem)
    own_weight.start()
    tables = [
        pltpu.make_async_copy(cos_in, cos_ref, table_sem.at[0]),
        pltpu.make_async_copy(sin_in, sin_ref, table_sem.at[1]),
    ]
    for table in tables:
        table.start()
    for j in range(local_heads):
        for t in range(3):
            own_rows(t, j).start()
    pl.semaphore_wait(barrier, (n - 1) + (nx - 1) + (cores - 1) + (ways - 1))
    for j in range(local_heads):
        for t in range(3):
            for off in range(1, n):
                rows_to(t, j, off).start()
        if j == 0:
            for r in range(CHUNKS):
                for xo in range(1, nx):
                    weight_x(xo, r).start()
            if cores > 1:
                for r in range(CHUNKS):
                    for way in range(ways):
                        weight_core(0, r, way).start()

    lane = lax.broadcasted_iota(jnp.int32, (1, width), 1)
    low_map = lane < head_size
    low_half = lax.rem(lane, head_size) < head_size // 2

    def norm_rotate(block, gain):
        x = block.astype(jnp.float32)
        square = x * x
        low = jnp.sum(jnp.where(low_map, square, 0.0), axis=1, keepdims=True)
        high = jnp.sum(jnp.where(low_map, 0.0, square), axis=1, keepdims=True)
        low = lax.rsqrt(low * (1.0 / head_size) + EPSILON)
        high = lax.rsqrt(high * (1.0 / head_size) + EPSILON)
        y = x * jnp.where(low_map, low, high) * gain
        quarter = head_size // 2
        turned = jnp.where(low_half, pltpu.roll(y, width - quarter, 1), pltpu.roll(y, quarter, 1))
        return (y * cos_ref[...] + turned * sin_ref[...]).astype(jnp.bfloat16)

    def heads_to(j, i):
        column = pl.multiple_of(me * width, width)
        off = lax.rem(i + n - me, n)
        return pltpu.make_async_remote_copy(
            src_ref=heads_out.at[j, i], dst_ref=hrx.at[j, :, pl.ds(column, width)],
            send_sem=ret_send.at[j, off], recv_sem=ret_recv.at[j, off],
            device_id={"sp": i}, device_id_type=MESH,
        )

    def heads_from(j, off):
        peer = lax.rem(me + n - off, n)
        column = pl.multiple_of(peer * width, width)
        block = hrx.at[j, :, pl.ds(column, width)]
        return pltpu.make_async_remote_copy(
            src_ref=block, dst_ref=block, send_sem=ret_send.at[j, off],
            recv_sem=ret_recv.at[j, off], device_id={"sp": peer}, device_id_type=MESH,
        )

    groups = math.gcd(n, 4)
    per_group = n // groups
    segment = length // groups
    factor = head_size ** (-0.5) * math.log2(math.e)
    contract = (((1,), (1,)), ((), ()))

    def query_block(j, g, i, lam):
        rows = pl.ds(i * tok, tok) if isinstance(i, int) else pl.ds(pl.multiple_of(i * tok, tok), tok)
        q = rot_q[rows, :]
        zero = jnp.zeros_like(q)
        both = jnp.concatenate([jnp.where(low_map, q, zero), jnp.where(low_map, zero, q)], axis=0)
        start = g * segment
        spans = ([(0, start)] if g else []) + [(start, segment)]
        parts = []
        for first, size in spans:
            scores = lax.dot_general(
                both, rot_k[first : first + size, :], contract, preferred_element_type=jnp.float32
            )
            if first == start:
                shape = (2 * tok, size)
                row = lax.rem(lax.broadcasted_iota(jnp.int32, shape, 0), tok) + i * tok
                column = lax.broadcasted_iota(jnp.int32, shape, 1) + first
                scores = jnp.where(column <= row, scores, -1e30)
            parts.append(scores)
        top = functools.reduce(jnp.maximum, [jnp.max(s, axis=1, keepdims=True) for s in parts])
        parts = [jnp.exp2((s - top) * factor) for s in parts]
        total = functools.reduce(jnp.add, [jnp.sum(e, axis=1, keepdims=True) for e in parts])
        inverse = 1.0 / total
        one, two = inverse[:tok], inverse[tok:] * lam
        raw = None
        for (first, size), e in zip(spans, parts):
            mixing = (e[:tok] * one - e[tok:] * two).astype(jnp.bfloat16)
            term = jnp.dot(mixing, rx[2, j, first : first + size, :], preferred_element_type=jnp.float32)
            raw = term if raw is None else raw + term
        scaled = raw * lax.rsqrt(jnp.mean(raw * raw, axis=1, keepdims=True) + EPSILON)
        result = (scaled * hg_ref[...] * OUT_SCALE).astype(jnp.bfloat16)

        @pl.when(i == me)
        def _():
            hrx[j, :, pl.ds(pl.multiple_of(me * width, width), width)] = result

        @pl.when(i != me)
        def _():
            heads_out[j, i] = result
            heads_to(j, i).start()

    def forward(stage):
        if stage < CHUNKS:
            for xo in range(1, nx):
                weight_x_in(xo, stage).wait_recv()
                if ways > 1:
                    weight_y(xo, stage).start()
                if cores > 1:
                    weight_core(xo, stage, 0).start()
        elif ways > 1:
            for xo in range(1, nx):
                weight_y_in(xo, stage - CHUNKS).wait_recv()
                if cores > 1:
                    weight_core(xo, stage - CHUNKS, 1).start()

    for table in tables:
        table.wait()
    for j in range(local_heads):
        lam = lam_ref[me * local_heads + j]
        for t, (target, gain) in enumerate(((rot_k, kg_ref), (rot_q, qg_ref), (None, None))):
            own_rows(t, j).wait()
            for off in range(1, n):
                rows_from(t, j, off).wait_recv()
            if target is not None:
                target[...] = norm_rotate(rx[t, j], jnp.concatenate([gain[...]] * 2, axis=1))
        for g in range(groups):
            if per_group == 1:
                query_block(j, g, g, lam)
            else:
                def step(b, carry, j=j, g=g, lam=lam):
                    query_block(j, g, g * per_group + b, lam)
                    return carry
                lax.fori_loop(0, per_group, step, 0)
        for stage in range(2 * CHUNKS):
            if j == min(stage, local_heads - 1):
                forward(stage)

    own_weight.wait()
    if cores > 1:
        for xo in range(nx):
            for r in range(CHUNKS):
                for way in range(ways):
                    weight_core_in(xo, r, way).wait_recv()

    for j in range(local_heads):
        for off in range(1, n):
            heads_from(j, off).wait_recv()
        rows = hrx[j]
        for index in range(n_dp):
            matching = jnp.concatenate(
                [wfull[index, pl.ds((s * local_heads + j) * width, width), :] for s in range(n)], axis=0
            )
            term = jnp.dot(rows, matching, preferred_element_type=jnp.float32)
            span = slice(index * cols, (index + 1) * cols)
            if j:
                term = total[:, span] + term
            if j == local_heads - 1:
                out_ref[0, :, span] = term.astype(out_ref.dtype)
            else:
                total[:, span] = term

    for j in range(local_heads):
        for off in range(1, n):
            for t in range(3):
                rows_to(t, j, off).wait_send()
            heads_to(j, sp_peer(off)).wait_send()
    for r in range(CHUNKS):
        for xo in range(nx):
            if xo:
                weight_x(xo, r).wait_send()
                if ways > 1:
                    weight_y(xo, r).wait_send()
            if cores > 1:
                for way in range(ways):
                    weight_core(xo, r, way).wait_send()


def local(n, n_dp, n_grp, query_rows, key_rows, value_rows, query_gain, key_gain, lambdas, head_gain, out_weight):
    tok = query_rows.shape[1]
    head_size = query_gain.shape[0]
    width = head_gain.shape[0]
    local_heads = lambdas.shape[0] // n
    length = tok * n
    depth, cols = out_weight.shape
    cores = CORES if n_dp % CORES == 0 else 1
    nx = n_dp // cores
    cosine, sine = rotation_tables(length, head_size)
    anywhere = pl.BlockSpec(memory_space=pl.ANY)
    vmem = pl.BlockSpec(memory_space=pltpu.VMEM)
    dma = pltpu.SemaphoreType.DMA
    return pl.pallas_call(
        functools.partial(kernel, n, n_dp, n_grp, head_size),
        out_shape=jax.ShapeDtypeStruct((1, tok, n_dp * cols), jnp.bfloat16),
        in_specs=[anywhere] * 3
        + [vmem, vmem, pl.BlockSpec(memory_space=pltpu.SMEM), vmem, anywhere, anywhere, anywhere],
        out_specs=vmem,
        scratch_shapes=[
            pltpu.VMEM((tok, n_dp * cols), jnp.float32),
            pltpu.VMEM((3, local_heads, length, width), jnp.bfloat16),
            pltpu.VMEM((length, width), jnp.bfloat16),
            pltpu.VMEM((length, width), jnp.bfloat16),
            pltpu.VMEM((local_heads, n, tok, width), jnp.bfloat16),
            pltpu.VMEM((local_heads, tok, n * width), jnp.bfloat16),
            pltpu.VMEM((n_dp, depth, cols), jnp.bfloat16),
            dma((3, local_heads, n)),
            dma((3, local_heads, n)),
            dma((local_heads, n)),
            dma((local_heads, n)),
            dma((nx, CHUNKS)),
            dma((nx, CHUNKS)),
            dma((nx, CHUNKS)),
            dma((nx, CHUNKS)),
            dma((nx, CHUNKS, WAYS)),
            dma((nx, CHUNKS, WAYS)),
            dma(()),
            pltpu.VMEM((length, width), jnp.float32),
            pltpu.VMEM((length, width), jnp.float32),
            dma((2,)),
        ],
        compiler_params=pltpu.CompilerParams(
            collective_id=0, has_side_effects=True, vmem_limit_bytes=56 * 1024 * 1024
        ),
    )(
        query_rows, key_rows, value_rows,
        query_gain[None, :], key_gain[None, :], lambdas, head_gain[None, :],
        out_weight, jnp.asarray(cosine), jnp.asarray(sine),
    )


def split_kernel(
    n, n_dp, n_grp, head_size, chunks, q_in, k_in, v_in, qg_in, kg_in, lam_in, hg_in, w_ref, cos_in, sin_in,
    out_ref, total, rows_in, rot, v_turn, big, small, big_out, small_out, kept, kept_top, gain_turn, heads, wfull,
    cos_ref, sin_ref, turn_ref, qg_ref, kg_ref, lam_ref, hg_ref, load_sem, big_send, small_send, came, wx_send, wx_recv, wy_send, wy_recv, wc_send, wc_recv,
):
    me = lax.axis_index("sp")
    dp = lax.axis_index("dp")
    ways = WAYS if n_grp == WAYS else 1
    grp = lax.axis_index("grp") if ways > 1 else 0
    cores = CORES if n_dp % CORES == 0 else 1
    nx = n_dp // cores
    xi, core = dp // cores, lax.rem(dp, cores)
    count, tok, width = v_turn.shape
    q_rot, k_rot = rot.at[0], rot.at[1]
    depth, cols = w_ref.shape
    piece = depth // (chunks * ways)
    per_chunk = count // chunks
    factor = head_size ** (-0.5) * math.log2(math.e)

    def dp_index(xo, co):
        return lax.rem(xi + xo, nx) * cores + lax.rem(core + co, cores)

    direct = chunks - 1
    alone = count - GROUP

    barrier = pltpu.get_barrier_semaphore()
    for here, there in TALKS:
        for one, other in ((here, there), (there, here)):
            @pl.when(me == one)
            def _(other=other):
                pl.semaphore_signal(barrier, inc=1, device_id={"sp": other}, device_id_type=MESH)
    talkers = sum(jnp.where((me == here) | (me == there), 1, 0) for here, there in TALKS)
    for xo in range(1, nx):
        pl.semaphore_signal(barrier, inc=1, device_id={"dp": dp_index(xo, 0)}, device_id_type=MESH)
    for co in range(1, cores):
        pl.semaphore_signal(barrier, inc=1, device_id={"dp": dp_index(0, co)}, device_id_type=MESH)
    if ways > 1:
        pl.semaphore_signal(barrier, inc=1, device_id={"grp": lax.rem(grp + 1, ways)}, device_id_type=MESH)

    own = pl.ds(pl.multiple_of(me * tok, tok), tok)
    loads = [
        pltpu.make_async_copy(qg_in, qg_ref, load_sem.at[6]),
        pltpu.make_async_copy(kg_in, kg_ref, load_sem.at[7]),
        pltpu.make_async_copy(hg_in, hg_ref, load_sem.at[8]),
        pltpu.make_async_copy(lam_in, lam_ref, load_sem.at[9]),
        pltpu.make_async_copy(cos_in.at[own, :], cos_ref, load_sem.at[3]),
        pltpu.make_async_copy(sin_in.at[own, :], sin_ref, load_sem.at[4]),
        pltpu.make_async_copy(q_in.at[0], rows_in.at[0], load_sem.at[0]),
        pltpu.make_async_copy(k_in.at[0], rows_in.at[1], load_sem.at[1]),
        pltpu.make_async_copy(v_in.at[0], rows_in.at[2], load_sem.at[2]),
    ]
    own_weight = pltpu.make_async_copy(w_ref, wfull.at[dp], load_sem.at[5])
    for load in loads:
        load.start()
    own_weight.start()

    def moved(source, target, send_sem, recv_sem, device):
        return pltpu.make_async_remote_copy(
            src_ref=source, dst_ref=target, send_sem=send_sem, recv_sem=recv_sem,
            device_id=device, device_id_type=MESH,
        )

    def piece_rows(r, way):
        first = (r * ways + lax.rem(grp + way, ways)) * piece
        return pl.ds(pl.multiple_of(first, piece), piece)

    def weight_x(xo, r, way=0):
        rows = piece_rows(r, way)
        return moved(
            w_ref.at[rows, :], wfull.at[dp, rows, :], wx_send.at[xo - 1], wx_recv.at[xo - 1, r + way],
            {"dp": dp_index(xo, 0)},
        )

    def weight_x_in(xo, r, way=0):
        block = wfull.at[dp_index(nx - xo, 0), piece_rows(r, way), :]
        return moved(block, block, wx_send.at[xo - 1], wx_recv.at[xo - 1, r + way], {"dp": dp_index(xo, 0)})

    def weight_y(xo, r):
        block = wfull.at[dp_index(nx - xo, 0), piece_rows(r, 0), :]
        return moved(
            block, block, wy_send.at[xo - 1], wy_recv.at[xo - 1, r], {"grp": lax.rem(grp + 1, ways)}
        )

    def weight_y_in(xo, r):
        block = wfull.at[dp_index(nx - xo, 0), piece_rows(r, 1), :]
        return moved(
            block, block, wy_send.at[xo - 1], wy_recv.at[xo - 1, r], {"grp": lax.rem(grp + 1, ways)}
        )

    def weight_core(xo, r, way):
        rows = piece_rows(r, way)
        target = wfull.at[dp_index(nx - xo, 0), rows, :]
        return moved(
            w_ref.at[rows, :] if xo == 0 else target, target,
            wc_send.at[xo], wc_recv.at[xo, r * per_chunk // GROUP], {"dp": dp_index(0, 1)},
        )

    def weight_core_in(xo, g, rows):
        block = wfull.at[dp_index(nx - xo, 1), rows, :]
        return moved(block, block, wc_send.at[xo], wc_recv.at[xo, g], {"dp": dp_index(0, 1)})

    def forward_x(r):
        for xo in range(1, nx):
            weight_x_in(xo, r).wait_recv()
            if ways > 1:
                weight_y(xo, r).start()
            if cores > 1:
                weight_core(xo, r, 0).start()

            @pl.when(r + DEEP < direct)
            def _(xo=xo):
                weight_x(xo, r + DEEP).start()

            for way in range(ways):
                @pl.when(r == max(direct - DEEP, 0) + way)
                def _(xo=xo, way=way):
                    weight_x(xo, direct, way).start()

    def forward_y(r):
        if ways > 1:
            for xo in range(1, nx):
                weight_y_in(xo, r).wait_recv()
                if cores > 1:
                    weight_core(xo, r, 1).start()

    def forward_direct():
        for way in range(ways):
            for xo in range(1, nx):
                weight_x_in(xo, direct, way).wait_recv()
                if cores > 1:
                    weight_core(xo, direct, way).start()

    def big_to(source, lane, slot, h, peer, what=0):
        return moved(source.at[h], big.at[h, slot], big_send.at[lane], came.at[what, h], {"sp": peer})

    def small_to(lane, slot, h, peer, what):
        source = small_out.at[h, min(lane, 1)]
        return moved(source, small.at[h, slot], small_send.at[lane], came.at[what, h], {"sp": peer})

    def came_in(block, what, h):
        moved(block, block, big_send.at[0], came.at[what, h], {"sp": lax.rem(me + 1, n)}).wait_recv()

    def gone(block, sem):
        moved(block, block, sem, came.at[0, 0], {"sp": lax.rem(me + 1, n)}).wait_send()

    lane = lax.broadcasted_iota(jnp.int32, (1, width), 1)
    low_map = lane < head_size
    half = head_size // 2
    down, across = (lax.broadcasted_iota(jnp.int32, (width, width), axis) for axis in range(2))
    partner = jnp.where(lax.rem(across, head_size) < half, across + half, across - half)
    swap = jnp.where(down == partner, 1.0, 0.0).astype(jnp.bfloat16)
    same_map = jnp.where((down < head_size) == (across < head_size), 1.0, 0.0).astype(jnp.bfloat16)
    sums = jnp.concatenate([same_map, same_map], axis=0)

    def norm_rotate(which, first):
        blocks = [rows_in[which, :, head_columns(first + i)] for i in range(GROUP)]
        stacked = jnp.concatenate(blocks, axis=0)
        x = stacked.astype(jnp.float32)
        square = x * x
        coarse = square.astype(jnp.bfloat16)
        fine = (square - coarse.astype(jnp.float32)).astype(jnp.bfloat16)
        total_square = jnp.dot(jnp.concatenate([coarse, fine], axis=1), sums, preferred_element_type=jnp.float32)
        other = jnp.dot(stacked, swap, preferred_element_type=jnp.float32)
        inverse = lax.rsqrt(total_square * (1.0 / head_size) + EPSILON)
        for i in range(GROUP):
            part = slice(i * tok, (i + 1) * tok)
            straight = x[part] * inverse[part] * turn_ref[2 * which]
            turned = other[part] * inverse[part] * turn_ref[2 * which + 1]
            rot[which, first + i] = (straight + turned).astype(jnp.bfloat16)

    for load in loads[:7]:
        load.wait()
    gain_turn[...] = jnp.broadcast_to(hg_ref[...], (tok, width)).T
    for which, gain in enumerate((qg_ref, kg_ref)):
        gain = gain[...]
        crossed = jnp.concatenate([gain[:, half:], gain[:, :half]], axis=1)
        turn_ref[2 * which] = cos_ref[...] * jnp.concatenate([gain, gain], axis=1)
        turn_ref[2 * which + 1] = sin_ref[...] * jnp.concatenate([crossed, crossed], axis=1)
    causal = lax.broadcasted_iota(jnp.int32, (tok, 2 * tok), 0) <= lax.rem(
        lax.broadcasted_iota(jnp.int32, (tok, 2 * tok), 1), tok
    )

    def head_columns(h):
        return pl.ds(pl.multiple_of(h * width, width), width)

    def turned_scores(keys, *queries):
        both = []
        for q in queries:
            zero = jnp.zeros_like(q)
            both += [jnp.where(low_map, q, zero), jnp.where(low_map, zero, q)]
        both = jnp.concatenate(both, axis=0)
        return lax.dot_general(keys, both, (((1,), (1,)), ((), ())), preferred_element_type=jnp.float32)

    def exponents(scores):
        top = jnp.max(scores, axis=0, keepdims=True)
        e = jnp.exp2((scores - top) * factor)
        return top * factor, e, jnp.sum(e, axis=0, keepdims=True)

    def mixing_of(e, scale, lam):
        one, two = scale[:, :tok], scale[:, tok:] * lam
        return (e[:, :tok] * one - e[:, tok:] * two).astype(jnp.bfloat16)

    def mixed(e, scale, lam, values):
        return jnp.dot(values, mixing_of(e, scale, lam), preferred_element_type=jnp.float32)

    def put_pair(ref, h, slot, pair):
        ref[h, slot, 0:1, :] = pair[:, :tok]
        ref[h, slot, 1:2, :] = pair[:, tok:]

    def get_pair(ref, h, slot):
        return jnp.concatenate([ref[h, slot, 0:1, :], ref[h, slot, 1:2, :]], axis=1)

    def joined(levels):
        top = functools.reduce(jnp.maximum, levels)
        return top + jnp.log2(functools.reduce(jnp.add, [jnp.exp2(l - top) for l in levels]))

    def finish(raw, h):
        scaled = raw * lax.rsqrt(jnp.mean(raw * raw, axis=0, keepdims=True) + EPSILON)
        result = (scaled * gain_turn[...] * OUT_SCALE).T
        heads[:, head_columns(h)] = result.astype(jnp.bfloat16)

    def partial_scores(keys, queries, slot, first, masked):
        scores = [turned_scores(k, q) for k, q in zip(keys, queries)]
        if masked:
            scores = [jnp.where(causal, s, -1e30) for s in scores]
        parts = [exponents(s) for s in scores]
        for i, (top, e, z) in enumerate(parts):
            kept[first + i, slot] = e
            put_pair(kept_top, first + i, slot, top)
            put_pair(small_out, first + i, slot, top + jnp.log2(z))

    def third_queries(h):
        big_to(q_rot, 1, 3, h, 2).start()
        big_to(q_rot, 0, 3, h, 1, 2).start()

    members = range(GROUP)
    ahead = jnp.where(me == 0, 1, 0)

    def begin(j, carry):
        first = j * GROUP

        @pl.when(j == 0)
        def _():
            loads[7].wait()
            loads[8].wait()

        norm_rotate(ahead, first)
        for i in members:
            v_turn[first + i] = rows_in[2, :, head_columns(first + i)].astype(jnp.float32).T.astype(jnp.bfloat16)
        return carry

    def spread(j, carry):
        first = j * GROUP

        @pl.when((me == 3) & (j == 0))
        def _():
            third_queries(0)

        @pl.when((me == 2) & (j == 0))
        def _():
            big_to(q_rot, 0, 2, 0, 1).start()

        @pl.when(me == 0)
        def _():
            for i in members:
                big_to(k_rot, 0, 0, first + i, 1).start()
                big_to(v_turn, 1, 1, first + i, 1).start()

        norm_rotate(1 - ahead, first)

        @pl.when((me == 2) & (first >= alone))
        def _():
            for i in members:
                big_to(k_rot, 2, 2, first + i, 3, 2).start()
                big_to(v_turn, 2, 3, first + i, 3, 2).start()

        @pl.when((me == 2) | ((me == 3) & (first < alone)))
        def _():
            partial_scores([k_rot[first + i] for i in members], [q_rot[first + i] for i in members], 0, first, True)

        @pl.when(me == 2)
        def _():
            for i in members:
                small_to(0, 0, first + i, 1, 1).start()

        @pl.when((me == 2) & (j == 0))
        def _():
            for i in range(1, AHEAD):
                big_to(q_rot, 0, 2, i, 1).start()

        @pl.when((me == 3) & (first < alone))
        def _():
            for i in members:
                if i:
                    third_queries(first + i)
                else:
                    @pl.when(j > 0)
                    def _():
                        third_queries(first)
                small_to(0, 1, first + i, 1, 3).start()

        return carry

    lax.fori_loop(0, 1, begin, 0)
    pl.semaphore_wait(barrier, talkers + (nx - 1) + (cores - 1) + (ways - 1))
    for r in range(min(DEEP, direct)):
        for xo in range(1, nx):
            weight_x(xo, r).start()
    if cores > 1:
        for r in range(chunks):
            for way in range(ways):
                weight_core(0, r, way).start()

    lax.fori_loop(0, 1, spread, 0)
    lax.fori_loop(1, count // GROUP, lambda j, carry: spread(j, begin(j, carry)), 0)

    @pl.when(me == 1)
    def _():
        for h in range(alone, count):
            small[h, 2] = jnp.full((2, tok), -1e30, jnp.float32)

    def lowest(h):
        scores = jnp.where(causal, turned_scores(k_rot[h], q_rot[h]), -1e30)
        _, e, z = exponents(scores)
        finish(mixed(e, 1.0 / z, lam_ref[h], v_turn[h]), h)

    def centre(h, third):
        if h is not None:
            came_in(big.at[h, 0:3], 0, h)
            came_in(small.at[h, 0], 1, h)
        if third is not None:
            came_in(big.at[third, 3], 2, third)

            @pl.when(third < alone)
            def _():
                came_in(small.at[third, 1:3], 3, third)

            @pl.when(third >= alone)
            def _():
                came_in(small.at[third, 1], 3, third)

        pair = 2 * tok
        scores, levels, places, values = [], [], [], []
        for place, x in ((1, h), (2, h), (3, third)):
            if x is None:
                continue
            keys = jnp.concatenate([big[x, 0], k_rot[x]], axis=0)
            values.append(jnp.concatenate([big[x, 1], v_turn[x]], axis=1))
            part = turned_scores(keys, q_rot[x] if place == 1 else big[x, place])
            if place == 1:
                part = jnp.concatenate([part[:tok], jnp.where(causal, part[tok:], -1e30)], axis=0)
            scores.append(part)
            levels.append([get_pair(small, x, slot) for slot in ((), (0,), (1, 2))[place - 1]])
            places.append((place, x))
        parts = [exponents(part) for part in scores]
        scales = []
        for (place, x), (top, e, z), others in zip(places, parts, levels):
            if place == 1:
                scales.append(1.0 / z)
            else:
                level = joined([top + jnp.log2(z)] + others)
                put_pair(small_out, x, place - 2, level)
                scales.append(jnp.exp2(top - level))
        mixing = [mixing_of(e, scale, lam_ref[x]) for (_, x), (_, e, _), scale in zip(places, parts, scales)]
        raws = [jnp.dot(v, m, preferred_element_type=jnp.float32) for v, m in zip(values, mixing)]
        for (place, x), raw in zip(places, raws):
            if place > 1:
                big_out[place - 2, x] = raw.astype(jnp.bfloat16)
        if third is not None:
            @pl.when(third < alone)
            def _():
                small_to(1, 1, third, 2, 3).start()

            small_to(2, 1, third, 3, 1).start()
        if h is not None:
            small_to(0, 0, h, 2, 1).start()
        if third is not None:
            big_to(big_out.at[1], 1, 0, third, 3).start()
        if h is not None:
            big_to(big_out.at[0], 0, 0, h, 2, 2).start()
            finish(raws[0], h)

    def upper_scores(h):
        @pl.when(h < alone)
        def _():
            came_in(big.at[h, 3], 0, h)
            partial_scores([k_rot[h]], [big[h, 3]], 1, h, False)
            small_to(1, 2, h, 1, 3).start()

        @pl.when(h + AHEAD < count)
        def _():
            big_to(q_rot, 0, 2, h + AHEAD, 1).start()

    def upper_raw(h, slot, level):
        scale = jnp.exp2(get_pair(kept_top, h, slot) - level)
        return mixed(kept[h, slot], scale, lam_ref[h], v_turn[h])

    def upper_help(h):
        came_in(small.at[h, 1], 3, h)
        big_out[1, h] = upper_raw(h, 1, get_pair(small, h, 1)).astype(jnp.bfloat16)
        big_to(big_out.at[1], 1, 1, h, 3).start()

    def upper_second(h):
        came_in(small.at[h, 0], 1, h)
        came_in(big.at[h, 0], 2, h)
        finish(upper_raw(h, 0, get_pair(small, h, 0)) + big[h, 0].astype(jnp.float32), h)

    def joint_scores(h):
        came_in(big.at[h, 2:4], 2, h)
        scores = turned_scores(jnp.concatenate([big[h, 2], k_rot[h]], axis=0), q_rot[h])
        scores = jnp.concatenate([scores[:tok], jnp.where(causal, scores[tok:], -1e30)], axis=0)
        top, e, z = exponents(scores)
        kept[h, 0] = e[:tok]
        kept[h, 1] = e[tok:]
        put_pair(kept_top, h, 0, top)
        put_pair(small_out, h, 0, top + jnp.log2(z))

    def upper_third(h):
        came_in(small.at[h, 1], 1, h)

        @pl.when(h < alone)
        def _():
            came_in(big.at[h, 0:2], 0, h)
            raw = upper_raw(h, 0, get_pair(small, h, 1)) + big[h, 0].astype(jnp.float32)
            finish(raw + big[h, 1].astype(jnp.float32), h)

        @pl.when(h >= alone)
        def _():
            came_in(big.at[h, 0], 0, h)
            scale = jnp.exp2(get_pair(kept_top, h, 0) - get_pair(small, h, 1))
            e = jnp.concatenate([kept[h, 0], kept[h, 1]], axis=0)
            values = jnp.concatenate([big[h, 3], v_turn[h]], axis=1)
            finish(mixed(e, scale, lam_ref[h], values) + big[h, 0].astype(jnp.float32), h)

    group = GROUP

    def project(g, first, last, parts=((0, GROUP),)):
        arrived = pl.ds(g * group * width, group * width)
        if cores > 1:
            for xo in range(nx):
                weight_core_in(xo, g, arrived).wait_recv()
        for low, high in parts:
            add_heads(g * group + low, high - low, first, last and high == group)

    def add_heads(low, number, first, last):
        rows = pl.ds(low * width, number * width)
        block = heads[:, rows]
        for index in range(n_dp):
            term = jnp.dot(block, wfull[index, rows, :], preferred_element_type=jnp.float32)
            span = slice(index * cols, (index + 1) * cols)
            if not first:
                term = total[:, span] + term
            if last:
                out_ref[0, :, span] = term.astype(out_ref.dtype)
            else:
                total[:, span] = term

    groups = count // group

    def turned_order(at):
        early = (at >= alone - SWAP) & (at < alone)
        late = (at >= alone) & (at < alone + SWAP)
        return at + jnp.where(early, SWAP, jnp.where(late, -SWAP, 0))


    first_x = jnp.where(me == 1, 2, 1)
    first_y = first_x + 2 * per_chunk
    last_x = first_x + direct * per_chunk

    def step(it, carry):
        @pl.when((me == 2) & (it < count))
        def _():
            upper_scores(it)

        turn = lax.rem(it - first_x + per_chunk, per_chunk) == 0

        @pl.when(turn & (it >= first_x) & (it < last_x))
        def _():
            forward_x((it - first_x) // per_chunk)

        @pl.when(turn & (it >= first_y) & (it < first_y + direct * per_chunk))
        def _():
            forward_y((it - first_y) // per_chunk)

        @pl.when(it == jnp.where(me < 2, last_x, HELP + alone + 1))
        def _():
            forward_direct()

        @pl.when((me == 0) & (it < count))
        def _():
            lowest(it)

        @pl.when((me == 1) & (it < BEHIND))
        def _():
            centre(it, None)

        @pl.when((me == 1) & (it >= BEHIND) & (it < count))
        def _():
            centre(it, jnp.where(it == count - 1, it - 1, it - BEHIND))

        @pl.when((me == 1) & (it >= count - BEHIND) & (it < count))
        def _():
            centre(None, jnp.where(it == count - 1, it, it - 1))

        @pl.when((me == 2) & (it >= HELP) & (it < HELP + alone))
        def _():
            upper_help(it - HELP)

        @pl.when((me == 2) & (it >= NEAR) & (it < NEAR + count))
        def _():
            upper_second(it - NEAR)

        @pl.when((me == 3) & (it >= GROUP) & (it < 2 * GROUP))
        def _():
            joint_scores(alone + it - GROUP)

        for i in range(GROUP):
            @pl.when((me == 3) & (it == LAG + PACES[i]))
            def _(i=i):
                big_to(q_rot, 0, 3, alone + i, 1, 2).start()
                small_to(0, 1, alone + i, 1, 3).start()

        @pl.when((me == 3) & (it >= LAG))
        def _():
            upper_third(turned_order(it - LAG))

        for g in range(groups - 1):
            @pl.when(it == g * group + PROJECT + jnp.where(me == 3, LATE, jnp.where((me == 1) & (g == 1), 2, 0)))
            def _(g=g):
                if g == 0:
                    own_weight.wait()
                project(g, g == 0, False)

        return carry

    steps = count + NEAR
    lax.fori_loop(0, steps, step, 0)

    @pl.when(me == 3)
    def _():
        for h in range(steps - LAG, count - 2):
            upper_third(h)

    project(groups - 1, False, False, ((0, GROUP - 2),))

    @pl.when(me == 3)
    def _():
        for h in range(max(steps - LAG, count - 2), count):
            upper_third(h)

    add_heads(count - 2, 2, False, True)

    whole, most = q_rot.at[:], q_rot.at[0:alone]
    rows = small_out.at[:, 0]
    most_rows = small_out.at[0:alone, 0]

    @pl.when(me == 0)
    def _():
        gone(whole, big_send.at[0])
        gone(whole, big_send.at[1])

    @pl.when(me == 1)
    def _():
        gone(whole, big_send.at[0])
        gone(whole, big_send.at[1])
        gone(rows, small_send.at[0])
        gone(most_rows, small_send.at[1])
        gone(rows, small_send.at[2])

    @pl.when(me == 2)
    def _():
        gone(whole, big_send.at[0])
        gone(most, big_send.at[1])
        gone(q_rot.at[0 : 2 * GROUP], big_send.at[2])
        gone(rows, small_send.at[0])
        gone(most_rows, small_send.at[1])

    @pl.when(me == 3)
    def _():
        gone(whole, big_send.at[0])
        gone(most, big_send.at[1])
        gone(rows, small_send.at[0])

    for xo in range(nx):
        if xo:
            sent_x = wfull.at[0, 0 : (direct + ways) * piece, :]
            moved(sent_x, sent_x, wx_send.at[xo - 1], wx_recv.at[0, 0], {"dp": dp_index(xo, 0)}).wait_send()
            if ways > 1:
                sent_y = wfull.at[0, 0 : direct * piece, :]
                moved(sent_y, sent_y, wy_send.at[xo - 1], wy_recv.at[0, 0], {"dp": dp_index(xo, 0)}).wait_send()
        if cores > 1:
            sent_core = wfull.at[0]
            moved(sent_core, sent_core, wc_send.at[xo], wc_recv.at[0, 0], {"dp": dp_index(0, 1)}).wait_send()


def split_local(n, n_dp, n_grp, query_rows, key_rows, value_rows, query_gain, key_gain, lambdas, head_gain, out_weight):
    tok = query_rows.shape[1]
    head_size = query_gain.shape[0]
    width = head_gain.shape[0]
    count = lambdas.shape[0]
    depth, cols = out_weight.shape
    ways = WAYS if n_grp == WAYS else 1
    chunks = count // ways
    cores = CORES if n_dp % CORES == 0 else 1
    nx = n_dp // cores
    cosine, sine = rotation_tables(tok * n, head_size)
    anywhere = pl.BlockSpec(memory_space=pl.ANY)
    vmem = pl.BlockSpec(memory_space=pltpu.VMEM)
    dma = pltpu.SemaphoreType.DMA
    across = max(nx - 1, 1)
    return pl.pallas_call(
        functools.partial(split_kernel, n, n_dp, n_grp, head_size, chunks),
        out_shape=pltpu.VMEM((1, tok, n_dp * cols), jnp.bfloat16),
        in_specs=[anywhere] * 3
        + [anywhere] * 7,
        out_specs=vmem,
        scratch_shapes=[
            pltpu.VMEM((tok, n_dp * cols), jnp.float32),
            pltpu.VMEM((3, tok, count * width), jnp.bfloat16),
            pltpu.VMEM((2, count, tok, width), jnp.bfloat16),
            pltpu.VMEM((count, tok, width), jnp.bfloat16),
            pltpu.VMEM((count, 4, tok, width), jnp.bfloat16),
            pltpu.VMEM((count, 3, 2, tok), jnp.float32),
            pltpu.VMEM((2, count, tok, width), jnp.bfloat16),
            pltpu.VMEM((count, 2, 2, tok), jnp.float32),
            pltpu.VMEM((count, 2, tok, 2 * tok), jnp.float32),
            pltpu.VMEM((count, 2, 2, tok), jnp.float32),
            pltpu.VMEM((width, tok), jnp.float32),
            pltpu.VMEM((tok, count * width), jnp.bfloat16),
            pltpu.VMEM((n_dp, depth, cols), jnp.bfloat16),
            pltpu.VMEM((tok, width), jnp.float32),
            pltpu.VMEM((tok, width), jnp.float32),
            pltpu.VMEM((4, tok, width), jnp.float32),
            pltpu.VMEM((1, head_size), jnp.float32),
            pltpu.VMEM((1, head_size), jnp.float32),
            pltpu.SMEM((count,), jnp.float32),
            pltpu.VMEM((1, width), jnp.float32),
            dma((10,)),
            dma((3,)),
            dma((3,)),
            dma((4, count)),
            dma((across,)),
            dma((across, chunks - 1 + ways)),
            dma((across,)),
            dma((across, chunks)),
            dma((nx,)),
            dma((nx, count // GROUP)),
        ],
        compiler_params=pltpu.CompilerParams(
            collective_id=0, has_side_effects=True, vmem_limit_bytes=56 * 1024 * 1024
        ),
    )(
        query_rows, key_rows, value_rows,
        query_gain[None, :], key_gain[None, :], lambdas, head_gain[None, :],
        out_weight, jnp.asarray(cosine), jnp.asarray(sine),
    )


def plan(n, tok, width, count, n_grp):
    ways = WAYS if n_grp == WAYS else 1
    fits = n == PARTS and tok == width and count % (GROUP * ways) == 0
    return split_local if fits else local


def solution(mesh):
    rows = P(("grp", "dp"), "sp", None)
    n, n_dp, n_grp = mesh.shape["sp"], mesh.shape["dp"], mesh.shape["grp"]

    def body(*args):
        chosen = plan(n, args[0].shape[1], args[6].shape[0], args[5].shape[0], n_grp)
        return chosen(n, n_dp, n_grp, *args)

    return jax.shard_map(
        body,
        mesh=mesh,
        in_specs=(rows, rows, rows, P(), P(), P(), P(), P(None, "dp")),
        out_specs=rows,
        check_vma=False,
    )
```
